32 devices in a mesh: sp: 16 (over z, y, x), tp: 2 (over core).
Axes of the slice: x: 2, y: 2, z: 4, core: 2. Of those that a mesh axis runs over, the one named last changes fastest.
Arguments:
- tokens: bfloat16 [4096, 3072], P('sp', 'tp'), may hold values from -6 to 6
- norm_gain: float32 [3072], replicated, may hold values from 0.1 to 1.9
- outer_gate_w: bfloat16 [3072, 1536], P('sp', 'tp'), may hold values from -0.109375 to 0.109375
- inner_gate_w: bfloat16 [3072, 1536], P('sp', 'tp'), may hold values from -0.109375 to 0.109375
- signal_w: bfloat16 [3072, 1536], P('sp', 'tp'), may hold values from -0.109375 to 0.109375
- conv_taps: float32 [3, 1536], P(None, 'tp'), may hold values from -3.5 to 3.5
- query_w: bfloat16 [3072, 1536], P('sp', 'tp'), may hold values from -1.5 to 1.5
- key_w: bfloat16 [3072, 512], P('sp', 'tp'), may hold values from -1.5 to 1.5
- value_w: bfloat16 [3072, 512], P('sp', 'tp'), may hold values from -0.109375 to 0.109375
- sink_logits: float32 [24], P('tp'), may hold values from -1 to 5
- out_conv_w: bfloat16 [1536, 3072], P('tp', 'sp'), may hold values from -0.109375 to 0.109375
- out_attn_w: bfloat16 [1536, 3072], P('tp', 'sp'), may hold values from -0.109375 to 0.109375
Outputs:
- mixed: bfloat16 [4096, 3072], P(('sp', 'tp'))
The draws below stay inside these ranges and needn't reach their ends.
All inputs are finite; a program needn't handle non-finite values.
Results may differ from the reference program's by a relative error of at most 0.02.
Values may be sent and summed in bfloat16 or wider, within the bound.
A program may use at most 64 MiB of HBM per device.

```python
import jax
import jax.numpy as jnp
from jax import lax

D = 3072
CONV = 1536
QHEADS = 24
KVHEADS = 8
HEAD = 64
TAPS = 3
WINDOW = 128
TOKENS = 4096
N_TP = 2


def draw_query_w(key, part):
    drawn = jax.random.normal(jax.random.fold_in(key, 21), (D, QHEADS * HEAD), jnp.float32) * D ** (-0.5)
    return jnp.clip(drawn, -1.5, 1.5).astype(jnp.bfloat16)


def draw_key_w(key, part):
    drawn = jax.random.normal(jax.random.fold_in(key, 22), (D, KVHEADS * HEAD), jnp.float32) * D ** (-0.5)
    return jnp.clip(drawn, -1.5, 1.5).astype(jnp.bfloat16)


def levels(key, dims, split, smallest, largest):
    def one(dim, parts):
        heights = jax.random.uniform(jax.random.fold_in(jax.random.fold_in(key, 6), dim), (parts,), jnp.float32, smallest / len(split), largest / len(split))
        return jnp.repeat(jnp.exp(heights), dims[dim] // parts).reshape((-1,) + (1,) * (len(dims) - dim - 1))

    level = one(*split[0])
    for cut in split[1:]:
        level = level * one(*cut)
    return level


def noise(key, shape, width, most, split=(), kind=jnp.bfloat16):
    entries = jax.random.normal(key, shape, jnp.float32) * width
    if len(split) > 0:
        entries = levels(key, shape, split, -0.22, 0.18) * entries
    return jnp.clip(entries, min=-most, max=most).astype(kind)


def setup_inputs(seed: int = 0) -> dict:
    key_of = jax.random.split(jax.random.key(seed), 13)
    tokens = noise(key_of[0], (TOKENS, D), 1.0, 6.0, ((0, 16), (1, 2)))
    norm_gain = jnp.clip(1.0 + 0.18 * jax.random.normal(key_of[1], (D,), jnp.float32), 0.1, 1.9)
    outer_gate_w = noise(key_of[2], (D, CONV), D ** -0.5, 0.109375, ((0, 16), (1, 2)))
    inner_gate_w = noise(key_of[3], (D, CONV), D ** -0.5, 0.109375, ((0, 16), (1, 2)))
    signal_w = noise(key_of[4], (D, CONV), D ** -0.5, 0.109375, ((0, 16), (1, 2)))
    conv_taps = noise(key_of[5], (TAPS, CONV), TAPS ** -0.5, 3.5, ((1, 2),), jnp.float32)
    query_w = draw_query_w(jax.random.fold_in(key_of[12], 71), 0)
    key_w = draw_key_w(jax.random.fold_in(key_of[12], 71), 0)
    value_w = noise(key_of[8], (D, KVHEADS * HEAD), D ** -0.5, 0.109375, ((0, 16), (1, 2)))
    sink_logits = jnp.clip(-1.0 + 6.0 * jax.random.uniform(key_of[9], (QHEADS,), jnp.float32) ** levels(key_of[9], (QHEADS,), ((0, 2),), -0.2, 0.2), -1.0, 5.0)
    out_conv_w = noise(key_of[10], (CONV, D), (CONV + QHEADS * HEAD) ** -0.5, 0.109375, ((0, 2), (1, 16)))
    out_attn_w = noise(key_of[11], (QHEADS * HEAD, D), (CONV + QHEADS * HEAD) ** -0.5, 0.109375, ((0, 2), (1, 16)))
    return dict(tokens=tokens, norm_gain=norm_gain, outer_gate_w=outer_gate_w, inner_gate_w=inner_gate_w, signal_w=signal_w, conv_taps=conv_taps, query_w=query_w, key_w=key_w, value_w=value_w, sink_logits=sink_logits, out_conv_w=out_conv_w, out_attn_w=out_attn_w)


def reference(tokens, norm_gain, outer_gate_w, inner_gate_w, signal_w, conv_taps, query_w, key_w, value_w, sink_logits, out_conv_w, out_attn_w):
    f32 = jnp.float32
    bf16 = jnp.bfloat16
    x32 = tokens.astype(f32)
    normed = (x32 * lax.rsqrt(lax.optimization_barrier(jnp.mean(x32 * x32, axis=-1, keepdims=True)) + 1e-06) * norm_gain).astype(bf16)

    def project(weight):
        return jnp.dot(normed, weight, preferred_element_type=f32).astype(bf16)
    outer = project(outer_gate_w)
    inner = project(inner_gate_w)
    signal = project(signal_w)
    queries = project(query_w)
    keys = project(key_w)
    values = project(value_w)
    gated = (inner.astype(f32) * signal.astype(f32)).astype(bf16)
    padded = jnp.concatenate([jnp.zeros((TAPS - 1, CONV), bf16), gated], axis=0).astype(f32)
    conv = sum((conv_taps[k] * padded[k:k + TOKENS] for k in range(TAPS)))
    conv_out = (outer.astype(f32) * conv).astype(bf16)
    group = QHEADS // KVHEADS
    span = min(512, TOKENS)
    slopes = jnp.exp2(-8.0 * jnp.arange(1, QHEADS + 1, dtype=f32) / QHEADS).reshape(KVHEADS, group)
    sinks = sink_logits.reshape(KVHEADS, group)[:, :, None]
    keys_pad = jnp.concatenate([jnp.zeros((WINDOW, KVHEADS * HEAD), bf16), keys], axis=0)
    values_pad = jnp.concatenate([jnp.zeros((WINDOW, KVHEADS * HEAD), bf16), values], axis=0)

    def attend(block):
        start = (block * span).astype(jnp.int32)
        qb = lax.dynamic_slice_in_dim(queries, start, span, 0).reshape(span, KVHEADS, group, HEAD).astype(f32)
        kb = lax.dynamic_slice_in_dim(keys_pad, start, span + WINDOW, 0).reshape(span + WINDOW, KVHEADS, HEAD).astype(f32)
        vb = lax.dynamic_slice_in_dim(values_pad, start, span + WINDOW, 0).reshape(span + WINDOW, KVHEADS, HEAD).astype(f32)
        scores = jnp.einsum('qhgd,shd->hgqs', qb, kb) * HEAD ** (-0.5)
        qpos = start + jnp.arange(span, dtype=jnp.int32)
        kpos = start - WINDOW + jnp.arange(span + WINDOW, dtype=jnp.int32)
        dist = qpos[:, None] - kpos[None, :]
        valid = (dist >= 0) & (dist < WINDOW) & (kpos >= 0)[None, :]
        scores = scores - slopes[:, :, None, None] * dist.astype(f32)
        scores = jnp.where(valid, scores, -1e+30)
        top = jnp.maximum(lax.optimization_barrier(jnp.max(scores, axis=-1)), sinks)
        expo = jnp.exp(scores - top[..., None])
        total = lax.optimization_barrier(jnp.sum(expo, axis=-1)) + jnp.exp(sinks - top)
        probs = (expo / total[..., None]).astype(bf16).astype(f32)
        out = jnp.einsum('hgqs,shd->qhgd', probs, vb)
        return out.reshape(span, QHEADS * HEAD)
    attn_out = lax.map(attend, jnp.arange(TOKENS // span, dtype=jnp.int32)).reshape(TOKENS, QHEADS * HEAD).astype(bf16)
    conv_part = CONV // N_TP
    attn_part = QHEADS * HEAD // N_TP
    total_sum = jnp.zeros((TOKENS, D), f32)
    for index in range(N_TP):
        conv_cols = conv_out[:, index * conv_part:(index + 1) * conv_part]
        attn_cols = attn_out[:, index * attn_part:(index + 1) * attn_part]
        partial_value = jnp.dot(conv_cols, out_conv_w[index * conv_part:(index + 1) * conv_part], preferred_element_type=f32)
        partial_value = partial_value + jnp.dot(attn_cols, out_attn_w[index * attn_part:(index + 1) * attn_part], preferred_element_type=f32)
        total_sum = total_sum + partial_value.astype(bf16).astype(f32)
    return total_sum.astype(bf16)
```

```python
import functools

import jax
import jax.numpy as jnp
from jax import lax
from jax.experimental import pallas as pl
from jax.experimental.pallas import tpu as pltpu
from jax.sharding import PartitionSpec as P

QHEADS = 24
KVHEADS = 8
HEAD = 64
TAPS = 3
WINDOW = 128
PLANE = 4
MESH = pl.DeviceIdType.MESH


def from_behind(value, axis, steps):
    count = lax.axis_size(axis)
    initial, last = (max(0, -steps), min(count, count - steps))
    return lax.ppermute(value, axis, [(source, source + steps) for source in range(initial, last)])


def add_products(pieces, normed):
    return tuple((jnp.dot(normed, piece, preferred_element_type=jnp.float32) for piece in pieces))


def convolve(gated, before, outer, conv_taps):
    extended = jnp.concatenate([before, gated], axis=0).astype(jnp.float32)
    length = gated.shape[0]
    conv = sum((conv_taps[k] * extended[k : k + length] for k in range(conv_taps.shape[0])))
    return (outer.astype(jnp.float32) * conv).astype(jnp.bfloat16)


def attention(queries, keys_ext, values_ext, sink_logits, offset):
    f32 = jnp.float32
    length = queries.shape[0]
    kv_local = keys_ext.shape[1] // HEAD
    group = QHEADS // KVHEADS
    heads_local = kv_local * group
    span = min(512, length)
    first = lax.axis_index("tp") * heads_local + 1
    slopes = jnp.exp2(
        -8.0 * (first + jnp.arange(heads_local, dtype=jnp.int32)).astype(f32) / QHEADS
    ).reshape(kv_local, group)
    sinks = sink_logits.reshape(kv_local, group)[:, :, None]

    def attend(block):
        start = block * span
        qblock = queries.reshape(span, kv_local, group, HEAD)
        kblock = keys_ext.reshape(span + WINDOW, kv_local, HEAD)
        vblock = values_ext.reshape(span + WINDOW, kv_local, HEAD)
        scores = jnp.einsum(
            "qhgd,shd->hgqs", qblock, kblock, preferred_element_type=f32
        ) * HEAD ** (-0.5)
        qpos = offset + start + jnp.arange(span, dtype=jnp.int32)
        kpos = offset + start - WINDOW + jnp.arange(span + WINDOW, dtype=jnp.int32)
        dist = qpos[:, None] - kpos[None, :]
        valid = (dist >= 0) & (dist < WINDOW) & (kpos >= 0)[None, :]
        scores = scores - slopes[:, :, None, None] * dist.astype(f32)
        scores = jnp.where(valid, scores, -1e30)
        top = jnp.maximum(jnp.max(scores, axis=-1), sinks)
        expo = jnp.exp(scores - top[..., None])
        total = jnp.sum(expo, axis=-1) + jnp.exp(sinks - top)
        probs = (expo / total[..., None]).astype(jnp.bfloat16)
        out = jnp.einsum("hgqs,shd->qhgd", probs, vblock, preferred_element_type=f32)
        return out.reshape(span, heads_local * HEAD)

    blocks = lax.map(attend, jnp.arange(length // span, dtype=jnp.int32))
    return blocks.reshape(length, heads_local * HEAD).astype(jnp.bfloat16)


def body(
    tokens,
    norm_gain,
    outer_gate_w,
    inner_gate_w,
    signal_w,
    conv_taps,
    query_w,
    key_w,
    value_w,
    sink_logits,
    out_conv_w,
    out_attn_w,
):
    f32 = jnp.float32
    bf16 = jnp.bfloat16
    whole = lax.all_gather(tokens, "tp", axis=1, tiled=True)
    x32 = whole.astype(f32)
    normed = (
        x32 * lax.rsqrt(jnp.mean(x32 * x32, axis=-1, keepdims=True) + 1e-06) * norm_gain
    ).astype(bf16)
    length = normed.shape[0]
    offset = lax.axis_index("sp") * length

    def fold_rows(pieces):
        return add_products(pieces, normed)

    conv_weights = (outer_gate_w, inner_gate_w, signal_w)
    conv_results = fold_rows(
        (
            lax.all_gather(conv_weights[0], "sp", axis=0, tiled=True),
            lax.all_gather(conv_weights[1], "sp", axis=0, tiled=True),
            lax.all_gather(conv_weights[2], "sp", axis=0, tiled=True),
        )
    )
    outer, inner, signal = tuple((result.astype(bf16) for result in conv_results))
    gated = (inner.astype(f32) * signal.astype(f32)).astype(bf16)
    before = from_behind(gated[length - TAPS + 1 :], "sp", 1)
    conv_out = convolve(gated, before, outer, conv_taps)
    attn_weights = (query_w, key_w, value_w)
    attn_results = fold_rows(
        (
            lax.all_gather(attn_weights[0], "sp", axis=0, tiled=True),
            lax.all_gather(attn_weights[1], "sp", axis=0, tiled=True),
            lax.all_gather(attn_weights[2], "sp", axis=0, tiled=True),
        )
    )
    queries, keys, values = tuple((result.astype(bf16) for result in attn_results))
    keys_before, values_before = from_behind(
        (keys[length - WINDOW :], values[length - WINDOW :]), "sp", 1
    )
    keys_ext = jnp.concatenate([keys_before, keys], axis=0)
    values_ext = jnp.concatenate([values_before, values], axis=0)
    attn_out = attention(queries, keys_ext, values_ext, sink_logits, offset)
    conv_whole, attn_whole = (
        lax.all_gather(out_conv_w, "sp", axis=1, tiled=True),
        lax.all_gather(out_attn_w, "sp", axis=1, tiled=True),
    )
    result = jnp.dot(conv_out, conv_whole, preferred_element_type=f32)
    mixed = lax.psum_scatter(
        (result + jnp.dot(attn_out, attn_whole, preferred_element_type=f32)).astype(jnp.bfloat16),
        "tp",
        scatter_dimension=0,
        tiled=True,
    ).astype(jnp.float32)
    return mixed.astype(bf16)

class Stream:
    def __init__(self, at, src, buf, sems, split):
        self.at, self.src, self.buf, self.split = at, src, buf, split
        self.zs, self.zr, self.ys, self.yr, self.xs, self.xr = sems
        self.rows = src.shape[1] // split

    def part(self, s):
        return pl.ds(s * self.rows, self.rows)

    def slot(self, t, origin, y, x, s):
        return self.buf.at[t, origin, y, x, self.part(s)]

    def origin(self, up, d):
        return self.at.z - d if up else self.at.z + d

    def column(self, r):
        return self.at.x if r == 0 else 1 - self.at.x

    def z_copy(self, up, d, r, t, s, send_d):
        at = self.at
        dst = self.slot(t, self.origin(up, d), at.y, self.column(r), s)
        src = self.src.at[2 * t + at.x, self.part(s)] if d == 0 and r == 0 else dst
        i = ((((0 if up else 1) * (at.layers - 1) + send_d) * 2 + r) * 2 + t) * self.split + s
        return remote(src, dst, self.zs.at[i], self.zr.at[i], at.above if up else at.below)

    def z_send(self, up, d, r, t, s, action="start"):
        z, layers = self.at.z, self.at.layers
        if d >= layers - 1:
            return
        if up:
            go = (z >= d) & (z + (1 if t else 2) < layers)
        else:
            go = (z + d < layers) & (z >= (2 if t else 1))

        @pl.when(go)
        def _():
            getattr(self.z_copy(up, d, r, t, s, d), action)()

    def y_copy(self, up, d, r, s, y):
        at = self.at
        dst = self.slot(at.zl, self.origin(up, d), y, self.column(r), s)
        src = self.src.at[2 * at.zl + at.x, self.part(s)] if d == 0 and r == 0 else dst
        m = d if up or d == 0 else at.layers - 1 + d
        i = (m * 2 + r) * self.split + s
        return remote(src, dst, self.ys.at[i], self.yr.at[i], at.ypeer)

    def x_copy(self, t, s, receive=False):
        at = self.at
        src = self.src.at[2 * t + 1 - at.x, self.part(s)]
        dst = self.slot(t, at.z, at.y, 1 - at.x if receive else at.x, s)
        i = t * self.split + s
        return remote(src, dst, self.xs.at[i], self.xr.at[i], at.xpeer)

    def start_z(self):
        for s in range(self.split):
            for t in range(2):
                self.z_send(True, 0, 0, 1 - t, s)
                self.z_send(False, 0, 0, t, s)

    def start_x(self):
        for s in range(self.split):
            for t in range(2):
                self.x_copy(t, s).start()

    def start_y(self):
        for s in range(self.split):
            self.y_copy(True, 0, 0, s, self.at.y).start()

    def on_x(self):
        for s in range(self.split):
            for t in range(2):
                self.x_copy(t, s, True).wait_recv()
                self.z_send(True, 0, 1, t, s)
                self.z_send(False, 0, 1, t, s)

                @pl.when(self.at.zl == t)
                def _():
                    self.y_copy(True, 0, 1, s, self.at.y).start()

    def on_z(self, d, r):
        z, layers, zl = self.at.z, self.at.layers, self.at.zl

        def arrive(up, t, s):
            if up:
                here = (z >= d) if t else (z >= d) & (z + 1 < layers)
            else:
                here = (z + d < layers) & (z >= 1) if t else (z + d < layers)

            @pl.when(here)
            def _():
                self.z_copy(up, d, r, t, s, d - 1).wait_recv()
                self.z_send(up, d, r, t, s)

                @pl.when(zl == t)
                def _():
                    self.y_copy(up, d, r, s, self.at.y).start()

        for s in range(self.split):
            for t in range(2):
                arrive(True, 1 - t, s)
                arrive(False, t, s)

    def on_y(self, d, action="wait_recv"):
        z, layers, y = self.at.z, self.at.layers, self.at.y
        side = 1 - y if action == "wait_recv" else y

        def each(up):
            for r in range(2):
                for s in range(self.split):
                    getattr(self.y_copy(up, d, r, s, side), action)()

        if d == 0:
            each(True)
            return

        @pl.when(z >= d)
        def _():
            each(True)

        @pl.when(z + d < layers)
        def _():
            each(False)

    def finish(self):
        for s in range(self.split):
            for t in range(2):
                self.x_copy(t, s).wait_send()
        for d in range(self.at.layers):
            self.on_y(d, "wait_send")
            for r in range(2):
                for t in range(2):
                    for s in range(self.split):
                        self.z_send(True, d, r, t, s, "wait_send")
                        self.z_send(False, d, r, t, s, "wait_send")


class Place:
    def __init__(self, count):
        me, core = lax.axis_index("sp"), lax.axis_index("tp")
        self.me, self.core, self.layers = me, core, count // PLANE
        self.z, self.y, self.x = me // PLANE, lax.rem(me // 2, 2), lax.rem(me, 2)
        self.zl, self.zh = lax.rem(self.z, 2), self.z // 2
        self.spot = 2 * self.zl + self.x

        def device(sp, tp=core):
            return {"sp": sp, "tp": tp}

        self.partner = device(me, 1 - core)
        self.xpeer = device(me + 1 - 2 * self.x)
        self.ypeer = device(me + 2 - 4 * self.y)
        self.zpeer = device(me + PLANE * (1 - 2 * self.zl))
        self.above, self.below = device(me + PLANE), device(me - PLANE)
        self.after, self.prior = device(me + PLANE + 2), device(me - PLANE - 2)
        self.has_after = (self.y == 1) & (self.zh + 1 < self.layers // 2)
        self.has_prior = (self.y == 0) & (self.zh > 0)

    def greet(self):
        barrier = pltpu.get_barrier_semaphore()

        def signal(target):
            pl.semaphore_signal(barrier, inc=1, device_id=target, device_id_type=MESH)

        for target in (self.partner, self.xpeer, self.ypeer):
            signal(target)
        number = 3
        for go, target in (
            (self.z + 1 < self.layers, self.above),
            (self.z > 0, self.below),
            (self.has_after, self.after),
            (self.has_prior, self.prior),
        ):
            pl.when(go)(functools.partial(signal, target))
            number = number + jnp.where(go, 1, 0)
        pl.semaphore_wait(barrier, number)


def remote(src, dst, send_sem, recv_sem, target):
    return pltpu.make_async_remote_copy(
        src_ref=src, dst_ref=dst, send_sem=send_sem, recv_sem=recv_sem, device_id=target, device_id_type=MESH
    )


def layer_kernel(
    count, chans, wide, split, slopes_ref, sinks_ref, tok_ref, w_ref, o_ref, gain_ref, taps_ref, out_ref,
    x_ref, nrm_ref, wbuf, obuf, acc_ref, ext, gext, hid, dsend, drecv, own, s1, r1, s2, r2,
    wzs, wzr, wys, wyr, wxs, wxr, ozs, ozr, oys, oyr, oxs, oxr, ts, tr, hs, hr, ds, dr, fs, fr, gs, gr,
):
    f32, bf16 = jnp.float32, jnp.bfloat16
    at = Place(count)
    core, layers, x, y, z, zl, zh, spot = at.core, at.layers, at.x, at.y, at.z, at.zl, at.zh, at.spot
    rows, half = tok_ref.shape
    length = 2 * rows
    group = wide // HEAD
    front = 8
    ins = Stream(at, w_ref, wbuf, (wzs, wzr, wys, wyr, wxs, wxr), split)
    outs = Stream(at, o_ref, obuf, (ozs, ozr, oys, oyr, oxs, oxr), 1)
    at.greet()

    def block(p, side=None):
        return x_ref.at[core if side is None else side, pl.ds(pl.multiple_of(p * rows, rows), rows)]

    p_own, p_x, p_z, p_far = spot, 2 * zl + 1 - x, 2 * (1 - zl) + x, 2 * (1 - zl) + 1 - x
    ins.start_z()
    ins.start_x()
    ins.start_y()
    tok_x = remote(tok_ref, block(p_own), ts.at[0], tr.at[0], at.xpeer)
    tok_z = remote(tok_ref, block(p_own), ts.at[1], tr.at[1], at.zpeer)
    tok_far = remote(block(p_z), block(p_z), ts.at[2], tr.at[2], at.xpeer)
    swaps = [
        remote(tok_ref if k == 0 else block(p), block(p), ts.at[3 + k], tr.at[3 + k], at.partner)
        for k, p in enumerate((p_own, p_x, p_z, p_far))
    ]
    tok_x.start()
    tok_z.start()
    swaps[0].start()
    wbuf[zl, z, y, x] = w_ref[2 * zl + x]
    x_ref[core, pl.ds(pl.multiple_of(p_own * rows, rows), rows), :] = tok_ref[...]
    span = 2 * half // layers
    strip = 32

    def normalise(k, p):
        remote(tok_ref, block(p, 1 - core), ts.at[3 + k], tr.at[3 + k], at.partner).wait_recv()

        def step(i, carry):
            at_rows = pl.ds(pl.multiple_of(p * rows + i * strip, strip), strip)
            whole = jnp.concatenate([x_ref[0, at_rows, :], x_ref[1, at_rows, :]], axis=1).astype(f32)
            mean = jnp.sum(whole * whole, axis=1, keepdims=True) / (2 * half)
            scaled = (whole * lax.rsqrt(mean + 1e-06) * gain_ref[...]).astype(bf16)
            for j in range(layers):
                nrm_ref[j, at_rows, :] = scaled[:, j * span : (j + 1) * span]
            return carry

        lax.fori_loop(0, rows // strip, step, 0)

    def add_layer(origin, fresh):
        def step(i, carry):
            at_rows = pl.ds(pl.multiple_of(i * rows, rows), rows)
            product = jnp.dot(
                nrm_ref[origin, at_rows, :],
                wbuf[zl, origin].reshape(span, wbuf.shape[5]),
                preferred_element_type=f32,
            )
            acc_ref[at_rows, :] = product if fresh else acc_ref[at_rows, :] + product
            return carry

        lax.fori_loop(0, PLANE, step, 0)

    def add_both(d):
        ins.on_y(d)

        @pl.when(z >= d)
        def _():
            add_layer(z - d, False)

        @pl.when(z + d < layers)
        def _():
            add_layer(z + d, False)

    ins.on_x()
    ins.on_z(1, 0)
    remote(tok_ref, block(p_z), ts.at[1], tr.at[1], at.zpeer).wait_recv()
    tok_far.start()
    swaps[2].start()
    outs.start_x()
    remote(tok_ref, block(p_x), ts.at[0], tr.at[0], at.xpeer).wait_recv()
    swaps[1].start()
    ins.on_z(1, 1)
    normalise(0, p_own)
    normalise(2, p_z)
    if layers > 2:
        ins.on_z(2, 0)
    normalise(1, p_x)
    remote(tok_ref, block(p_far), ts.at[2], tr.at[2], at.xpeer).wait_recv()
    swaps[3].start()
    if layers > 2:
        ins.on_z(2, 1)
    normalise(3, p_far)
    outs.start_z()
    ins.on_y(0)
    add_layer(z, True)
    for d in range(3, layers):
        ins.on_z(d, 0)
        ins.on_z(d, 1)
    add_both(1)
    outs.start_y()
    outs.on_x()
    obuf[zl, z, y, x] = o_ref[2 * zl + x]
    for d in range(2, layers):
        add_both(d)
    outs.on_z(1, 0)

    def spread(i, carry):
        run, start = i // 4, pl.multiple_of(lax.rem(i, 4) * WINDOW, WINDOW)
        chunk = acc_ref[pl.ds(pl.multiple_of(i * WINDOW, WINDOW), WINDOW), :].astype(bf16)
        ext[run, pl.ds(start + WINDOW, WINDOW), :] = chunk[:, 3 * chans + wide :]
        product = chunk[:, chans : 2 * chans].astype(f32) * chunk[:, 2 * chans : 3 * chans].astype(f32)
        gext[run, pl.ds(start + front, WINDOW), :] = product.astype(bf16).astype(f32)
        return carry

    lax.fori_loop(0, 2 * length // WINDOW, spread, 0)

    def tails(run, after, target, action):
        kv = remote(
            ext.at[run, pl.ds(length, WINDOW)], ext.at[after, pl.ds(0, WINDOW)],
            hs.at[2 * run], hr.at[2 * after], target,
        )
        gated = remote(
            gext.at[run, pl.ds(length, front)], gext.at[after, pl.ds(0, front)],
            hs.at[2 * run + 1], hr.at[2 * after + 1], target,
        )
        for copy in (kv, gated):
            getattr(copy, action)()

    def all_tails(action):
        @pl.when(y == 0)
        def _():
            for run in range(2):
                tails(run, run, at.ypeer, action)

        @pl.when(y == 1)
        def _():
            tails(0, 1, at.ypeer, action)

        @pl.when(at.has_after)
        def _():
            tails(1, 0, at.after, action)

    all_tails("start")
    first_run = (y == 0) & (zh == 0)

    @pl.when(first_run)
    def _():
        ext[0, 0:WINDOW, :] = jnp.zeros((WINDOW, 2 * HEAD), bf16)
        gext[0, 0:front, :] = jnp.zeros((front, chans), f32)

    taps = sum(jnp.where(spot == c, taps_ref[:, c * chans : (c + 1) * chans], 0.0) for c in range(PLANE))
    row = lax.broadcasted_iota(jnp.int32, (WINDOW, 2 * WINDOW), 0)
    col = lax.broadcasted_iota(jnp.int32, (WINDOW, 2 * WINDOW), 1)
    dist = WINDOW + row - col
    near = (dist >= 0) & (dist < WINDOW)
    far = dist.astype(f32)

    def mix(run, blk):
        start = pl.multiple_of(blk * WINDOW, WINDOW)
        chunk = acc_ref[pl.ds(pl.multiple_of(run * length + start, WINDOW), WINDOW), :].astype(bf16)
        window = gext[run, pl.ds(start, WINDOW + front), :]
        conv = sum(
            taps[k : k + 1, :] * window[front - TAPS + 1 + k : front - TAPS + 1 + k + WINDOW]
            for k in range(TAPS)
        )
        pieces = [(chunk[:, :chans].astype(f32) * conv).astype(bf16)]
        kv = ext[run, pl.ds(start, 2 * WINDOW), :]
        keys, values = kv[:, :HEAD], kv[:, HEAD:]
        offset = ((2 * zh + run) * 2 + y) * length
        valid = near & (offset + start - WINDOW + col >= 0)
        for g in range(group):
            first = 3 * chans + g * HEAD
            scores = lax.dot_general(
                chunk[:, first : first + HEAD], keys, (((1,), (1,)), ((), ())), preferred_element_type=f32
            ) * HEAD ** (-0.5)
            scores = jnp.where(valid, scores - slopes_ref[(core * PLANE + spot) * group + g] * far, -1e30)
            sink = sinks_ref[spot * group + g]
            top = jnp.maximum(jnp.max(scores, axis=1, keepdims=True), sink)
            expo = jnp.exp(scores - top)
            total = jnp.sum(expo, axis=1, keepdims=True) + jnp.exp(sink - top)
            probs = (expo / total).astype(bf16)
            pieces.append(jnp.dot(probs, values, preferred_element_type=f32).astype(bf16))
        place = pl.ds(pl.multiple_of((2 * run + blk // 2) * WINDOW, WINDOW), WINDOW)
        hid[lax.rem(blk, 2), place, :] = jnp.concatenate(pieces, axis=1)

    def inner_block(i, carry):
        mix(i // 3, 1 + lax.rem(i, 3))
        return carry

    def first_block(i, carry):
        mix(i, 0)
        return carry

    lax.fori_loop(0, 3, inner_block, 0)
    outs.on_z(1, 1)
    if layers > 2:
        outs.on_z(2, 0)
    lax.fori_loop(3, 6, inner_block, 0)
    if layers > 2:
        outs.on_z(2, 1)

    def tails_in(after, target):
        for k, (ref, size) in enumerate(((ext, WINDOW), (gext, front))):
            remote(
                ref.at[after, pl.ds(length, size)], ref.at[after, pl.ds(0, size)],
                hs.at[2 * after + k], hr.at[2 * after + k], target,
            ).wait_recv()

    @pl.when(y == 1)
    def _():
        tails_in(0, at.ypeer)

    @pl.when(at.has_prior)
    def _():
        tails_in(0, at.prior)

    tails_in(1, at.ypeer)
    lax.fori_loop(0, 2, first_block, 0)
    for d in range(3, layers):
        outs.on_z(d, 0)
        outs.on_z(d, 1)

    lower = z < layers // 2
    cols = obuf.shape[2] * obuf.shape[3] * obuf.shape[4]

    def chunk_at(i):
        return jnp.where(lower, i, layers - 1 - i)

    def product(side, i):
        return lax.dot_general(
            hid[side], obuf[zl, chunk_at(i)].reshape(cols, hid.shape[2]),
            (((1,), (1,)), ((), ())), preferred_element_type=f32,
        )

    def slab(p):
        return pl.ds(pl.multiple_of(p * WINDOW, WINDOW), WINDOW)

    def swap(i):
        return remote(dsend.at[i], drecv.at[i], ds.at[i], dr.at[i], at.partner)

    def first_hop(i, j):
        if i % 2 == 0:
            target, p = at.xpeer, (2 * (1 - zl) if j == 0 else 2 * zl) + 1 - x
        else:
            target, p = at.zpeer, 2 * (1 - zl) + ((1 - x) if j == 0 else x)
        return remote(s1.at[i, slab(p)], r1.at[i, j], fs.at[2 * i + j], fr.at[2 * i + j], target)

    def second_hop(i):
        return remote(s2.at[i], r2.at[i], gs.at[i], gr.at[i], at.zpeer if i % 2 == 0 else at.xpeer)

    def begin(i):
        dsend[i] = product(1 - core, i).astype(bf16)
        own[i % 2] = product(core, i)
        swap(i).start()

    def fold(i):
        swap(i).wait_recv()
        s1[i] = (own[i % 2] + drecv[i].astype(f32)).astype(bf16)
        first_hop(i, 0).start()
        first_hop(i, 1).start()

    def relay(i):
        first_hop(i, 0).wait_recv()
        p = p_z if i % 2 == 0 else p_x
        s2[i] = (s1[i, slab(p), :].astype(f32) + r1[i, 0].astype(f32)).astype(bf16)
        second_hop(i).start()

    def collect(i):
        first_hop(i, 1).wait_recv()
        second_hop(i).wait_recv()
        total = s1[i, slab(p_own), :].astype(f32) + r1[i, 1].astype(f32) + r2[i].astype(f32)
        out_ref[:, pl.ds(pl.multiple_of(chunk_at(i) * cols, cols), cols)] = total.astype(out_ref.dtype)

    ready = -1
    for i in range(layers):
        need = max(i, layers // 2 - 1 - i)
        while ready < need:
            ready += 1
            outs.on_y(ready)
        begin(i)
        if i > 0:
            fold(i - 1)
    fold(layers - 1)
    for i in range(layers):
        relay(i)
    for i in range(layers):
        collect(i)

    ins.finish()
    outs.finish()
    all_tails("wait_send")
    for copy in [tok_x, tok_z, tok_far] + swaps:
        copy.wait_send()
    for i in range(layers):
        swap(i).wait_send()
        first_hop(i, 0).wait_send()
        first_hop(i, 1).wait_send()
        second_hop(i).wait_send()


def whole_layer(count, tokens, wblocks, oblocks, gain, taps, slopes, sinks, wide):
    layers = count // PLANE
    rows, half = tokens.shape
    _, depth, width = wblocks.shape
    _, cols, inner = oblocks.shape
    chans = taps.shape[1] // PLANE
    bf16, f32 = jnp.bfloat16, jnp.float32
    dma = pltpu.SemaphoreType.DMA
    split = 2
    length = 2 * rows
    slab = 4 * cols

    def sems(parts):
        hops = 2 * (layers - 1) * 4 * parts
        return [dma((hops,))] * 2 + [dma(((2 * layers - 1) * 2 * parts,))] * 2 + [dma((2 * parts,))] * 2

    smem = pl.BlockSpec(memory_space=pltpu.SMEM)
    vmem = pl.BlockSpec(memory_space=pltpu.VMEM)
    return pl.pallas_call(
        functools.partial(layer_kernel, count, chans, wide, split),
        out_shape=jax.ShapeDtypeStruct((rows // 2, 2 * half), bf16),
        in_specs=[smem] * 2 + [vmem] * 5,
        out_specs=vmem,
        scratch_shapes=[
            pltpu.VMEM((2, PLANE * rows, half), bf16),
            pltpu.VMEM((layers, PLANE * rows, 2 * half // layers), bf16),
            pltpu.VMEM((2, layers, 2, 2, depth, width), bf16),
            pltpu.VMEM((2, layers, 2, 2, cols, inner), bf16),
            pltpu.VMEM((PLANE * rows, width), f32),
            pltpu.VMEM((2, WINDOW + length, 2 * HEAD), bf16),
            pltpu.VMEM((2, 8 + length, chans), f32),
            pltpu.VMEM((2, PLANE * WINDOW, inner), bf16),
            pltpu.VMEM((layers, PLANE * WINDOW, slab), bf16),
            pltpu.VMEM((layers, PLANE * WINDOW, slab), bf16),
            pltpu.VMEM((2, PLANE * WINDOW, slab), f32),
            pltpu.VMEM((layers, PLANE * WINDOW, slab), bf16),
            pltpu.VMEM((layers, 2, WINDOW, slab), bf16),
            pltpu.VMEM((layers, WINDOW, slab), bf16),
            pltpu.VMEM((layers, WINDOW, slab), bf16),
        ]
        + sems(split)
        + sems(1)
        + [dma((7,))] * 2
        + [dma((4,))] * 2
        + [dma((layers,))] * 2
        + [dma((2 * layers,))] * 2
        + [dma((layers,))] * 2,
        compiler_params=pltpu.CompilerParams(
            collective_id=0, has_side_effects=True, vmem_limit_bytes=60 << 20
        ),
    )(slopes, sinks, tokens, wblocks, oblocks, gain, taps)


def pack_kernel(*refs):
    *weights, out_ref = refs
    for p in range(PLANE):
        pieces = []
        for ref in weights:
            width = ref.shape[1] // PLANE
            pieces.append(ref[:, p * width : (p + 1) * width])
        out_ref[p] = jnp.concatenate(pieces, axis=1)


def pack(weights):
    depth = weights[0].shape[0]
    cols = sum(w.shape[1] for w in weights) // PLANE
    return pl.pallas_call(
        pack_kernel,
        out_shape=jax.ShapeDtypeStruct((PLANE, depth, cols), weights[0].dtype),
        in_specs=[pl.BlockSpec(memory_space=pltpu.VMEM)] * len(weights),
        out_specs=pl.BlockSpec(memory_space=pltpu.VMEM),
    )(*weights)


def plane_body(
    tokens,
    norm_gain,
    outer_gate_w,
    inner_gate_w,
    signal_w,
    conv_taps,
    query_w,
    key_w,
    value_w,
    sink_logits,
    out_conv_w,
    out_attn_w,
):
    if tokens.shape[0] != 2 * WINDOW:
        return body(
            tokens, norm_gain, outer_gate_w, inner_gate_w, signal_w, conv_taps,
            query_w, key_w, value_w, sink_logits, out_conv_w, out_attn_w,
        )
    count = lax.axis_size("sp")
    chans = outer_gate_w.shape[1] // PLANE
    wide = query_w.shape[1] // PLANE
    wblocks = pack((outer_gate_w, inner_gate_w, signal_w, query_w, key_w, value_w))
    cols = out_conv_w.shape[1]
    oblocks = jnp.concatenate(
        [out_conv_w.reshape(PLANE, chans, cols), out_attn_w.reshape(PLANE, wide, cols)], axis=1
    ).transpose(0, 2, 1)
    slopes = jnp.array([2.0 ** (-8.0 * h / QHEADS) for h in range(1, QHEADS + 1)], jnp.float32)
    return whole_layer(
        count, tokens, wblocks, oblocks, norm_gain.reshape(1, -1), conv_taps, slopes, sink_logits, wide
    )


def solution(mesh):
    kv_local = KVHEADS // mesh.shape["tp"]
    fits = mesh.shape["tp"] == 2 and kv_local == PLANE and mesh.shape["sp"] % (2 * PLANE) == 0
    chosen = plane_body if fits else body
    in_specs = (
        P("sp", "tp"),
        P(),
        P("sp", "tp"),
        P("sp", "tp"),
        P("sp", "tp"),
        P(None, "tp"),
        P("sp", "tp"),
        P("sp", "tp"),
        P("sp", "tp"),
        P("tp"),
        P("tp", "sp"),
        P("tp", "sp"),
    )
    out_specs = P(("sp", "tp"), None)
    return jax.shard_map(chosen, mesh=mesh, in_specs=in_specs, out_specs=out_specs, check_vma=False)
```

```python
import functools

import jax
import jax.numpy as jnp
from jax import lax
from jax.experimental import pallas as pl
from jax.experimental.pallas import tpu as pltpu
from jax.sharding import PartitionSpec as P

QHEADS = 24
KVHEADS = 8
HEAD = 64
TAPS = 3
WINDOW = 128
PLANE = 4
LAYERS = 4
PAIR, APART, BOTH = 1, 2, 3
FAR, NEAR = (0,), (1,)
MESH = pl.DeviceIdType.MESH


def from_behind(value, axis, steps):
    count = lax.axis_size(axis)
    initial, last = (max(0, -steps), min(count, count - steps))
    return lax.ppermute(value, axis, [(source, source + steps) for source in range(initial, last)])


def add_products(pieces, normed):
    return tuple((jnp.dot(normed, piece, preferred_element_type=jnp.float32) for piece in pieces))


def convolve(gated, before, outer, conv_taps):
    extended = jnp.concatenate([before, gated], axis=0).astype(jnp.float32)
    length = gated.shape[0]
    conv = sum((conv_taps[k] * extended[k : k + length] for k in range(conv_taps.shape[0])))
    return (outer.astype(jnp.float32) * conv).astype(jnp.bfloat16)


def attention(queries, keys_ext, values_ext, sink_logits, offset):
    f32 = jnp.float32
    length = queries.shape[0]
    kv_local = keys_ext.shape[1] // HEAD
    group = QHEADS // KVHEADS
    heads_local = kv_local * group
    span = min(512, length)
    first = lax.axis_index("tp") * heads_local + 1
    slopes = jnp.exp2(
        -8.0 * (first + jnp.arange(heads_local, dtype=jnp.int32)).astype(f32) / QHEADS
    ).reshape(kv_local, group)
    sinks = sink_logits.reshape(kv_local, group)[:, :, None]

    def attend(block):
        start = block * span
        qblock = queries.reshape(span, kv_local, group, HEAD)
        kblock = keys_ext.reshape(span + WINDOW, kv_local, HEAD)
        vblock = values_ext.reshape(span + WINDOW, kv_local, HEAD)
        scores = jnp.einsum(
            "qhgd,shd->hgqs", qblock, kblock, preferred_element_type=f32
        ) * HEAD ** (-0.5)
        qpos = offset + start + jnp.arange(span, dtype=jnp.int32)
        kpos = offset + start - WINDOW + jnp.arange(span + WINDOW, dtype=jnp.int32)
        dist = qpos[:, None] - kpos[None, :]
        valid = (dist >= 0) & (dist < WINDOW) & (kpos >= 0)[None, :]
        scores = scores - slopes[:, :, None, None] * dist.astype(f32)
        scores = jnp.where(valid, scores, -1e30)
        top = jnp.maximum(jnp.max(scores, axis=-1), sinks)
        expo = jnp.exp(scores - top[..., None])
        total = jnp.sum(expo, axis=-1) + jnp.exp(sinks - top)
        probs = (expo / total[..., None]).astype(jnp.bfloat16)
        out = jnp.einsum("hgqs,shd->qhgd", probs, vblock, preferred_element_type=f32)
        return out.reshape(span, heads_local * HEAD)

    blocks = lax.map(attend, jnp.arange(length // span, dtype=jnp.int32))
    return blocks.reshape(length, heads_local * HEAD).astype(jnp.bfloat16)


def body(
    tokens,
    norm_gain,
    outer_gate_w,
    inner_gate_w,
    signal_w,
    conv_taps,
    query_w,
    key_w,
    value_w,
    sink_logits,
    out_conv_w,
    out_attn_w,
):
    f32 = jnp.float32
    bf16 = jnp.bfloat16
    whole = lax.all_gather(tokens, "tp", axis=1, tiled=True)
    x32 = whole.astype(f32)
    normed = (
        x32 * lax.rsqrt(jnp.mean(x32 * x32, axis=-1, keepdims=True) + 1e-06) * norm_gain
    ).astype(bf16)
    length = normed.shape[0]
    offset = lax.axis_index("sp") * length

    def fold_rows(pieces):
        return add_products(pieces, normed)

    conv_weights = (outer_gate_w, inner_gate_w, signal_w)
    conv_results = fold_rows(
        (
            lax.all_gather(conv_weights[0], "sp", axis=0, tiled=True),
            lax.all_gather(conv_weights[1], "sp", axis=0, tiled=True),
            lax.all_gather(conv_weights[2], "sp", axis=0, tiled=True),
        )
    )
    outer, inner, signal = tuple((result.astype(bf16) for result in conv_results))
    gated = (inner.astype(f32) * signal.astype(f32)).astype(bf16)
    before = from_behind(gated[length - TAPS + 1 :], "sp", 1)
    conv_out = convolve(gated, before, outer, conv_taps)
    attn_weights = (query_w, key_w, value_w)
    attn_results = fold_rows(
        (
            lax.all_gather(attn_weights[0], "sp", axis=0, tiled=True),
            lax.all_gather(attn_weights[1], "sp", axis=0, tiled=True),
            lax.all_gather(attn_weights[2], "sp", axis=0, tiled=True),
        )
    )
    queries, keys, values = tuple((result.astype(bf16) for result in attn_results))
    keys_before, values_before = from_behind(
        (keys[length - WINDOW :], values[length - WINDOW :]), "sp", 1
    )
    keys_ext = jnp.concatenate([keys_before, keys], axis=0)
    values_ext = jnp.concatenate([values_before, values], axis=0)
    attn_out = attention(queries, keys_ext, values_ext, sink_logits, offset)
    conv_whole, attn_whole = (
        lax.all_gather(out_conv_w, "sp", axis=1, tiled=True),
        lax.all_gather(out_attn_w, "sp", axis=1, tiled=True),
    )
    result = jnp.dot(conv_out, conv_whole, preferred_element_type=f32)
    mixed = lax.psum_scatter(
        (result + jnp.dot(attn_out, attn_whole, preferred_element_type=f32)).astype(jnp.bfloat16),
        "tp",
        scatter_dimension=0,
        tiled=True,
    ).astype(jnp.float32)
    return mixed.astype(bf16)

class Stream:
    def __init__(self, at, src, buf, sems, split):
        self.at, self.src, self.buf, self.split = at, src, buf, split
        self.zs, self.zr, self.ys, self.yr, self.xs, self.xr = sems
        self.rows = src.shape[1] // split

    def part(self, s):
        return pl.ds(s * self.rows, self.rows)

    def slot(self, t, origin, y, x, s):
        return self.buf.at[t, origin, y, x, self.part(s)]

    def origin(self, up, d):
        return self.at.z - d if up else self.at.z + d

    def column(self, r):
        return self.at.x if r == 0 else 1 - self.at.x

    def z_copy(self, up, d, r, t, s, send_d):
        at = self.at
        dst = self.slot(t, self.origin(up, d), at.y, self.column(r), s)
        src = self.src.at[2 * t + at.x, self.part(s)] if d == 0 and r == 0 else dst
        i = ((((0 if up else 1) * (at.layers - 1) + send_d) * 2 + r) * 2 + t) * self.split + s
        return remote(src, dst, self.zs.at[i], self.zr.at[i], at.above if up else at.below)

    def z_send(self, up, d, r, t, s, action="start", only=True):
        z, layers = self.at.z, self.at.layers
        if d >= layers - 1:
            return
        if up:
            go = (z >= d) & (z + (1 if t else 2) < layers)
        else:
            go = (z + d < layers) & (z >= (2 if t else 1))

        @pl.when(go & only)
        def _():
            getattr(self.z_copy(up, d, r, t, s, d), action)()

    def y_copy(self, up, d, r, s, y):
        at = self.at
        dst = self.slot(at.zl, self.origin(up, d), y, self.column(r), s)
        src = self.src.at[2 * at.zl + at.x, self.part(s)] if d == 0 and r == 0 else dst
        m = d if up or d == 0 else at.layers - 1 + d
        i = (m * 2 + r) * self.split + s
        return remote(src, dst, self.ys.at[i], self.yr.at[i], at.ypeer)

    def x_copy(self, t, s, receive=False):
        at = self.at
        src = self.src.at[2 * t + 1 - at.x, self.part(s)]
        dst = self.slot(t, at.z, at.y, 1 - at.x if receive else at.x, s)
        i = t * self.split + s
        return remote(src, dst, self.xs.at[i], self.xr.at[i], at.xpeer)

    def send_z(self, r, s, which=FAR + NEAR, only=True):
        for k in which:
            self.z_send(True, 0, r, 1 - k, s, only=only)
            self.z_send(False, 0, r, k, s, only=only)

    def start_x(self):
        for s in range(self.split):
            for t in range(2):
                self.x_copy(t, s).start()

    def wait_x(self, s):
        for t in range(2):
            self.x_copy(t, s, True).wait_recv()

    def send_y(self, r, s, only=True):
        @pl.when(only)
        def _():
            self.y_copy(True, 0, r, s, self.at.y).start()

    def on_z(self, d, r, s, which=FAR + NEAR, sides=BOTH, only=True):
        z, layers, zl = self.at.z, self.at.layers, self.at.zl

        def arrive(up, t):
            if up:
                here = (z >= d) if t else (z >= d) & (z + 1 < layers)
            else:
                here = (z + d < layers) & (z >= 1) if t else (z + d < layers)
            if sides == PAIR:
                here = here & (zl == (1 if up else 0))
            elif sides == APART:
                here = here & (zl == (0 if up else 1))

            @pl.when(here & only)
            def _():
                self.z_copy(up, d, r, t, s, d - 1).wait_recv()
                self.z_send(up, d, r, t, s)

                @pl.when(zl == t)
                def _():
                    self.y_copy(up, d, r, s, self.at.y).start()

        for k in which:
            arrive(True, 1 - k)
            arrive(False, k)

    def on_y(self, d, action="wait_recv", sides=BOTH):
        z, layers, y, zl = self.at.z, self.at.layers, self.at.y, self.at.zl
        side = 1 - y if action == "wait_recv" else y

        def each(up):
            for r in range(2):
                for s in range(self.split):
                    getattr(self.y_copy(up, d, r, s, side), action)()

        if d == 0:
            each(True)
            return

        from_below, from_above = z >= d, z + d < layers
        if sides != BOTH:
            near = 1 if sides == PAIR else 0
            from_below, from_above = from_below & (zl == near), from_above & (zl == 1 - near)

        @pl.when(from_below)
        def _():
            each(True)

        @pl.when(from_above)
        def _():
            each(False)

    def finish(self):
        for s in range(self.split):
            for t in range(2):
                self.x_copy(t, s).wait_send()
        for d in range(self.at.layers):
            self.on_y(d, "wait_send")
            for r in range(2):
                for t in range(2):
                    for s in range(self.split):
                        self.z_send(True, d, r, t, s, "wait_send")
                        self.z_send(False, d, r, t, s, "wait_send")


def join(weights, out_ref):
    for p in range(PLANE):
        pieces = []
        for ref in weights:
            width = ref.shape[1] // PLANE
            pieces.append(ref[:, p * width : (p + 1) * width])
        out_ref[p] = jnp.concatenate(pieces, axis=1)


class Place:
    def __init__(self, count):
        me, core = lax.axis_index("sp"), lax.axis_index("tp")
        self.me, self.core, self.layers = me, core, count // PLANE
        self.z, self.y, self.x = me // PLANE, lax.rem(me // 2, 2), lax.rem(me, 2)
        self.zl, self.zh = lax.rem(self.z, 2), self.z // 2
        self.spot = 2 * self.zl + self.x

        def device(sp, tp=core):
            return {"sp": sp, "tp": tp}

        self.partner = device(me, 1 - core)
        self.xpeer = device(me + 1 - 2 * self.x)
        self.ypeer = device(me + 2 - 4 * self.y)
        self.zpeer = device(me + PLANE * (1 - 2 * self.zl))
        self.above, self.below = device(me + PLANE), device(me - PLANE)
        self.after, self.prior = device(me + PLANE + 2), device(me - PLANE - 2)
        self.has_after = (self.y == 1) & (self.zh + 1 < self.layers // 2)
        self.has_prior = (self.y == 0) & (self.zh > 0)

    def greet(self):
        barrier = pltpu.get_barrier_semaphore()

        def signal(target):
            pl.semaphore_signal(barrier, inc=1, device_id=target, device_id_type=MESH)

        for target in (self.partner, self.xpeer, self.ypeer):
            signal(target)
        number = 3
        for go, target in (
            (self.z + 1 < self.layers, self.above),
            (self.z > 0, self.below),
            (self.has_after, self.after),
            (self.has_prior, self.prior),
        ):
            pl.when(go)(functools.partial(signal, target))
            number = number + jnp.where(go, 1, 0)
        return lambda: pl.semaphore_wait(barrier, number)


def remote(src, dst, send_sem, recv_sem, target):
    return pltpu.make_async_remote_copy(
        src_ref=src, dst_ref=dst, send_sem=send_sem, recv_sem=recv_sem, device_id=target, device_id_type=MESH
    )


def layer_entry(
    count, chans, wide, split, slopes_ref, sinks_ref, tok_hbm, *refs,
):
    raw_hbm, (gain_hbm, taps_hbm, out_ref), refs = refs[:8], refs[8:11], refs[11:]
    raw, refs = refs[:8], refs[8:]
    layer_kernel(count, chans, wide, split, slopes_ref, sinks_ref, tok_hbm, raw_hbm, gain_hbm, taps_hbm, out_ref, raw, *refs)


def layer_kernel(
    count, chans, wide, split, slopes_ref, sinks_ref, tok_hbm, raw_hbm, gain_hbm, taps_hbm, out_ref, raw,
    gain_ref, taps_ref, w_ref, o_ref, ls, x_ref, nrm_ref, wbuf, obuf, acc_ref, ext, gext, hid, dsend, drecv, own, s1, r1, s2, r2,
    wzs, wzr, wys, wyr, wxs, wxr, ozs, ozr, oys, oyr, oxs, oxr, ts, tr, hs, hr, ds, dr, fs, fr, gs, gr,
):
    f32, bf16 = jnp.float32, jnp.bfloat16
    at = Place(count)
    core, layers, x, y, z, zl, zh, spot = at.core, at.layers, at.x, at.y, at.z, at.zl, at.zh, at.spot
    rows, half = tok_hbm.shape
    length = 2 * rows
    group = wide // HEAD
    front = 8
    ins = Stream(at, w_ref, wbuf, (wzs, wzr, wys, wyr, wxs, wxr), split)
    outs = Stream(at, o_ref, obuf, (ozs, ozr, oys, oyr, oxs, oxr), 1)
    arrived = at.greet()

    def block(p, side=None):
        return x_ref.at[core if side is None else side, pl.ds(pl.multiple_of(p * rows, rows), rows)]

    p_own, p_x, p_z, p_far = spot, 2 * zl + 1 - x, 2 * (1 - zl) + x, 2 * (1 - zl) + 1 - x
    loads = [
        pltpu.make_async_copy(src, dst, ls.at[k])
        for k, (src, dst) in enumerate(
            list(zip(raw_hbm[:6], raw[:6]))
            + [(tok_hbm, block(p_own))]
            + list(zip(raw_hbm[6:], raw[6:]))
            + [(gain_hbm, gain_ref), (taps_hbm, taps_ref)]
        )
    ]
    for load in loads:
        load.start()
    for load in loads[:6]:
        load.wait()
    join(raw[:6], w_ref)
    loads[6].wait()
    arrived()
    at_end = (z == 0) | (z == layers - 1)
    inside = jnp.logical_not(at_end)
    ins.send_z(0, 0, FAR)
    ins.start_x()
    ins.send_y(0, 0)
    ins.send_y(0, 1)
    ins.send_z(0, 1, FAR)
    ins.send_z(0, 0, NEAR)
    ins.send_z(0, 1, NEAR, at_end)
    def half_block(p, n):
        return x_ref.at[core, pl.ds(pl.multiple_of(p * rows + n * (rows // 2), rows // 2), rows // 2)]

    def tok_z(n, p=p_own):
        return remote(half_block(p, n), half_block(p, n), ts.at[1 + n], tr.at[1 + n], at.zpeer)

    def tok_far(n, p=p_z):
        return remote(half_block(p, n), half_block(p, n), ts.at[3 + n], tr.at[3 + n], at.xpeer)

    def send_tok_z(n, only):
        @pl.when(only)
        def _():
            tok_z(n).start()

    tok_x = remote(block(p_own), block(p_own), ts.at[0], tr.at[0], at.xpeer)
    swaps = [
        remote(block(p), block(p), ts.at[5 + k], tr.at[5 + k], at.partner)
        for k, p in enumerate((p_own, p_x, p_z, p_far))
    ]
    tok_x.start()
    send_tok_z(0, at_end)
    swaps[0].start()
    wbuf[zl, z, y, x] = w_ref[2 * zl + x]
    for load in loads[7:]:
        load.wait()
    join(raw[6:], o_ref)
    obuf[zl, z, y, x] = o_ref[2 * zl + x]
    span = 2 * half // layers
    strip = 32

    def normalise(k, p):
        remote(block(p, core), block(p, 1 - core), ts.at[5 + k], tr.at[5 + k], at.partner).wait_recv()

        def step(i, carry):
            at_rows = pl.ds(pl.multiple_of(p * rows + i * strip, strip), strip)
            whole = jnp.concatenate([x_ref[0, at_rows, :], x_ref[1, at_rows, :]], axis=1).astype(f32)
            mean = jnp.sum(whole * whole, axis=1, keepdims=True) / (2 * half)
            scaled = (whole * lax.rsqrt(mean + 1e-06) * gain_ref[...]).astype(bf16)
            for j in range(layers):
                nrm_ref[j, at_rows, :] = scaled[:, j * span : (j + 1) * span]
            return carry

        lax.fori_loop(0, rows // strip, step, 0)

    def add_layer(origin, fresh):
        def step(i, carry):
            at_rows = pl.ds(pl.multiple_of(i * rows, rows), rows)
            product = jnp.dot(
                nrm_ref[origin, at_rows, :],
                wbuf[zl, origin].reshape(span, wbuf.shape[5]),
                preferred_element_type=f32,
            )
            acc_ref[at_rows, :] = product if fresh else acc_ref[at_rows, :] + product
            return carry

        lax.fori_loop(0, PLANE, step, 0)

    def add_both(d):
        ins.on_y(d)

        @pl.when(z >= d)
        def _():
            add_layer(z - d, False)

        @pl.when(z + d < layers)
        def _():
            add_layer(z + d, False)

    def from_x(s):
        ins.wait_x(s)
        ins.send_z(1, s, FAR)
        ins.send_z(1, s, NEAR, at_end)
        ins.send_y(1, s)
        ins.on_z(1, 0, s, FAR)

    from_x(0)
    send_tok_z(0, inside)
    send_tok_z(1, at_end)
    ins.on_z(1, 0, 0, NEAR, APART)
    from_x(1)
    send_tok_z(1, inside)
    ins.send_z(0, 1, NEAR, inside)
    for s in range(split):
        ins.send_z(1, s, NEAR, inside)
    normalise(0, p_own)
    ins.on_z(1, 1, 0, FAR, PAIR, at_end)
    ins.on_z(2, 0, 0, FAR, only=at_end)
    ins.on_z(1, 1, 0, FAR, APART)
    ins.on_z(2, 0, 0, FAR, only=inside)
    ins.on_z(1, 1, 1, FAR, APART)
    tok_z(0, p_z).wait_recv()
    tok_far(0).start()
    ins.on_z(2, 0, 1, FAR, only=inside)
    ins.on_z(1, 1, 1, FAR, PAIR, at_end)
    ins.on_z(1, 0, 1, NEAR, APART)
    ins.on_z(1, 1, 0, FAR, PAIR, inside)
    for s in range(split):
        ins.on_z(1, 0, s, NEAR, PAIR)
    remote(block(p_x), block(p_x), ts.at[0], tr.at[0], at.xpeer).wait_recv()
    swaps[1].start()
    ins.on_z(2, 0, 1, FAR, only=at_end)
    ins.on_z(1, 1, 0, NEAR, APART)
    normalise(1, p_x)
    ins.on_z(1, 1, 1, NEAR, APART)
    tok_z(1, p_z).wait_recv()
    tok_far(1).start()
    swaps[2].start()
    outs.start_x()
    ins.on_z(2, 1, 0, FAR, only=inside)
    ins.on_z(2, 1, 0, FAR, only=at_end)
    normalise(2, p_z)
    ins.on_z(2, 0, 0, NEAR, only=inside)
    ins.on_z(1, 1, 1, FAR, PAIR, inside)
    for s in range(split):
        ins.on_z(1, 1, s, NEAR, PAIR)
    ins.on_z(3, 0, 0)
    outs.send_z(0, 0, only=at_end)
    ins.on_z(2, 0, 1, NEAR, only=inside)
    tok_far(0, p_far).wait_recv()
    tok_far(1, p_far).wait_recv()
    swaps[3].start()
    ins.on_z(2, 1, 1, FAR)
    ins.on_z(3, 0, 1)
    normalise(3, p_far)
    ins.on_z(2, 1, 0, NEAR, only=inside)
    ins.on_z(3, 1, 0)
    ins.on_y(0)
    add_layer(z, True)
    ins.on_z(2, 1, 1, NEAR, only=inside)
    outs.wait_x(0)
    outs.on_z(1, 0, 0, FAR, PAIR, inside)
    outs.send_z(0, 0, FAR, inside)
    outs.send_z(1, 0, FAR)
    outs.send_z(1, 0, NEAR, at_end)
    outs.send_y(0, 0, inside)
    outs.send_y(1, 0, inside)
    ins.on_z(3, 1, 1)
    add_both(1)
    outs.send_y(0, 0, at_end)
    outs.send_y(1, 0, at_end)
    outs.on_z(1, 1, 0, FAR, PAIR, inside)
    outs.on_z(2, 0, 0, FAR, only=inside)
    add_both(2)
    outs.on_z(1, 0, 0, FAR, APART)
    add_both(3)

    def spread(i, carry):
        run, start = i // 4, pl.multiple_of(lax.rem(i, 4) * WINDOW, WINDOW)
        chunk = acc_ref[pl.ds(pl.multiple_of(i * WINDOW, WINDOW), WINDOW), :].astype(bf16)
        ext[run, pl.ds(start + WINDOW, WINDOW), :] = chunk[:, 3 * chans + wide :]
        product = chunk[:, chans : 2 * chans].astype(f32) * chunk[:, 2 * chans : 3 * chans].astype(f32)
        gext[run, pl.ds(start + front, WINDOW), :] = product.astype(bf16).astype(f32)
        return carry

    lax.fori_loop(0, 2 * length // WINDOW, spread, 0)

    def tails(run, after, target, action):
        kv = remote(
            ext.at[run, pl.ds(length, WINDOW)], ext.at[after, pl.ds(0, WINDOW)],
            hs.at[2 * run], hr.at[2 * after], target,
        )
        gated = remote(
            gext.at[run, pl.ds(length, front)], gext.at[after, pl.ds(0, front)],
            hs.at[2 * run + 1], hr.at[2 * after + 1], target,
        )
        for copy in (kv, gated):
            getattr(copy, action)()

    def all_tails(action):
        @pl.when(y == 0)
        def _():
            for run in range(2):
                tails(run, run, at.ypeer, action)

        @pl.when(y == 1)
        def _():
            tails(0, 1, at.ypeer, action)

        @pl.when(at.has_after)
        def _():
            tails(1, 0, at.after, action)

    all_tails("start")
    for r in range(2):
        outs.on_z(1, r, 0, NEAR, PAIR)
        outs.send_z(r, 0, NEAR, inside)
    first_run = (y == 0) & (zh == 0)

    @pl.when(first_run)
    def _():
        ext[0, 0:WINDOW, :] = jnp.zeros((WINDOW, 2 * HEAD), bf16)
        gext[0, 0:front, :] = jnp.zeros((front, chans), f32)

    taps = sum(jnp.where(spot == c, taps_ref[:, c * chans : (c + 1) * chans], 0.0) for c in range(PLANE))
    row = lax.broadcasted_iota(jnp.int32, (WINDOW, 2 * WINDOW), 0)
    col = lax.broadcasted_iota(jnp.int32, (WINDOW, 2 * WINDOW), 1)
    dist = WINDOW + row - col
    near = (dist >= 0) & (dist < WINDOW)
    far = dist.astype(f32)

    def mix(run, blk):
        start = pl.multiple_of(blk * WINDOW, WINDOW)
        chunk = acc_ref[pl.ds(pl.multiple_of(run * length + start, WINDOW), WINDOW), :].astype(bf16)
        window = gext[run, pl.ds(start, WINDOW + front), :]
        conv = sum(
            taps[k : k + 1, :] * window[front - TAPS + 1 + k : front - TAPS + 1 + k + WINDOW]
            for k in range(TAPS)
        )
        pieces = [(chunk[:, :chans].astype(f32) * conv).astype(bf16)]
        kv = ext[run, pl.ds(start, 2 * WINDOW), :]
        keys, values = kv[:, :HEAD], kv[:, HEAD:]
        offset = ((2 * zh + run) * 2 + y) * length
        valid = near & (offset + start - WINDOW + col >= 0)
        for g in range(group):
            first = 3 * chans + g * HEAD
            scores = lax.dot_general(
                chunk[:, first : first + HEAD], keys, (((1,), (1,)), ((), ())), preferred_element_type=f32
            ) * HEAD ** (-0.5)
            scores = jnp.where(valid, scores - slopes_ref[(core * PLANE + spot) * group + g] * far, -1e30)
            sink = sinks_ref[spot * group + g]
            top = jnp.maximum(jnp.max(scores, axis=1, keepdims=True), sink)
            expo = jnp.exp(scores - top)
            total = jnp.sum(expo, axis=1, keepdims=True) + jnp.exp(sink - top)
            probs = (expo / total).astype(bf16)
            pieces.append(jnp.dot(probs, values, preferred_element_type=f32).astype(bf16))
        place = pl.ds(pl.multiple_of((2 * run + blk // 2) * WINDOW, WINDOW), WINDOW)
        hid[lax.rem(blk, 2), place, :] = jnp.concatenate(pieces, axis=1)

    def inner_block(i, carry):
        mix(i // 3, 1 + lax.rem(i, 3))
        return carry

    def first_block(i, carry):
        mix(i, 0)
        return carry

    for r in range(2):
        outs.on_z(1, r, 0, FAR, PAIR, at_end)
    outs.on_z(3, 0, 0)
    outs.on_z(1, 1, 0, FAR, APART)
    lax.fori_loop(0, 3, inner_block, 0)
    outs.on_z(2, 1, 0, FAR, only=inside)
    outs.on_z(2, 0, 0, FAR, only=at_end)
    lax.fori_loop(3, 6, inner_block, 0)
    outs.on_z(2, 0, 0, NEAR, only=inside)

    def tails_in(after, target):
        for k, (ref, size) in enumerate(((ext, WINDOW), (gext, front))):
            remote(
                ref.at[after, pl.ds(length, size)], ref.at[after, pl.ds(0, size)],
                hs.at[2 * after + k], hr.at[2 * after + k], target,
            ).wait_recv()

    @pl.when(y == 1)
    def _():
        tails_in(0, at.ypeer)

    @pl.when(at.has_prior)
    def _():
        tails_in(0, at.prior)

    tails_in(1, at.ypeer)
    lax.fori_loop(0, 2, first_block, 0)

    lower = z < layers // 2
    cols = obuf.shape[3] * obuf.shape[4]
    order = [(0, True), (1, True), (0, False), (1, False), (3, True), (2, True), (3, False), (2, False)]
    chunks = len(order)

    def chunk_at(h):
        i, mine = order[h]
        return jnp.where(lower, i, layers - 1 - i), y if mine else 1 - y

    def product(side, h):
        layer, row_y = chunk_at(h)
        return lax.dot_general(
            hid[side], obuf[zl, layer, row_y].reshape(cols, hid.shape[2]),
            (((1,), (1,)), ((), ())), preferred_element_type=f32,
        )

    def slab(p):
        return pl.ds(pl.multiple_of(p * WINDOW, WINDOW), WINDOW)

    def swap(i):
        return remote(dsend.at[i], drecv.at[i], ds.at[i], dr.at[i], at.partner)

    def first_hop(i, j):
        if i % 2 == 0:
            target, p = at.xpeer, (2 * (1 - zl) if j == 0 else 2 * zl) + 1 - x
        else:
            target, p = at.zpeer, 2 * (1 - zl) + ((1 - x) if j == 0 else x)
        return remote(s1.at[i, slab(p)], r1.at[i, j], fs.at[2 * i + j], fr.at[2 * i + j], target)

    def second_hop(i):
        return remote(s2.at[i], r2.at[i], gs.at[i], gr.at[i], at.zpeer if i % 2 == 0 else at.xpeer)

    def begin(i):
        dsend[i] = product(1 - core, i).astype(bf16)
        own[i % 2] = product(core, i)
        swap(i).start()

    def fold(i):
        swap(i).wait_recv()
        s1[i] = (own[i % 2] + drecv[i].astype(f32)).astype(bf16)
        first_hop(i, 0).start()
        first_hop(i, 1).start()

    def relay(i):
        first_hop(i, 0).wait_recv()
        p = p_z if i % 2 == 0 else p_x
        s2[i] = (s1[i, slab(p), :].astype(f32) + r1[i, 0].astype(f32)).astype(bf16)
        second_hop(i).start()

    def collect(i):
        first_hop(i, 1).wait_recv()
        second_hop(i).wait_recv()
        total = s1[i, slab(p_own), :].astype(f32) + r1[i, 1].astype(f32) + r2[i].astype(f32)
        layer, row_y = chunk_at(i)
        out_ref[:, pl.ds(pl.multiple_of((layer * 2 + row_y) * cols, cols), cols)] = total.astype(out_ref.dtype)

    begin(0)
    outs.on_z(1, 0, 0, NEAR, APART)
    begin(1)
    fold(0)
    outs.on_z(2, 1, 0, FAR, only=at_end)
    outs.on_y(0)
    outs.on_y(1, sides=PAIR)
    begin(2)
    fold(1)
    outs.on_z(1, 1, 0, NEAR, APART)
    begin(3)
    fold(2)
    outs.on_z(2, 1, 0, NEAR, only=inside)
    outs.on_z(3, 1, 0)
    begin(4)
    fold(3)
    relay(0)
    begin(5)
    fold(4)
    relay(1)
    outs.on_y(2)
    outs.on_y(3)
    begin(6)
    fold(5)
    outs.on_y(1, sides=APART)
    begin(7)
    fold(6)
    fold(7)
    for h in range(2, chunks):
        relay(h)
        collect(h - 2)
    for h in range(chunks - 2, chunks):
        collect(h)

    def phase_finish():
        ins.finish()
        outs.finish()
        all_tails("wait_send")
        for copy in [tok_x, tok_z(0), tok_z(1), tok_far(0), tok_far(1)] + swaps:
            copy.wait_send()
        for i in range(chunks):
            swap(i).wait_send()
            first_hop(i, 0).wait_send()
            first_hop(i, 1).wait_send()
            second_hop(i).wait_send()

    phase_finish()


def whole_layer(count, tokens, weights, gain, taps, slopes, sinks, wide):
    layers = count // PLANE
    rows, half = tokens.shape
    depth = weights[0].shape[0]
    width = sum(w.shape[1] for w in weights[:6]) // PLANE
    cols = weights[6].shape[0]
    inner = sum(w.shape[1] for w in weights[6:]) // PLANE
    chans = taps.shape[1] // PLANE
    bf16, f32 = jnp.bfloat16, jnp.float32
    dma = pltpu.SemaphoreType.DMA
    split = 2
    length = 2 * rows
    slab = 2 * cols
    chunks = 2 * layers

    def sems(parts):
        hops = 2 * (layers - 1) * 4 * parts
        return [dma((hops,))] * 2 + [dma(((2 * layers - 1) * 2 * parts,))] * 2 + [dma((2 * parts,))] * 2

    smem = pl.BlockSpec(memory_space=pltpu.SMEM)
    vmem = pl.BlockSpec(memory_space=pltpu.VMEM)
    return pl.pallas_call(
        functools.partial(layer_entry, count, chans, wide, split),
        out_shape=jax.ShapeDtypeStruct((rows // 2, 2 * half), bf16),
        in_specs=[smem] * 2 + [pl.BlockSpec(memory_space=pltpu.HBM)] * 11,
        out_specs=vmem,
        scratch_shapes=[pltpu.VMEM(w.shape, bf16) for w in weights]
        + [
            pltpu.VMEM(gain.shape, f32),
            pltpu.VMEM(taps.shape, f32),
            pltpu.VMEM((PLANE, depth, width), bf16),
            pltpu.VMEM((PLANE, cols, inner), bf16),
            dma((11,)),
            pltpu.VMEM((2, PLANE * rows, half), bf16),
            pltpu.VMEM((layers, PLANE * rows, 2 * half // layers), bf16),
            pltpu.VMEM((2, layers, 2, 2, depth, width), bf16),
            pltpu.VMEM((2, layers, 2, 2, cols, inner), bf16),
            pltpu.VMEM((PLANE * rows, width), f32),
            pltpu.VMEM((2, WINDOW + length, 2 * HEAD), bf16),
            pltpu.VMEM((2, 8 + length, chans), f32),
            pltpu.VMEM((2, PLANE * WINDOW, inner), bf16),
            pltpu.VMEM((chunks, PLANE * WINDOW, slab), bf16),
            pltpu.VMEM((chunks, PLANE * WINDOW, slab), bf16),
            pltpu.VMEM((2, PLANE * WINDOW, slab), f32),
            pltpu.VMEM((chunks, PLANE * WINDOW, slab), bf16),
            pltpu.VMEM((chunks, 2, WINDOW, slab), bf16),
            pltpu.VMEM((chunks, WINDOW, slab), bf16),
            pltpu.VMEM((chunks, WINDOW, slab), bf16),
        ]
        + sems(split)
        + sems(1)
        + [dma((9,))] * 2
        + [dma((4,))] * 2
        + [dma((chunks,))] * 2
        + [dma((2 * chunks,))] * 2
        + [dma((chunks,))] * 2,
        compiler_params=pltpu.CompilerParams(
            collective_id=0, has_side_effects=True, vmem_limit_bytes=60 << 20
        ),
    )(slopes, sinks, tokens, *weights, gain, taps)


def plane_body(
    tokens,
    norm_gain,
    outer_gate_w,
    inner_gate_w,
    signal_w,
    conv_taps,
    query_w,
    key_w,
    value_w,
    sink_logits,
    out_conv_w,
    out_attn_w,
):
    if tokens.shape[0] != 2 * WINDOW:
        return body(
            tokens, norm_gain, outer_gate_w, inner_gate_w, signal_w, conv_taps,
            query_w, key_w, value_w, sink_logits, out_conv_w, out_attn_w,
        )
    count = lax.axis_size("sp")
    wide = query_w.shape[1] // PLANE
    weights = (outer_gate_w, inner_gate_w, signal_w, query_w, key_w, value_w, out_conv_w.T, out_attn_w.T)
    slopes = jnp.array([2.0 ** (-8.0 * h / QHEADS) for h in range(1, QHEADS + 1)], jnp.float32)
    return whole_layer(
        count, tokens, weights, norm_gain.reshape(1, -1), conv_taps, slopes, sink_logits, wide
    )


def solution(mesh):
    kv_local = KVHEADS // mesh.shape["tp"]
    fits = mesh.shape["tp"] == 2 and kv_local == PLANE and mesh.shape["sp"] == LAYERS * PLANE
    chosen = plane_body if fits else body
    in_specs = (
        P("sp", "tp"),
        P(),
        P("sp", "tp"),
        P("sp", "tp"),
        P("sp", "tp"),
        P(None, "tp"),
        P("sp", "tp"),
        P("sp", "tp"),
        P("sp", "tp"),
        P("tp"),
        P("tp", "sp"),
        P("tp", "sp"),
    )
    out_specs = P(("sp", "tp"), None)
    return jax.shard_map(chosen, mesh=mesh, in_specs=in_specs, out_specs=out_specs, check_vma=False)
```

```python
import functools

import jax
import jax.numpy as jnp
from jax import lax
from jax.experimental import pallas as pl
from jax.experimental.pallas import tpu as pltpu
from jax.sharding import PartitionSpec as P

QHEADS = 24
KVHEADS = 8
HEAD = 64
TAPS = 3
WINDOW = 128
PLANE = 4
LAYERS = 4
PAIR, APART, BOTH = 1, 2, 3
FAR, NEAR = (0,), (1,)
MESH = pl.DeviceIdType.MESH


def from_behind(value, axis, steps):
    count = lax.axis_size(axis)
    initial, last = (max(0, -steps), min(count, count - steps))
    return lax.ppermute(value, axis, [(source, source + steps) for source in range(initial, last)])


def add_products(pieces, normed):
    return tuple((jnp.dot(normed, piece, preferred_element_type=jnp.float32) for piece in pieces))


def convolve(gated, before, outer, conv_taps):
    extended = jnp.concatenate([before, gated], axis=0).astype(jnp.float32)
    length = gated.shape[0]
    conv = sum((conv_taps[k] * extended[k : k + length] for k in range(conv_taps.shape[0])))
    return (outer.astype(jnp.float32) * conv).astype(jnp.bfloat16)


def attention(queries, keys_ext, values_ext, sink_logits, offset):
    f32 = jnp.float32
    length = queries.shape[0]
    kv_local = keys_ext.shape[1] // HEAD
    group = QHEADS // KVHEADS
    heads_local = kv_local * group
    span = min(512, length)
    first = lax.axis_index("tp") * heads_local + 1
    slopes = jnp.exp2(
        -8.0 * (first + jnp.arange(heads_local, dtype=jnp.int32)).astype(f32) / QHEADS
    ).reshape(kv_local, group)
    sinks = sink_logits.reshape(kv_local, group)[:, :, None]

    def attend(block):
        start = block * span
        qblock = queries.reshape(span, kv_local, group, HEAD)
        kblock = keys_ext.reshape(span + WINDOW, kv_local, HEAD)
        vblock = values_ext.reshape(span + WINDOW, kv_local, HEAD)
        scores = jnp.einsum(
            "qhgd,shd->hgqs", qblock, kblock, preferred_element_type=f32
        ) * HEAD ** (-0.5)
        qpos = offset + start + jnp.arange(span, dtype=jnp.int32)
        kpos = offset + start - WINDOW + jnp.arange(span + WINDOW, dtype=jnp.int32)
        dist = qpos[:, None] - kpos[None, :]
        valid = (dist >= 0) & (dist < WINDOW) & (kpos >= 0)[None, :]
        scores = scores - slopes[:, :, None, None] * dist.astype(f32)
        scores = jnp.where(valid, scores, -1e30)
        top = jnp.maximum(jnp.max(scores, axis=-1), sinks)
        expo = jnp.exp(scores - top[..., None])
        total = jnp.sum(expo, axis=-1) + jnp.exp(sinks - top)
        probs = (expo / total[..., None]).astype(jnp.bfloat16)
        out = jnp.einsum("hgqs,shd->qhgd", probs, vblock, preferred_element_type=f32)
        return out.reshape(span, heads_local * HEAD)

    blocks = lax.map(attend, jnp.arange(length // span, dtype=jnp.int32))
    return blocks.reshape(length, heads_local * HEAD).astype(jnp.bfloat16)


def body(
    tokens,
    norm_gain,
    outer_gate_w,
    inner_gate_w,
    signal_w,
    conv_taps,
    query_w,
    key_w,
    value_w,
    sink_logits,
    out_conv_w,
    out_attn_w,
):
    f32 = jnp.float32
    bf16 = jnp.bfloat16
    whole = lax.all_gather(tokens, "tp", axis=1, tiled=True)
    x32 = whole.astype(f32)
    normed = (
        x32 * lax.rsqrt(jnp.mean(x32 * x32, axis=-1, keepdims=True) + 1e-06) * norm_gain
    ).astype(bf16)
    length = normed.shape[0]
    offset = lax.axis_index("sp") * length

    def fold_rows(pieces):
        return add_products(pieces, normed)

    conv_weights = (outer_gate_w, inner_gate_w, signal_w)
    conv_results = fold_rows(
        (
            lax.all_gather(conv_weights[0], "sp", axis=0, tiled=True),
            lax.all_gather(conv_weights[1], "sp", axis=0, tiled=True),
            lax.all_gather(conv_weights[2], "sp", axis=0, tiled=True),
        )
    )
    outer, inner, signal = tuple((result.astype(bf16) for result in conv_results))
    gated = (inner.astype(f32) * signal.astype(f32)).astype(bf16)
    before = from_behind(gated[length - TAPS + 1 :], "sp", 1)
    conv_out = convolve(gated, before, outer, conv_taps)
    attn_weights = (query_w, key_w, value_w)
    attn_results = fold_rows(
        (
            lax.all_gather(attn_weights[0], "sp", axis=0, tiled=True),
            lax.all_gather(attn_weights[1], "sp", axis=0, tiled=True),
            lax.all_gather(attn_weights[2], "sp", axis=0, tiled=True),
        )
    )
    queries, keys, values = tuple((result.astype(bf16) for result in attn_results))
    keys_before, values_before = from_behind(
        (keys[length - WINDOW :], values[length - WINDOW :]), "sp", 1
    )
    keys_ext = jnp.concatenate([keys_before, keys], axis=0)
    values_ext = jnp.concatenate([values_before, values], axis=0)
    attn_out = attention(queries, keys_ext, values_ext, sink_logits, offset)
    conv_whole, attn_whole = (
        lax.all_gather(out_conv_w, "sp", axis=1, tiled=True),
        lax.all_gather(out_attn_w, "sp", axis=1, tiled=True),
    )
    result = jnp.dot(conv_out, conv_whole, preferred_element_type=f32)
    mixed = lax.psum_scatter(
        (result + jnp.dot(attn_out, attn_whole, preferred_element_type=f32)).astype(jnp.bfloat16),
        "tp",
        scatter_dimension=0,
        tiled=True,
    ).astype(jnp.float32)
    return mixed.astype(bf16)

class Stream:
    def __init__(self, at, src, buf, sems, split):
        self.at, self.src, self.buf, self.split = at, src, buf, split
        self.zs, self.zr, self.ys, self.yr, self.xs, self.xr = sems
        self.rows = src.shape[1] // split

    def part(self, s):
        return pl.ds(s * self.rows, self.rows)

    def slot(self, t, origin, y, x, s):
        return self.buf.at[t, origin, y, x, self.part(s)]

    def origin(self, up, d):
        return self.at.z - d if up else self.at.z + d

    def column(self, r):
        return self.at.x if r == 0 else 1 - self.at.x

    def z_copy(self, up, d, r, t, s, send_d):
        at = self.at
        dst = self.slot(t, self.origin(up, d), at.y, self.column(r), s)
        src = self.src.at[2 * t + at.x, self.part(s)] if d == 0 and r == 0 else dst
        side = 0 if up else 1
        i = (((side * (at.layers - 1) + send_d) * 2 + r) * 2 + t) * self.split + s
        return remote(src, dst, self.zs.at[2 * side + t], self.zr.at[i], at.above if up else at.below)

    def z_send(self, up, d, r, t, s, only=True):
        z, layers = self.at.z, self.at.layers
        if d >= layers - 1:
            return
        if up:
            go = (z >= d) & (z + (1 if t else 2) < layers)
        else:
            go = (z + d < layers) & (z >= (2 if t else 1))

        @pl.when(go & only)
        def _():
            self.z_copy(up, d, r, t, s, d).start()

    def y_copy(self, up, d, r, s, y):
        at = self.at
        dst = self.slot(at.zl, self.origin(up, d), y, self.column(r), s)
        src = self.src.at[2 * at.zl + at.x, self.part(s)] if d == 0 and r == 0 else dst
        m = d if up or d == 0 else at.layers - 1 + d
        return remote(src, dst, self.ys.at[0], self.yr.at[m], at.ypeer)

    def x_copy(self, t, s, receive=False):
        at = self.at
        src = self.src.at[2 * t + 1 - at.x, self.part(s)]
        dst = self.slot(t, at.z, at.y, 1 - at.x if receive else at.x, s)
        return remote(src, dst, self.xs.at[0], self.xr.at[t * self.split + s], at.xpeer)

    def send_z(self, r, s, which=FAR + NEAR, only=True):
        for k in which:
            self.z_send(True, 0, r, 1 - k, s, only=only)
            self.z_send(False, 0, r, k, s, only=only)

    def start_x(self):
        for s in range(self.split):
            for t in range(2):
                self.x_copy(t, s).start()

    def wait_x(self, s):
        for t in range(2):
            self.x_copy(t, s, True).wait_recv()

    def send_y(self, r, s, only=True):
        @pl.when(only)
        def _():
            self.y_copy(True, 0, r, s, self.at.y).start()

    def on_z(self, d, r, s, which=FAR + NEAR, sides=BOTH, only=True):
        z, layers, zl = self.at.z, self.at.layers, self.at.zl

        def arrive(up, t):
            if up:
                here = (z >= d) if t else (z >= d) & (z + 1 < layers)
            else:
                here = (z + d < layers) & (z >= 1) if t else (z + d < layers)
            if sides == PAIR:
                here = here & (zl == (1 if up else 0))
            elif sides == APART:
                here = here & (zl == (0 if up else 1))

            @pl.when(here & only)
            def _():
                self.z_copy(up, d, r, t, s, d - 1).wait_recv()
                self.z_send(up, d, r, t, s)

                @pl.when(zl == t)
                def _():
                    self.y_copy(up, d, r, s, self.at.y).start()

        for k in which:
            arrive(True, 1 - k)
            arrive(False, k)

    def on_y(self, d, sides=BOTH, up=None):
        z, layers, y, zl = self.at.z, self.at.layers, self.at.y, self.at.zl

        def each(up):
            ref = self.buf.at[zl, self.origin(up, d), 1 - y]
            m = d if up or d == 0 else layers - 1 + d
            remote(ref, ref, self.ys.at[0], self.yr.at[m], self.at.ypeer).wait_recv()

        if d == 0 or up is not None:
            each(up is not False)
            return
        from_below, from_above = z >= d, z + d < layers
        if sides != BOTH:
            near = 1 if sides == PAIR else 0
            from_below, from_above = from_below & (zl == near), from_above & (zl == 1 - near)

        @pl.when(from_below)
        def _():
            each(True)

        @pl.when(from_above)
        def _():
            each(False)

    def finish(self):
        at = self.at
        layers = at.layers

        def sent(ref, sem):
            remote(ref, ref, sem, self.yr.at[0], at.ypeer).wait_send()

        sent(self.buf.at[0, 0, 0], self.xs.at[0])
        sent(self.buf.at[0, :, 0], self.ys.at[0])
        for up in (True, False):
            for t in range(2):
                for z in range(layers):
                    beyond = layers - z if up else z + 1
                    if beyond > (1 if (t == 1) == up else 2):
                        number = z + 1 if up else layers - z

                        @pl.when(at.z == z)
                        def _():
                            sent(self.buf.at[0, pl.ds(0, number), 0], self.zs.at[(0 if up else 2) + t])


def join(weights, out_ref):
    for p in range(PLANE):
        pieces = []
        for ref in weights:
            width = ref.shape[1] // PLANE
            pieces.append(ref[:, p * width : (p + 1) * width])
        out_ref[p] = jnp.concatenate(pieces, axis=1)


class Place:
    def __init__(self, count):
        me, core = lax.axis_index("sp"), lax.axis_index("tp")
        self.me, self.core, self.layers = me, core, count // PLANE
        self.z, self.y, self.x = me // PLANE, lax.rem(me // 2, 2), lax.rem(me, 2)
        self.zl, self.zh = lax.rem(self.z, 2), self.z // 2
        self.spot = 2 * self.zl + self.x

        def device(sp, tp=core):
            return {"sp": sp, "tp": tp}

        self.partner = device(me, 1 - core)
        self.xpeer = device(me + 1 - 2 * self.x)
        self.ypeer = device(me + 2 - 4 * self.y)
        self.zpeer = device(me + PLANE * (1 - 2 * self.zl))
        self.above, self.below = device(me + PLANE), device(me - PLANE)
        self.after, self.prior = device(me + PLANE + 2), device(me - PLANE - 2)
        self.has_after = (self.y == 1) & (self.zh + 1 < self.layers // 2)
        self.has_prior = (self.y == 0) & (self.zh > 0)

    def greet(self):
        barrier = pltpu.get_barrier_semaphore()

        def signal(target):
            pl.semaphore_signal(barrier, inc=1, device_id=target, device_id_type=MESH)

        for target in (self.partner, self.xpeer, self.ypeer):
            signal(target)
        number = 3
        for go, target in (
            (self.z + 1 < self.layers, self.above),
            (self.z > 0, self.below),
            (self.has_after, self.after),
            (self.has_prior, self.prior),
        ):
            pl.when(go)(functools.partial(signal, target))
            number = number + jnp.where(go, 1, 0)
        return lambda: pl.semaphore_wait(barrier, number)


def remote(src, dst, send_sem, recv_sem, target):
    return pltpu.make_async_remote_copy(
        src_ref=src, dst_ref=dst, send_sem=send_sem, recv_sem=recv_sem, device_id=target, device_id_type=MESH
    )


def layer_entry(
    count, chans, wide, split, slopes_ref, sinks_ref, tok_hbm, *refs,
):
    raw_hbm, (gain_hbm, taps_hbm, out_hbm), refs = refs[:8], refs[8:11], refs[11:]
    raw, refs = refs[:8], refs[8:]
    layer_kernel(count, chans, wide, split, slopes_ref, sinks_ref, tok_hbm, raw_hbm, gain_hbm, taps_hbm, out_hbm, raw, *refs)


def layer_kernel(
    count, chans, wide, split, slopes_ref, sinks_ref, tok_hbm, raw_hbm, gain_hbm, taps_hbm, out_hbm, raw,
    gain_ref, taps_ref, w_ref, o_ref, out_ref, ls, os, x_ref, nrm_ref, wbuf, obuf, acc_ref, ext, gext, bias, hid, dsend, drecv, own, s1, r1, s2, r2,
    wzs, wzr, wys, wyr, wxs, wxr, ozs, ozr, oys, oyr, oxs, oxr, ts, tr, hs, hr, ds, dr, fs, fr, gs, gr,
):
    f32, bf16 = jnp.float32, jnp.bfloat16
    at = Place(count)
    core, layers, x, y, z, zl, zh, spot = at.core, at.layers, at.x, at.y, at.z, at.zl, at.zh, at.spot
    rows, half = tok_hbm.shape
    length = 2 * rows
    group = wide // HEAD
    front = 8
    ins = Stream(at, w_ref, wbuf, (wzs, wzr, wys, wyr, wxs, wxr), split)
    outs = Stream(at, o_ref, obuf, (ozs, ozr, oys, oyr, oxs, oxr), 1)
    arrived = at.greet()

    def block(p, side=None):
        return x_ref.at[core if side is None else side, pl.ds(pl.multiple_of(p * rows, rows), rows)]

    p_own, p_x, p_z, p_far = spot, 2 * zl + 1 - x, 2 * (1 - zl) + x, 2 * (1 - zl) + 1 - x
    loads = [
        pltpu.make_async_copy(src, dst, ls.at[k])
        for k, (src, dst) in enumerate(
            list(zip(raw_hbm[:6], raw[:6]))
            + [(tok_hbm, block(p_own))]
            + list(zip(raw_hbm[6:], raw[6:]))
            + [(gain_hbm, gain_ref), (taps_hbm, taps_ref)]
        )
    ]
    for load in loads:
        load.start()
    for load in loads[:6]:
        load.wait()
    join(raw[:6], w_ref)
    loads[6].wait()
    arrived()
    at_end = (z == 0) | (z == layers - 1)
    inside = jnp.logical_not(at_end)
    ins.send_z(0, 0, FAR)
    ins.start_x()
    ins.send_y(0, 0)
    ins.send_y(0, 1)
    ins.send_z(0, 1, FAR)
    ins.send_z(0, 0, NEAR)
    ins.send_z(0, 1, NEAR, at_end)
    def half_block(p, n):
        return x_ref.at[core, pl.ds(pl.multiple_of(p * rows + n * (rows // 2), rows // 2), rows // 2)]

    def tok_z(n, p=p_own):
        return remote(half_block(p, n), half_block(p, n), ts.at[0], tr.at[1 + n], at.zpeer)

    def tok_far(n, p=p_z):
        return remote(half_block(p, n), half_block(p, n), ts.at[0], tr.at[3 + n], at.xpeer)

    def send_tok_z(n, only):
        @pl.when(only)
        def _():
            tok_z(n).start()

    tok_x = remote(block(p_own), block(p_own), ts.at[0], tr.at[0], at.xpeer)
    swaps = [
        remote(block(p), block(p), ts.at[1], tr.at[5 + k], at.partner)
        for k, p in enumerate((p_own, p_x, p_z, p_far))
    ]
    tok_x.start()
    tok_z(0).start()
    swaps[0].start()
    wbuf[zl, z, y, x] = w_ref[2 * zl + x]
    for load in loads[7:]:
        load.wait()
    join(raw[6:], o_ref)
    obuf[zl, z, y, x] = o_ref[2 * zl + x]
    span = 2 * half // layers
    strip = 32

    def normalise(k, p):
        remote(block(p, core), block(p, 1 - core), ts.at[1], tr.at[5 + k], at.partner).wait_recv()

        def step(i, carry):
            at_rows = pl.ds(pl.multiple_of(p * rows + i * strip, strip), strip)
            whole = jnp.concatenate([x_ref[0, at_rows, :], x_ref[1, at_rows, :]], axis=1).astype(f32)
            mean = jnp.sum(whole * whole, axis=1, keepdims=True) / (2 * half)
            scaled = (whole * lax.rsqrt(mean + 1e-06) * gain_ref[...]).astype(bf16)
            for j in range(layers):
                nrm_ref[j, at_rows, :] = scaled[:, j * span : (j + 1) * span]
            return carry

        lax.fori_loop(0, rows // strip, step, 0)

    def add_layer(origin, fresh):
        def step(i, carry):
            at_rows = pl.ds(pl.multiple_of(i * rows, rows), rows)
            product = jnp.dot(
                nrm_ref[origin, at_rows, :],
                wbuf[zl, origin].reshape(span, wbuf.shape[5]),
                preferred_element_type=f32,
            )
            acc_ref[at_rows, :] = product if fresh else acc_ref[at_rows, :] + product
            return carry

        lax.fori_loop(0, PLANE, step, 0)

    def add_row(origin, row_y):
        size = span // 2

        def step(i, carry):
            at_rows = pl.ds(pl.multiple_of(i * rows, rows), rows)
            acc_ref[at_rows, :] += jnp.dot(
                nrm_ref[origin, at_rows, pl.ds(pl.multiple_of(row_y * size, size), size)],
                wbuf[zl, origin, row_y].reshape(size, wbuf.shape[5]),
                preferred_element_type=f32,
            )
            return carry

        lax.fori_loop(0, PLANE, step, 0)

    def add_last():
        def two(d, up):
            add_row(ins.origin(up, d), y)
            ins.on_y(d, up=up)
            add_row(ins.origin(up, d), 1 - y)

        for above in (False, True):
            for d, where in ((3, at_end), (2, inside)):
                mine = (z >= d) if above else (z + d < layers)

                @pl.when(mine & where)
                def _():
                    two(d, above)

    def add_both(d):
        ins.on_y(d)

        @pl.when(z >= d)
        def _():
            add_layer(z - d, False)

        @pl.when(z + d < layers)
        def _():
            add_layer(z + d, False)

    def from_x(s):
        ins.wait_x(s)
        ins.send_z(1, s, FAR)
        ins.send_z(1, s, NEAR, at_end)
        ins.send_y(1, s)
        ins.on_z(1, 0, s, FAR)

    from_x(0)
    send_tok_z(1, at_end)
    ins.on_z(1, 0, 0, NEAR, APART)
    from_x(1)
    send_tok_z(1, inside)
    ins.send_z(0, 1, NEAR, inside)
    for s in range(split):
        ins.send_z(1, s, NEAR, inside)
    outs.send_y(0, 0, inside)
    normalise(0, p_own)
    ins.on_z(1, 1, 0, FAR, PAIR, at_end)
    ins.on_z(2, 0, 0, FAR, only=at_end)
    ins.on_z(1, 1, 0, FAR, APART)
    ins.on_z(2, 0, 0, FAR, only=inside)
    ins.on_z(1, 1, 1, FAR, APART)
    tok_z(0, p_z).wait_recv()
    tok_far(0).start()
    ins.on_z(2, 0, 1, FAR, only=inside)
    ins.on_z(1, 1, 1, FAR, PAIR, at_end)
    ins.on_z(1, 0, 1, NEAR, APART)
    ins.on_z(1, 1, 0, FAR, PAIR, inside)
    for s in range(split):
        ins.on_z(1, 0, s, NEAR, PAIR)
    remote(block(p_x), block(p_x), ts.at[0], tr.at[0], at.xpeer).wait_recv()
    swaps[1].start()
    ins.on_z(2, 0, 1, FAR, only=at_end)
    outs.send_y(0, 0, at_end)
    ins.on_z(1, 1, 0, NEAR, APART)
    normalise(1, p_x)
    ins.on_z(1, 1, 1, NEAR, APART)
    tok_z(1, p_z).wait_recv()
    tok_far(1).start()
    swaps[2].start()
    outs.start_x()
    ins.on_z(2, 1, 0, FAR, only=inside)
    ins.on_z(2, 1, 0, FAR, only=at_end)
    normalise(2, p_z)
    ins.on_z(2, 0, 0, NEAR, only=inside)
    ins.on_z(1, 1, 1, FAR, PAIR, inside)
    for s in range(split):
        ins.on_z(1, 1, s, NEAR, PAIR)
    ins.on_z(3, 0, 0)
    outs.send_z(0, 0, only=at_end)
    ins.on_z(2, 0, 1, NEAR, only=inside)
    tok_far(0, p_far).wait_recv()
    tok_far(1, p_far).wait_recv()
    swaps[3].start()
    ins.on_z(2, 1, 1, FAR)
    ins.on_z(3, 0, 1)
    normalise(3, p_far)
    ins.on_z(2, 1, 0, NEAR, only=inside)
    ins.on_z(3, 1, 0)
    ins.on_y(0)
    add_layer(z, True)
    ins.on_z(2, 1, 1, NEAR, only=inside)
    outs.wait_x(0)
    outs.on_z(1, 0, 0, FAR, PAIR, inside)
    outs.send_z(0, 0, FAR, inside)
    outs.send_z(1, 0, FAR)
    outs.send_z(1, 0, NEAR, at_end)
    outs.send_y(1, 0, inside)
    ins.on_z(3, 1, 1)
    add_both(1)
    outs.send_y(1, 0, at_end)
    outs.on_z(1, 1, 0, FAR, PAIR, inside)
    outs.on_z(2, 0, 0, FAR, only=inside)

    @pl.when(at_end)
    def _():
        add_both(2)

    outs.on_z(1, 0, 0, FAR, APART)
    add_last()

    def spread(i, carry):
        run, start = i // 4, pl.multiple_of(lax.rem(i, 4) * WINDOW, WINDOW)
        chunk = acc_ref[pl.ds(pl.multiple_of(i * WINDOW, WINDOW), WINDOW), :].astype(bf16)
        ext[run, pl.ds(start + WINDOW, WINDOW), :] = chunk[:, 3 * chans + wide :]
        product = chunk[:, chans : 2 * chans].astype(f32) * chunk[:, 2 * chans : 3 * chans].astype(f32)
        gext[run, pl.ds(start + front, WINDOW), :] = product.astype(bf16).astype(f32)
        return carry

    lax.fori_loop(0, 2 * length // WINDOW, spread, 0)

    def tails(run, after, target, action):
        kv = remote(
            ext.at[run, pl.ds(length, WINDOW)], ext.at[after, pl.ds(0, WINDOW)],
            hs.at[2 * run], hr.at[2 * after], target,
        )
        gated = remote(
            gext.at[run, pl.ds(length, front)], gext.at[after, pl.ds(0, front)],
            hs.at[2 * run + 1], hr.at[2 * after + 1], target,
        )
        for copy in (kv, gated):
            getattr(copy, action)()

    def all_tails(action):
        @pl.when(y == 0)
        def _():
            for run in range(2):
                tails(run, run, at.ypeer, action)

        @pl.when(y == 1)
        def _():
            tails(0, 1, at.ypeer, action)

        @pl.when(at.has_after)
        def _():
            tails(1, 0, at.after, action)

    all_tails("start")
    for r in range(2):
        outs.on_z(1, r, 0, NEAR, PAIR)
        outs.send_z(r, 0, NEAR, inside)
    first_run = (y == 0) & (zh == 0)

    @pl.when(first_run)
    def _():
        ext[0, 0:WINDOW, :] = jnp.zeros((WINDOW, 2 * HEAD), bf16)
        gext[0, 0:front, :] = jnp.zeros((front, chans), f32)

    taps = sum(jnp.where(spot == c, taps_ref[:, c * chans : (c + 1) * chans], 0.0) for c in range(PLANE))
    row = lax.broadcasted_iota(jnp.int32, (WINDOW, 2 * WINDOW), 0)
    col = lax.broadcasted_iota(jnp.int32, (WINDOW, 2 * WINDOW), 1)
    dist = WINDOW + row - col
    near = (dist >= 0) & (dist < WINDOW)
    far = dist.astype(f32)

    for g in range(group):
        bias[g] = jnp.where(near, -slopes_ref[(core * PLANE + spot) * group + g] * far, -1e30)
    ones = jnp.where(lax.broadcasted_iota(jnp.int32, (2 * WINDOW, HEAD), 1) == 0, 1.0, 0.0).astype(bf16)

    def mix(run, blk, first=False):
        start = pl.multiple_of(blk * WINDOW, WINDOW)
        chunk = acc_ref[pl.ds(pl.multiple_of(run * length + start, WINDOW), WINDOW), :].astype(bf16)
        window = gext[run, pl.ds(start, WINDOW + front), :]
        conv = sum(
            taps[k : k + 1, :] * window[front - TAPS + 1 + k : front - TAPS + 1 + k + WINDOW]
            for k in range(TAPS)
        )
        pieces = [(chunk[:, :chans].astype(f32) * conv).astype(bf16)]
        kv = ext[run, pl.ds(start, 2 * WINDOW), :]
        keys, values = kv[:, :HEAD], jnp.concatenate([kv[:, HEAD:], ones], axis=1)
        offset = ((2 * zh + run) * 2 + y) * length
        for g in range(group):
            at_head = 3 * chans + g * HEAD
            query = chunk[:, at_head : at_head + HEAD] * jnp.asarray(HEAD ** (-0.5), bf16)
            scores = bias[g] + lax.dot_general(
                query, keys, (((1,), (1,)), ((), ())), preferred_element_type=f32
            )
            if first:
                scores = jnp.where(offset - WINDOW + col >= 0, scores, -1e30)
            sink = sinks_ref[spot * group + g]
            top = jnp.maximum(jnp.max(scores, axis=1, keepdims=True), sink)
            expo = jnp.exp(scores - top).astype(bf16)
            summed = jnp.dot(expo, values, preferred_element_type=f32)
            total = summed[:, HEAD : HEAD + 1] + jnp.exp(sink - top)
            pieces.append((summed[:, :HEAD] / total).astype(bf16))
        place = pl.ds(pl.multiple_of((2 * run + blk // 2) * WINDOW, WINDOW), WINDOW)
        hid[lax.rem(blk, 2), place, :] = jnp.concatenate(pieces, axis=1)

    def mix_run(run):
        for blk in range(1, 4):
            mix(run, blk)

    def mix_first():
        for run in range(2):
            mix(run, 0, True)

    for r in range(2):
        outs.on_z(1, r, 0, FAR, PAIR, at_end)
    outs.on_z(3, 0, 0)
    outs.on_z(1, 1, 0, FAR, APART)
    mix_run(0)
    outs.on_z(2, 1, 0, FAR, only=inside)
    mix_run(1)

    def tails_in(after, target):
        for k, (ref, size) in enumerate(((ext, WINDOW), (gext, front))):
            remote(
                ref.at[after, pl.ds(length, size)], ref.at[after, pl.ds(0, size)],
                hs.at[2 * after + k], hr.at[2 * after + k], target,
            ).wait_recv()

    @pl.when(y == 1)
    def _():
        tails_in(0, at.ypeer)

    @pl.when(at.has_prior)
    def _():
        tails_in(0, at.prior)

    tails_in(1, at.ypeer)
    mix_first()

    lower = z < layers // 2
    cols = obuf.shape[3] * obuf.shape[4]
    order = [(0, True), (1, True), (0, False), (1, False), (3, True), (2, True), (3, False), (2, False)]
    chunks = len(order)

    def chunk_at(h):
        i, mine = order[h]
        return jnp.where(lower, i, layers - 1 - i), y if mine else 1 - y

    def product(side, h):
        layer, row_y = chunk_at(h)
        return lax.dot_general(
            hid[side], obuf[zl, layer, row_y].reshape(cols, hid.shape[2]),
            (((1,), (1,)), ((), ())), preferred_element_type=f32,
        )

    def slab(p):
        return pl.ds(pl.multiple_of(p * WINDOW, WINDOW), WINDOW)

    def swap(i):
        return remote(dsend.at[i], drecv.at[i], ds.at[0], dr.at[i], at.partner)

    def first_hop(i, j):
        if i % 2 == 0:
            target, p = at.xpeer, (2 * (1 - zl) if j == 0 else 2 * zl) + 1 - x
        else:
            target, p = at.zpeer, 2 * (1 - zl) + ((1 - x) if j == 0 else x)
        return remote(s1.at[i, slab(p)], r1.at[i, j], fs.at[0], fr.at[2 * i + j], target)

    def second_hop(i):
        return remote(s2.at[i], r2.at[i], gs.at[0], gr.at[i], at.zpeer if i % 2 == 0 else at.xpeer)

    def begin(i):
        dsend[i] = product(1 - core, i).astype(bf16)
        own[i % 2] = product(core, i)
        swap(i).start()

    def fold(i):
        swap(i).wait_recv()
        s1[i] = (own[i % 2] + drecv[i].astype(f32)).astype(bf16)
        first_hop(i, 0).start()
        first_hop(i, 1).start()

    def relay(i):
        first_hop(i, 0).wait_recv()
        p = p_z if i % 2 == 0 else p_x
        s2[i] = (s1[i, slab(p), :].astype(f32) + r1[i, 0].astype(f32)).astype(bf16)
        second_hop(i).start()

    def out_copy(i):
        layer, row_y = chunk_at(i)
        return pltpu.make_async_copy(
            out_ref.at[i], out_hbm.at[:, pl.ds(pl.multiple_of((layer * 2 + row_y) * cols, cols), cols)], os.at[0]
        )

    def collect(i):
        first_hop(i, 1).wait_recv()
        second_hop(i).wait_recv()
        total = s1[i, slab(p_own), :].astype(f32) + r1[i, 1].astype(f32) + r2[i].astype(f32)
        out_ref[i] = total.astype(out_ref.dtype)
        out_copy(i).start()

    begin(0)
    outs.on_z(2, 0, 0, FAR, only=at_end)
    begin(1)
    fold(0)
    outs.on_z(2, 0, 0, NEAR, only=inside)
    outs.on_z(1, 0, 0, NEAR, APART)
    outs.on_z(2, 1, 0, FAR, only=at_end)
    outs.on_y(0)
    outs.on_y(1, sides=PAIR)
    begin(2)
    fold(1)
    outs.on_z(1, 1, 0, NEAR, APART)
    begin(3)
    fold(2)
    outs.on_z(2, 1, 0, NEAR, only=inside)
    outs.on_z(3, 1, 0)
    begin(4)
    fold(3)
    relay(0)
    begin(5)
    fold(4)
    relay(1)
    relay(2)
    relay(3)
    outs.on_y(2)
    outs.on_y(3)
    begin(6)
    fold(5)
    outs.on_y(1, sides=APART)
    begin(7)
    fold(6)
    relay(4)
    fold(7)
    collect(0)
    collect(1)
    relay(5)
    collect(2)
    relay(6)
    collect(3)
    relay(7)
    for h in range(4, chunks):
        collect(h)

    def phase_finish():
        pltpu.make_async_copy(out_ref, out_ref, os.at[0]).wait()
        ins.finish()
        outs.finish()
        all_tails("wait_send")
        for ref, sem in (
            (x_ref.at[0, pl.ds(0, 3 * rows)], ts.at[0]),
            (x_ref.at[0], ts.at[1]),
            (dsend, ds.at[0]),
            (s1.at[pl.ds(0, chunks // 2)], fs.at[0]),
            (s2, gs.at[0]),
        ):
            remote(ref, ref, sem, dr.at[0], at.partner).wait_send()

    phase_finish()


def whole_layer(count, tokens, weights, gain, taps, slopes, sinks, wide):
    layers = count // PLANE
    rows, half = tokens.shape
    depth = weights[0].shape[0]
    width = sum(w.shape[1] for w in weights[:6]) // PLANE
    cols = weights[6].shape[0]
    inner = sum(w.shape[1] for w in weights[6:]) // PLANE
    chans = taps.shape[1] // PLANE
    bf16, f32 = jnp.bfloat16, jnp.float32
    dma = pltpu.SemaphoreType.DMA
    split = 2
    length = 2 * rows
    slab = 2 * cols
    chunks = 2 * layers

    def sems(parts):
        hops = 2 * (layers - 1) * 4 * parts
        return [dma((number,)) for number in (4, hops, 1, 2 * layers - 1, 1, 2 * parts)]

    smem = pl.BlockSpec(memory_space=pltpu.SMEM)
    return pl.pallas_call(
        functools.partial(layer_entry, count, chans, wide, split),
        out_shape=jax.ShapeDtypeStruct((rows // 2, 2 * half), bf16),
        in_specs=[smem] * 2 + [pl.BlockSpec(memory_space=pltpu.HBM)] * 11,
        out_specs=pl.BlockSpec(memory_space=pltpu.HBM),
        scratch_shapes=[pltpu.VMEM(w.shape, bf16) for w in weights]
        + [
            pltpu.VMEM(gain.shape, f32),
            pltpu.VMEM(taps.shape, f32),
            pltpu.VMEM((PLANE, depth, width), bf16),
            pltpu.VMEM((PLANE, cols, inner), bf16),
            pltpu.VMEM((chunks, WINDOW, slab), bf16),
            dma((11,)),
            dma((1,)),
            pltpu.VMEM((2, PLANE * rows, half), bf16),
            pltpu.VMEM((layers, PLANE * rows, 2 * half // layers), bf16),
            pltpu.VMEM((2, layers, 2, 2, depth, width), bf16),
            pltpu.VMEM((2, layers, 2, 2, cols, inner), bf16),
            pltpu.VMEM((PLANE * rows, width), f32),
            pltpu.VMEM((2, WINDOW + length, 2 * HEAD), bf16),
            pltpu.VMEM((2, 8 + length, chans), f32),
            pltpu.VMEM((QHEADS // KVHEADS, WINDOW, 2 * WINDOW), f32),
            pltpu.VMEM((2, PLANE * WINDOW, inner), bf16),
            pltpu.VMEM((chunks, PLANE * WINDOW, slab), bf16),
            pltpu.VMEM((chunks, PLANE * WINDOW, slab), bf16),
            pltpu.VMEM((2, PLANE * WINDOW, slab), f32),
            pltpu.VMEM((chunks, PLANE * WINDOW, slab), bf16),
            pltpu.VMEM((chunks, 2, WINDOW, slab), bf16),
            pltpu.VMEM((chunks, WINDOW, slab), bf16),
            pltpu.VMEM((chunks, WINDOW, slab), bf16),
        ]
        + sems(split)
        + sems(1)
        + [dma((number,)) for number in (2, 9, 4, 4, 1, chunks, 1, 2 * chunks, 1, chunks)],
        compiler_params=pltpu.CompilerParams(
            collective_id=0, has_side_effects=True, vmem_limit_bytes=60 << 20
        ),
    )(slopes, sinks, tokens, *weights, gain, taps)


def plane_body(
    tokens,
    norm_gain,
    outer_gate_w,
    inner_gate_w,
    signal_w,
    conv_taps,
    query_w,
    key_w,
    value_w,
    sink_logits,
    out_conv_w,
    out_attn_w,
):
    if tokens.shape[0] != 2 * WINDOW:
        return body(
            tokens, norm_gain, outer_gate_w, inner_gate_w, signal_w, conv_taps,
            query_w, key_w, value_w, sink_logits, out_conv_w, out_attn_w,
        )
    count = lax.axis_size("sp")
    wide = query_w.shape[1] // PLANE
    weights = (outer_gate_w, inner_gate_w, signal_w, query_w, key_w, value_w, out_conv_w.T, out_attn_w.T)
    slopes = jnp.array([2.0 ** (-8.0 * h / QHEADS) for h in range(1, QHEADS + 1)], jnp.float32)
    return whole_layer(
        count, tokens, weights, norm_gain.reshape(1, -1), conv_taps, slopes, sink_logits, wide
    )


def solution(mesh):
    kv_local = KVHEADS // mesh.shape["tp"]
    fits = mesh.shape["tp"] == 2 and kv_local == PLANE and mesh.shape["sp"] == LAYERS * PLANE
    chosen = plane_body if fits else body
    in_specs = (
        P("sp", "tp"),
        P(),
        P("sp", "tp"),
        P("sp", "tp"),
        P("sp", "tp"),
        P(None, "tp"),
        P("sp", "tp"),
        P("sp", "tp"),
        P("sp", "tp"),
        P("tp"),
        P("tp", "sp"),
        P("tp", "sp"),
    )
    out_specs = P(("sp", "tp"), None)
    return jax.shard_map(chosen, mesh=mesh, in_specs=in_specs, out_specs=out_specs, check_vma=False)
```

```python
import functools

import jax
import jax.numpy as jnp
from jax import lax
from jax.experimental import pallas as pl
from jax.experimental.pallas import tpu as pltpu
from jax.sharding import PartitionSpec as P

QHEADS = 24
KVHEADS = 8
HEAD = 64
TAPS = 3
WINDOW = 128
PLANE = 4
LAYERS = 4
PAIR, APART, BOTH = 1, 2, 3
FAR, NEAR = (0,), (1,)
MESH = pl.DeviceIdType.MESH


def from_behind(value, axis, steps):
    count = lax.axis_size(axis)
    initial, last = (max(0, -steps), min(count, count - steps))
    return lax.ppermute(value, axis, [(source, source + steps) for source in range(initial, last)])


def add_products(pieces, normed):
    return tuple((jnp.dot(normed, piece, preferred_element_type=jnp.float32) for piece in pieces))


def convolve(gated, before, outer, conv_taps):
    extended = jnp.concatenate([before, gated], axis=0).astype(jnp.float32)
    length = gated.shape[0]
    conv = sum((conv_taps[k] * extended[k : k + length] for k in range(conv_taps.shape[0])))
    return (outer.astype(jnp.float32) * conv).astype(jnp.bfloat16)


def attention(queries, keys_ext, values_ext, sink_logits, offset):
    f32 = jnp.float32
    length = queries.shape[0]
    kv_local = keys_ext.shape[1] // HEAD
    group = QHEADS // KVHEADS
    heads_local = kv_local * group
    span = min(512, length)
    first = lax.axis_index("tp") * heads_local + 1
    slopes = jnp.exp2(
        -8.0 * (first + jnp.arange(heads_local, dtype=jnp.int32)).astype(f32) / QHEADS
    ).reshape(kv_local, group)
    sinks = sink_logits.reshape(kv_local, group)[:, :, None]

    def attend(block):
        start = block * span
        qblock = queries.reshape(span, kv_local, group, HEAD)
        kblock = keys_ext.reshape(span + WINDOW, kv_local, HEAD)
        vblock = values_ext.reshape(span + WINDOW, kv_local, HEAD)
        scores = jnp.einsum(
            "qhgd,shd->hgqs", qblock, kblock, preferred_element_type=f32
        ) * HEAD ** (-0.5)
        qpos = offset + start + jnp.arange(span, dtype=jnp.int32)
        kpos = offset + start - WINDOW + jnp.arange(span + WINDOW, dtype=jnp.int32)
        dist = qpos[:, None] - kpos[None, :]
        valid = (dist >= 0) & (dist < WINDOW) & (kpos >= 0)[None, :]
        scores = scores - slopes[:, :, None, None] * dist.astype(f32)
        scores = jnp.where(valid, scores, -1e30)
        top = jnp.maximum(jnp.max(scores, axis=-1), sinks)
        expo = jnp.exp(scores - top[..., None])
        total = jnp.sum(expo, axis=-1) + jnp.exp(sinks - top)
        probs = (expo / total[..., None]).astype(jnp.bfloat16)
        out = jnp.einsum("hgqs,shd->qhgd", probs, vblock, preferred_element_type=f32)
        return out.reshape(span, heads_local * HEAD)

    blocks = lax.map(attend, jnp.arange(length // span, dtype=jnp.int32))
    return blocks.reshape(length, heads_local * HEAD).astype(jnp.bfloat16)


def body(
    tokens,
    norm_gain,
    outer_gate_w,
    inner_gate_w,
    signal_w,
    conv_taps,
    query_w,
    key_w,
    value_w,
    sink_logits,
    out_conv_w,
    out_attn_w,
):
    f32 = jnp.float32
    bf16 = jnp.bfloat16
    whole = lax.all_gather(tokens, "tp", axis=1, tiled=True)
    x32 = whole.astype(f32)
    normed = (
        x32 * lax.rsqrt(jnp.mean(x32 * x32, axis=-1, keepdims=True) + 1e-06) * norm_gain
    ).astype(bf16)
    length = normed.shape[0]
    offset = lax.axis_index("sp") * length

    def fold_rows(pieces):
        return add_products(pieces, normed)

    conv_weights = (outer_gate_w, inner_gate_w, signal_w)
    conv_results = fold_rows(
        (
            lax.all_gather(conv_weights[0], "sp", axis=0, tiled=True),
            lax.all_gather(conv_weights[1], "sp", axis=0, tiled=True),
            lax.all_gather(conv_weights[2], "sp", axis=0, tiled=True),
        )
    )
    outer, inner, signal = tuple((result.astype(bf16) for result in conv_results))
    gated = (inner.astype(f32) * signal.astype(f32)).astype(bf16)
    before = from_behind(gated[length - TAPS + 1 :], "sp", 1)
    conv_out = convolve(gated, before, outer, conv_taps)
    attn_weights = (query_w, key_w, value_w)
    attn_results = fold_rows(
        (
            lax.all_gather(attn_weights[0], "sp", axis=0, tiled=True),
            lax.all_gather(attn_weights[1], "sp", axis=0, tiled=True),
            lax.all_gather(attn_weights[2], "sp", axis=0, tiled=True),
        )
    )
    queries, keys, values = tuple((result.astype(bf16) for result in attn_results))
    keys_before, values_before = from_behind(
        (keys[length - WINDOW :], values[length - WINDOW :]), "sp", 1
    )
    keys_ext = jnp.concatenate([keys_before, keys], axis=0)
    values_ext = jnp.concatenate([values_before, values], axis=0)
    attn_out = attention(queries, keys_ext, values_ext, sink_logits, offset)
    conv_whole, attn_whole = (
        lax.all_gather(out_conv_w, "sp", axis=1, tiled=True),
        lax.all_gather(out_attn_w, "sp", axis=1, tiled=True),
    )
    result = jnp.dot(conv_out, conv_whole, preferred_element_type=f32)
    mixed = lax.psum_scatter(
        (result + jnp.dot(attn_out, attn_whole, preferred_element_type=f32)).astype(jnp.bfloat16),
        "tp",
        scatter_dimension=0,
        tiled=True,
    ).astype(jnp.float32)
    return mixed.astype(bf16)

class Stream:
    def __init__(self, at, src, buf, sems, split):
        self.at, self.src, self.buf, self.split = at, src, buf, split
        self.zs, self.zr, self.ys, self.yr, self.xs, self.xr = sems
        self.rows = src.shape[1] // split

    def part(self, s):
        return pl.ds(s * self.rows, self.rows)

    def slot(self, t, origin, y, x, s):
        return self.buf.at[t, origin, y, x, self.part(s)]

    def origin(self, up, d):
        return self.at.z - d if up else self.at.z + d

    def column(self, r):
        return self.at.x if r == 0 else 1 - self.at.x

    def z_copy(self, up, d, r, t, s, send_d):
        at = self.at
        dst = self.slot(t, self.origin(up, d), at.y, self.column(r), s)
        src = self.src.at[2 * t + at.x, self.part(s)] if d == 0 and r == 0 else dst
        side = 0 if up else 1
        i = (((side * (at.layers - 1) + send_d) * 2 + r) * 2 + t) * self.split + s
        return remote(src, dst, self.zs.at[2 * side + t], self.zr.at[i], at.above if up else at.below)

    def z_send(self, up, d, r, t, s, only=True):
        z, layers = self.at.z, self.at.layers
        if d >= layers - 1:
            return
        if up:
            go = (z >= d) & (z + (1 if t else 2) < layers)
        else:
            go = (z + d < layers) & (z >= (2 if t else 1))

        @pl.when(go & only)
        def _():
            self.z_copy(up, d, r, t, s, d).start()

    def y_copy(self, up, d, r, s, y):
        at = self.at
        dst = self.slot(at.zl, self.origin(up, d), y, self.column(r), s)
        src = self.src.at[2 * at.zl + at.x, self.part(s)] if d == 0 and r == 0 else dst
        m = d if up or d == 0 else at.layers - 1 + d
        return remote(src, dst, self.ys.at[0], self.yr.at[m], at.ypeer)

    def x_copy(self, t, s, receive=False):
        at = self.at
        src = self.src.at[2 * t + 1 - at.x, self.part(s)]
        dst = self.slot(t, at.z, at.y, 1 - at.x if receive else at.x, s)
        return remote(src, dst, self.xs.at[0], self.xr.at[t * self.split + s], at.xpeer)

    def send_z(self, r, s, which=FAR + NEAR, only=True):
        for k in which:
            self.z_send(True, 0, r, 1 - k, s, only=only)
            self.z_send(False, 0, r, k, s, only=only)

    def start_x(self):
        for s in range(self.split):
            for t in range(2):
                self.x_copy(t, s).start()

    def wait_x(self, s):
        for t in range(2):
            self.x_copy(t, s, True).wait_recv()

    def send_y(self, r, s, only=True):
        @pl.when(only)
        def _():
            self.y_copy(True, 0, r, s, self.at.y).start()

    def on_z(self, d, r, s, which=FAR + NEAR, sides=BOTH, only=True):
        z, layers, zl = self.at.z, self.at.layers, self.at.zl

        def arrive(up, t):
            if up:
                here = (z >= d) if t else (z >= d) & (z + 1 < layers)
            else:
                here = (z + d < layers) & (z >= 1) if t else (z + d < layers)
            if sides == PAIR:
                here = here & (zl == (1 if up else 0))
            elif sides == APART:
                here = here & (zl == (0 if up else 1))

            @pl.when(here & only)
            def _():
                self.z_copy(up, d, r, t, s, d - 1).wait_recv()
                self.z_send(up, d, r, t, s)

                @pl.when(zl == t)
                def _():
                    self.y_copy(up, d, r, s, self.at.y).start()

        for k in which:
            arrive(True, 1 - k)
            arrive(False, k)

    def on_y(self, d, sides=BOTH, up=None):
        z, layers, y, zl = self.at.z, self.at.layers, self.at.y, self.at.zl

        def each(up):
            ref = self.buf.at[zl, self.origin(up, d), 1 - y]
            m = d if up or d == 0 else layers - 1 + d
            remote(ref, ref, self.ys.at[0], self.yr.at[m], self.at.ypeer).wait_recv()

        if d == 0 or up is not None:
            each(up is not False)
            return
        from_below, from_above = z >= d, z + d < layers
        if sides != BOTH:
            near = 1 if sides == PAIR else 0
            from_below, from_above = from_below & (zl == near), from_above & (zl == 1 - near)

        @pl.when(from_below)
        def _():
            each(True)

        @pl.when(from_above)
        def _():
            each(False)

    def finish(self):
        at = self.at
        layers = at.layers

        def sent(ref, sem):
            remote(ref, ref, sem, self.yr.at[0], at.ypeer).wait_send()

        sent(self.buf.at[0, 0, 0], self.xs.at[0])
        sent(self.buf.at[0, :, 0], self.ys.at[0])
        for up in (True, False):
            for t in range(2):
                for z in range(layers):
                    beyond = layers - z if up else z + 1
                    if beyond > (1 if (t == 1) == up else 2):
                        number = z + 1 if up else layers - z

                        @pl.when(at.z == z)
                        def _():
                            sent(self.buf.at[0, pl.ds(0, number), 0], self.zs.at[(0 if up else 2) + t])


def join(weights, out_ref):
    for p in range(PLANE):
        pieces = []
        for ref in weights:
            width = ref.shape[1] // PLANE
            pieces.append(ref[:, p * width : (p + 1) * width])
        out_ref[p] = jnp.concatenate(pieces, axis=1)


class Place:
    def __init__(self, count):
        me, core = lax.axis_index("sp"), lax.axis_index("tp")
        self.me, self.core, self.layers = me, core, count // PLANE
        self.z, self.y, self.x = me // PLANE, lax.rem(me // 2, 2), lax.rem(me, 2)
        self.zl, self.zh = lax.rem(self.z, 2), self.z // 2
        self.spot = 2 * self.zl + self.x

        def device(sp, tp=core):
            return {"sp": sp, "tp": tp}

        self.partner = device(me, 1 - core)
        self.xpeer = device(me + 1 - 2 * self.x)
        self.ypeer = device(me + 2 - 4 * self.y)
        self.zpeer = device(me + PLANE * (1 - 2 * self.zl))
        self.above, self.below = device(me + PLANE), device(me - PLANE)
        self.after, self.prior = device(me + PLANE + 2), device(me - PLANE - 2)
        self.has_after = (self.y == 1) & (self.zh + 1 < self.layers // 2)
        self.has_prior = (self.y == 0) & (self.zh > 0)

    def greet(self):
        barrier = pltpu.get_barrier_semaphore()

        def signal(target):
            pl.semaphore_signal(barrier, inc=1, device_id=target, device_id_type=MESH)

        for target in (self.partner, self.xpeer, self.ypeer):
            signal(target)
        number = 3
        for go, target in (
            (self.z + 1 < self.layers, self.above),
            (self.z > 0, self.below),
            (self.has_after, self.after),
            (self.has_prior, self.prior),
        ):
            pl.when(go)(functools.partial(signal, target))
            number = number + jnp.where(go, 1, 0)
        return lambda: pl.semaphore_wait(barrier, number)


def remote(src, dst, send_sem, recv_sem, target):
    return pltpu.make_async_remote_copy(
        src_ref=src, dst_ref=dst, send_sem=send_sem, recv_sem=recv_sem, device_id=target, device_id_type=MESH
    )


def layer_entry(
    count, chans, wide, split, slopes_ref, sinks_ref, tok_hbm, *refs,
):
    raw_hbm, (gain_hbm, taps_hbm, out_hbm, far_hbm), refs = refs[:8], refs[8:12], refs[12:]
    raw, refs = refs[:8], refs[8:]
    layer_kernel(count, chans, wide, split, slopes_ref, sinks_ref, tok_hbm, raw_hbm, gain_hbm, taps_hbm, out_hbm, far_hbm, raw, *refs)


def layer_kernel(
    count, chans, wide, split, slopes_ref, sinks_ref, tok_hbm, raw_hbm, gain_hbm, taps_hbm, out_hbm, far_hbm, raw,
    gain_ref, taps_ref, w_ref, o_ref, out_ref, ls, os, x_ref, nrm_ref, wbuf, obuf, acc_ref, ext, gext, bias, hid, dsend, drecv, own, s1, r1, s2,
    wzs, wzr, wys, wyr, wxs, wxr, ozs, ozr, oys, oyr, oxs, oxr, ts, tr, hs, hr, ds, dr, fs, fr, gs, gr,
):
    f32, bf16 = jnp.float32, jnp.bfloat16
    at = Place(count)
    core, layers, x, y, z, zl, zh, spot = at.core, at.layers, at.x, at.y, at.z, at.zl, at.zh, at.spot
    rows, half = tok_hbm.shape
    length = 2 * rows
    group = wide // HEAD
    front = 8
    ins = Stream(at, w_ref, wbuf, (wzs, wzr, wys, wyr, wxs, wxr), split)
    outs = Stream(at, o_ref, obuf, (ozs, ozr, oys, oyr, oxs, oxr), 1)
    arrived = at.greet()

    def block(p, side=None):
        return x_ref.at[core if side is None else side, pl.ds(pl.multiple_of(p * rows, rows), rows)]

    p_own, p_x, p_z, p_far = spot, 2 * zl + 1 - x, 2 * (1 - zl) + x, 2 * (1 - zl) + 1 - x
    loads = [
        pltpu.make_async_copy(src, dst, ls.at[k])
        for k, (src, dst) in enumerate(
            list(zip(raw_hbm[:6], raw[:6]))
            + [(tok_hbm, block(p_own))]
            + list(zip(raw_hbm[6:], raw[6:]))
            + [(gain_hbm, gain_ref), (taps_hbm, taps_ref)]
        )
    ]
    for load in loads:
        load.start()
    for load in loads[:6]:
        load.wait()
    join(raw[:6], w_ref)
    loads[6].wait()
    arrived()
    at_end = (z == 0) | (z == layers - 1)
    inside = jnp.logical_not(at_end)
    ins.send_z(0, 0, FAR)
    ins.start_x()
    ins.send_y(0, 0)
    ins.send_y(0, 1)
    ins.send_z(0, 1, FAR)
    ins.send_z(0, 0, NEAR)
    ins.send_z(0, 1, NEAR, at_end)
    def half_block(p, n):
        return x_ref.at[core, pl.ds(pl.multiple_of(p * rows + n * (rows // 2), rows // 2), rows // 2)]

    def tok_z(n, p=p_own):
        return remote(half_block(p, n), half_block(p, n), ts.at[0], tr.at[1 + n], at.zpeer)

    def tok_far(n, p=p_z):
        return remote(half_block(p, n), half_block(p, n), ts.at[0], tr.at[3 + n], at.xpeer)

    def send_tok_z(n, only):
        @pl.when(only)
        def _():
            tok_z(n).start()

    tok_x = remote(block(p_own), block(p_own), ts.at[0], tr.at[0], at.xpeer)
    swaps = [
        remote(block(p), block(p), ts.at[1], tr.at[5 + k], at.partner)
        for k, p in enumerate((p_own, p_x, p_z, p_far))
    ]
    tok_x.start()
    tok_z(0).start()
    swaps[0].start()
    wbuf[zl, z, y, x] = w_ref[2 * zl + x]
    for load in loads[7:]:
        load.wait()
    join(raw[6:], o_ref)
    obuf[zl, z, y, x] = o_ref[2 * zl + x]
    span = 2 * half // layers
    strip = 32

    def normalise(k, p):
        remote(block(p, core), block(p, 1 - core), ts.at[1], tr.at[5 + k], at.partner).wait_recv()

        def step(i, carry):
            at_rows = pl.ds(pl.multiple_of(p * rows + i * strip, strip), strip)
            whole = jnp.concatenate([x_ref[0, at_rows, :], x_ref[1, at_rows, :]], axis=1).astype(f32)
            mean = jnp.sum(whole * whole, axis=1, keepdims=True) / (2 * half)
            scaled = (whole * lax.rsqrt(mean + 1e-06) * gain_ref[...]).astype(bf16)
            for j in range(layers):
                nrm_ref[j, at_rows, :] = scaled[:, j * span : (j + 1) * span]
            return carry

        lax.fori_loop(0, rows // strip, step, 0)

    def add_layer(origin, fresh):
        def step(i, carry):
            at_rows = pl.ds(pl.multiple_of(i * rows, rows), rows)
            product = jnp.dot(
                nrm_ref[origin, at_rows, :],
                wbuf[zl, origin].reshape(span, wbuf.shape[5]),
                preferred_element_type=f32,
            )
            acc_ref[at_rows, :] = product if fresh else acc_ref[at_rows, :] + product
            return carry

        lax.fori_loop(0, PLANE, step, 0)

    def add_row(origin, row_y):
        size = span // 2

        def step(i, carry):
            at_rows = pl.ds(pl.multiple_of(i * rows, rows), rows)
            acc_ref[at_rows, :] += jnp.dot(
                nrm_ref[origin, at_rows, pl.ds(pl.multiple_of(row_y * size, size), size)],
                wbuf[zl, origin, row_y].reshape(size, wbuf.shape[5]),
                preferred_element_type=f32,
            )
            return carry

        lax.fori_loop(0, PLANE, step, 0)

    def add_last():
        def two(d, up):
            add_row(ins.origin(up, d), y)
            ins.on_y(d, up=up)
            add_row(ins.origin(up, d), 1 - y)

        for above in (False, True):
            for d, where in ((3, at_end), (2, inside)):
                mine = (z >= d) if above else (z + d < layers)

                @pl.when(mine & where)
                def _():
                    two(d, above)

    def add_both(d):
        ins.on_y(d)

        @pl.when(z >= d)
        def _():
            add_layer(z - d, False)

        @pl.when(z + d < layers)
        def _():
            add_layer(z + d, False)

    def from_x(s):
        ins.wait_x(s)
        ins.send_z(1, s, FAR)
        ins.send_z(1, s, NEAR, at_end)
        ins.send_y(1, s)
        ins.on_z(1, 0, s, FAR)

    from_x(0)
    send_tok_z(1, at_end)
    ins.on_z(1, 0, 0, NEAR, APART)
    from_x(1)
    send_tok_z(1, inside)
    ins.send_z(0, 1, NEAR, inside)
    for s in range(split):
        ins.send_z(1, s, NEAR, inside)
    outs.send_y(0, 0, inside)
    normalise(0, p_own)
    ins.on_z(1, 1, 0, FAR, PAIR, at_end)
    ins.on_z(2, 0, 0, FAR, only=at_end)
    ins.on_z(1, 1, 0, FAR, APART)
    ins.on_z(2, 0, 0, FAR, only=inside)
    ins.on_z(1, 1, 1, FAR, APART)
    tok_z(0, p_z).wait_recv()
    tok_far(0).start()
    ins.on_z(2, 0, 1, FAR, only=inside)
    ins.on_z(1, 1, 1, FAR, PAIR, at_end)
    ins.on_z(1, 0, 1, NEAR, APART)
    ins.on_z(1, 1, 0, FAR, PAIR, inside)
    for s in range(split):
        ins.on_z(1, 0, s, NEAR, PAIR)
    remote(block(p_x), block(p_x), ts.at[0], tr.at[0], at.xpeer).wait_recv()
    swaps[1].start()
    ins.on_z(2, 0, 1, FAR, only=at_end)
    outs.send_y(0, 0, at_end)
    ins.on_z(1, 1, 0, NEAR, APART)
    normalise(1, p_x)
    ins.on_z(1, 1, 1, NEAR, APART)
    tok_z(1, p_z).wait_recv()
    tok_far(1).start()
    swaps[2].start()
    outs.start_x()
    ins.on_z(2, 1, 0, FAR, only=inside)
    ins.on_z(2, 1, 0, FAR, only=at_end)
    normalise(2, p_z)
    ins.on_z(2, 0, 0, NEAR, only=inside)
    ins.on_z(1, 1, 1, FAR, PAIR, inside)
    for s in range(split):
        ins.on_z(1, 1, s, NEAR, PAIR)
    ins.on_z(3, 0, 0)
    outs.send_z(0, 0, only=at_end)
    ins.on_z(2, 0, 1, NEAR, only=inside)
    tok_far(0, p_far).wait_recv()
    tok_far(1, p_far).wait_recv()
    swaps[3].start()
    ins.on_z(2, 1, 1, FAR)
    ins.on_z(3, 0, 1)
    normalise(3, p_far)
    ins.on_z(2, 1, 0, NEAR, only=inside)
    ins.on_z(3, 1, 0)
    ins.on_y(0)
    add_layer(z, True)
    ins.on_z(2, 1, 1, NEAR, only=inside)
    outs.wait_x(0)
    outs.on_z(1, 0, 0, FAR, PAIR, inside)
    outs.send_z(0, 0, FAR, inside)
    outs.send_z(1, 0, FAR)
    outs.send_z(1, 0, NEAR, at_end)
    outs.send_y(1, 0, inside)
    ins.on_z(3, 1, 1)
    add_both(1)
    outs.send_y(1, 0, at_end)
    outs.on_z(1, 1, 0, FAR, PAIR, inside)
    outs.on_z(2, 0, 0, FAR, only=inside)

    @pl.when(at_end)
    def _():
        add_both(2)

    outs.on_z(1, 0, 0, FAR, APART)
    add_last()

    def spread(i, carry):
        run, start = i // 4, pl.multiple_of(lax.rem(i, 4) * WINDOW, WINDOW)
        chunk = acc_ref[pl.ds(pl.multiple_of(i * WINDOW, WINDOW), WINDOW), :].astype(bf16)
        ext[run, pl.ds(start + WINDOW, WINDOW), :] = chunk[:, 3 * chans + wide :]
        product = chunk[:, chans : 2 * chans].astype(f32) * chunk[:, 2 * chans : 3 * chans].astype(f32)
        gext[run, pl.ds(start + front, WINDOW), :] = product.astype(bf16).astype(f32)
        return carry

    lax.fori_loop(0, 2 * length // WINDOW, spread, 0)

    def tails(run, after, target, action):
        kv = remote(
            ext.at[run, pl.ds(length, WINDOW)], ext.at[after, pl.ds(0, WINDOW)],
            hs.at[2 * run], hr.at[2 * after], target,
        )
        gated = remote(
            gext.at[run, pl.ds(length, front)], gext.at[after, pl.ds(0, front)],
            hs.at[2 * run + 1], hr.at[2 * after + 1], target,
        )
        for copy in (kv, gated):
            getattr(copy, action)()

    def all_tails(action):
        @pl.when(y == 0)
        def _():
            for run in range(2):
                tails(run, run, at.ypeer, action)

        @pl.when(y == 1)
        def _():
            tails(0, 1, at.ypeer, action)

        @pl.when(at.has_after)
        def _():
            tails(1, 0, at.after, action)

    all_tails("start")
    for r in range(2):
        outs.on_z(1, r, 0, NEAR, PAIR)
        outs.send_z(r, 0, NEAR, inside)
    first_run = (y == 0) & (zh == 0)

    @pl.when(first_run)
    def _():
        ext[0, 0:WINDOW, :] = jnp.zeros((WINDOW, 2 * HEAD), bf16)
        gext[0, 0:front, :] = jnp.zeros((front, chans), f32)

    taps = sum(jnp.where(spot == c, taps_ref[:, c * chans : (c + 1) * chans], 0.0) for c in range(PLANE))
    row = lax.broadcasted_iota(jnp.int32, (WINDOW, 2 * WINDOW), 0)
    col = lax.broadcasted_iota(jnp.int32, (WINDOW, 2 * WINDOW), 1)
    dist = WINDOW + row - col
    near = (dist >= 0) & (dist < WINDOW)
    far = dist.astype(f32)

    for g in range(group):
        bias[g] = jnp.where(near, -slopes_ref[(core * PLANE + spot) * group + g] * far, -1e30)
    ones = jnp.where(lax.broadcasted_iota(jnp.int32, (2 * WINDOW, HEAD), 1) == 0, 1.0, 0.0).astype(bf16)

    def mix(run, blk, first=False):
        start = pl.multiple_of(blk * WINDOW, WINDOW)
        chunk = acc_ref[pl.ds(pl.multiple_of(run * length + start, WINDOW), WINDOW), :].astype(bf16)
        window = gext[run, pl.ds(start, WINDOW + front), :]
        conv = sum(
            taps[k : k + 1, :] * window[front - TAPS + 1 + k : front - TAPS + 1 + k + WINDOW]
            for k in range(TAPS)
        )
        pieces = [(chunk[:, :chans].astype(f32) * conv).astype(bf16)]
        kv = ext[run, pl.ds(start, 2 * WINDOW), :]
        keys, values = kv[:, :HEAD], jnp.concatenate([kv[:, HEAD:], ones], axis=1)
        offset = ((2 * zh + run) * 2 + y) * length
        for g in range(group):
            at_head = 3 * chans + g * HEAD
            query = chunk[:, at_head : at_head + HEAD] * jnp.asarray(HEAD ** (-0.5), bf16)
            scores = bias[g] + lax.dot_general(
                query, keys, (((1,), (1,)), ((), ())), preferred_element_type=f32
            )
            if first:
                scores = jnp.where(offset - WINDOW + col >= 0, scores, -1e30)
            sink = sinks_ref[spot * group + g]
            top = jnp.maximum(jnp.max(scores, axis=1, keepdims=True), sink)
            expo = jnp.exp(scores - top).astype(bf16)
            summed = jnp.dot(expo, values, preferred_element_type=f32)
            total = summed[:, HEAD : HEAD + 1] + jnp.exp(sink - top)
            pieces.append((summed[:, :HEAD] / total).astype(bf16))
        place = pl.ds(pl.multiple_of((2 * run + blk // 2) * WINDOW, WINDOW), WINDOW)
        hid[lax.rem(blk, 2), place, :] = jnp.concatenate(pieces, axis=1)

    def mix_run(run):
        for blk in range(1, 4):
            mix(run, blk)

    def mix_first():
        for run in range(2):
            mix(run, 0, True)

    for r in range(2):
        outs.on_z(1, r, 0, FAR, PAIR, at_end)
    outs.on_z(3, 0, 0)
    outs.on_z(1, 1, 0, FAR, APART)
    mix_run(0)
    outs.on_z(2, 1, 0, FAR, only=inside)
    mix_run(1)

    def tails_in(after, target):
        for k, (ref, size) in enumerate(((ext, WINDOW), (gext, front))):
            remote(
                ref.at[after, pl.ds(length, size)], ref.at[after, pl.ds(0, size)],
                hs.at[2 * after + k], hr.at[2 * after + k], target,
            ).wait_recv()

    @pl.when(y == 1)
    def _():
        tails_in(0, at.ypeer)

    @pl.when(at.has_prior)
    def _():
        tails_in(0, at.prior)

    tails_in(1, at.ypeer)
    mix_first()

    lower = z < layers // 2
    cols = obuf.shape[3] * obuf.shape[4]
    order = [(0, True), (1, True), (0, False), (1, False), (3, True), (2, True), (3, False), (2, False)]
    chunks = len(order)

    def chunk_at(h):
        i, mine = order[h]
        return jnp.where(lower, i, layers - 1 - i), y if mine else 1 - y

    def product(side, h):
        layer, row_y = chunk_at(h)
        return lax.dot_general(
            hid[side], obuf[zl, layer, row_y].reshape(cols, hid.shape[2]),
            (((1,), (1,)), ((), ())), preferred_element_type=f32,
        )

    def slab(p):
        return pl.ds(pl.multiple_of(p * WINDOW, WINDOW), WINDOW)

    def swap(i):
        return remote(dsend.at[i], drecv.at[i], ds.at[0], dr.at[i], at.partner)

    def first_hop(i, j):
        if i % 2 == 0:
            target, p = at.xpeer, (2 * (1 - zl) if j == 0 else 2 * zl) + 1 - x
        else:
            target, p = at.zpeer, 2 * (1 - zl) + ((1 - x) if j == 0 else x)
        return remote(s1.at[i, slab(p)], r1.at[i, j], fs.at[0], fr.at[2 * i + j], target)

    def out_slab(i):
        layer, row_y = chunk_at(i)
        return pl.ds(pl.multiple_of((layer * 2 + row_y) * cols, cols), cols)

    def second_hop(i):
        return remote(s2.at[i], far_hbm.at[:, out_slab(i)], gs.at[0], gr.at[i], at.zpeer if i % 2 == 0 else at.xpeer)

    def begin(i):
        dsend[i] = product(1 - core, i).astype(bf16)
        own[i % 2] = product(core, i)
        swap(i).start()

    def fold(i):
        swap(i).wait_recv()
        s1[i] = (own[i % 2] + drecv[i].astype(f32)).astype(bf16)
        first_hop(i, 0).start()
        first_hop(i, 1).start()

    def relay(i):
        first_hop(i, 0).wait_recv()
        p = p_z if i % 2 == 0 else p_x
        s2[i] = (s1[i, slab(p), :].astype(f32) + r1[i, 0].astype(f32)).astype(bf16)
        second_hop(i).start()

    def out_copy(i):
        return pltpu.make_async_copy(out_ref.at[i], out_hbm.at[:, out_slab(i)], os.at[0])

    def collect(i):
        first_hop(i, 1).wait_recv()
        total = s1[i, slab(p_own), :].astype(f32) + r1[i, 1].astype(f32)
        out_ref[i] = total.astype(out_ref.dtype)
        out_copy(i).start()

    begin(0)
    outs.on_z(2, 0, 0, FAR, only=at_end)
    begin(1)
    fold(0)
    fold(1)
    outs.on_z(2, 1, 0, FAR, only=at_end)
    outs.on_z(2, 0, 0, NEAR, only=inside)
    outs.on_y(0)
    outs.on_y(1, sides=PAIR)
    begin(2)
    outs.on_z(1, 0, 0, NEAR, APART)
    outs.on_z(3, 1, 0)
    begin(3)
    fold(2)
    fold(3)
    outs.on_z(1, 1, 0, NEAR, APART)
    relay(0)
    outs.on_z(2, 1, 0, NEAR, only=inside)
    begin(4)
    relay(1)
    begin(5)
    fold(4)
    fold(5)
    collect(0)
    collect(1)
    relay(2)
    relay(3)
    outs.on_y(2)
    outs.on_y(3)
    begin(6)
    outs.on_y(1, sides=APART)
    begin(7)
    fold(6)
    fold(7)
    collect(2)
    collect(3)
    for h in range(4, chunks):
        relay(h)
        collect(h)

    def phase_finish():
        pltpu.make_async_copy(out_ref, out_ref, os.at[0]).wait()
        for h in range(chunks):
            second_hop(h).wait_recv()
        ins.finish()
        outs.finish()
        all_tails("wait_send")
        for ref, sem in (
            (x_ref.at[0, pl.ds(0, 3 * rows)], ts.at[0]),
            (x_ref.at[0], ts.at[1]),
            (dsend, ds.at[0]),
            (s1.at[pl.ds(0, chunks // 2)], fs.at[0]),
            (s2, gs.at[0]),
        ):
            remote(ref, ref, sem, dr.at[0], at.partner).wait_send()

    phase_finish()


def whole_layer(count, tokens, weights, gain, taps, slopes, sinks, wide):
    layers = count // PLANE
    rows, half = tokens.shape
    depth = weights[0].shape[0]
    width = sum(w.shape[1] for w in weights[:6]) // PLANE
    cols = weights[6].shape[0]
    inner = sum(w.shape[1] for w in weights[6:]) // PLANE
    chans = taps.shape[1] // PLANE
    bf16, f32 = jnp.bfloat16, jnp.float32
    dma = pltpu.SemaphoreType.DMA
    split = 2
    length = 2 * rows
    slab = 2 * cols
    chunks = 2 * layers

    def sems(parts):
        hops = 2 * (layers - 1) * 4 * parts
        return [dma((number,)) for number in (4, hops, 1, 2 * layers - 1, 1, 2 * parts)]

    smem = pl.BlockSpec(memory_space=pltpu.SMEM)
    return pl.pallas_call(
        functools.partial(layer_entry, count, chans, wide, split),
        out_shape=[jax.ShapeDtypeStruct((rows // 2, 2 * half), bf16)] * 2,
        in_specs=[smem] * 2 + [pl.BlockSpec(memory_space=pltpu.HBM)] * 11,
        out_specs=[pl.BlockSpec(memory_space=pltpu.HBM)] * 2,
        scratch_shapes=[pltpu.VMEM(w.shape, bf16) for w in weights]
        + [
            pltpu.VMEM(gain.shape, f32),
            pltpu.VMEM(taps.shape, f32),
            pltpu.VMEM((PLANE, depth, width), bf16),
            pltpu.VMEM((PLANE, cols, inner), bf16),
            pltpu.VMEM((chunks, WINDOW, slab), bf16),
            dma((11,)),
            dma((1,)),
            pltpu.VMEM((2, PLANE * rows, half), bf16),
            pltpu.VMEM((layers, PLANE * rows, 2 * half // layers), bf16),
            pltpu.VMEM((2, layers, 2, 2, depth, width), bf16),
            pltpu.VMEM((2, layers, 2, 2, cols, inner), bf16),
            pltpu.VMEM((PLANE * rows, width), f32),
            pltpu.VMEM((2, WINDOW + length, 2 * HEAD), bf16),
            pltpu.VMEM((2, 8 + length, chans), f32),
            pltpu.VMEM((QHEADS // KVHEADS, WINDOW, 2 * WINDOW), f32),
            pltpu.VMEM((2, PLANE * WINDOW, inner), bf16),
            pltpu.VMEM((chunks, PLANE * WINDOW, slab), bf16),
            pltpu.VMEM((chunks, PLANE * WINDOW, slab), bf16),
            pltpu.VMEM((2, PLANE * WINDOW, slab), f32),
            pltpu.VMEM((chunks, PLANE * WINDOW, slab), bf16),
            pltpu.VMEM((chunks, 2, WINDOW, slab), bf16),
            pltpu.VMEM((chunks, WINDOW, slab), bf16),
        ]
        + sems(split)
        + sems(1)
        + [dma((number,)) for number in (2, 9, 4, 4, 1, chunks, 1, 2 * chunks, 1, chunks)],
        compiler_params=pltpu.CompilerParams(
            collective_id=0, has_side_effects=True, vmem_limit_bytes=60 << 20
        ),
    )(slopes, sinks, tokens, *weights, gain, taps)


def plane_body(
    tokens,
    norm_gain,
    outer_gate_w,
    inner_gate_w,
    signal_w,
    conv_taps,
    query_w,
    key_w,
    value_w,
    sink_logits,
    out_conv_w,
    out_attn_w,
):
    if tokens.shape[0] != 2 * WINDOW:
        return body(
            tokens, norm_gain, outer_gate_w, inner_gate_w, signal_w, conv_taps,
            query_w, key_w, value_w, sink_logits, out_conv_w, out_attn_w,
        )
    count = lax.axis_size("sp")
    wide = query_w.shape[1] // PLANE
    weights = (outer_gate_w, inner_gate_w, signal_w, query_w, key_w, value_w, out_conv_w.T, out_attn_w.T)
    slopes = jnp.array([2.0 ** (-8.0 * h / QHEADS) for h in range(1, QHEADS + 1)], jnp.float32)
    near, far = whole_layer(
        count, tokens, weights, norm_gain.reshape(1, -1), conv_taps, slopes, sink_logits, wide
    )
    return (near.astype(jnp.float32) + far.astype(jnp.float32)).astype(jnp.bfloat16)


def solution(mesh):
    kv_local = KVHEADS // mesh.shape["tp"]
    fits = mesh.shape["tp"] == 2 and kv_local == PLANE and mesh.shape["sp"] == LAYERS * PLANE
    chosen = plane_body if fits else body
    in_specs = (
        P("sp", "tp"),
        P(),
        P("sp", "tp"),
        P("sp", "tp"),
        P("sp", "tp"),
        P(None, "tp"),
        P("sp", "tp"),
        P("sp", "tp"),
        P("sp", "tp"),
        P("tp"),
        P("tp", "sp"),
        P("tp", "sp"),
    )
    out_specs = P(("sp", "tp"), None)
    return jax.shard_map(chosen, mesh=mesh, in_specs=in_specs, out_specs=out_specs, check_vma=False)
```

```python
import functools

import jax
import jax.numpy as jnp
from jax import lax
from jax.experimental import pallas as pl
from jax.experimental.pallas import tpu as pltpu
from jax.sharding import PartitionSpec as P

QHEADS = 24
KVHEADS = 8
HEAD = 64
TAPS = 3
WINDOW = 128
PLANE = 4
LAYERS = 4
PAIR, APART, BOTH = 1, 2, 3
FAR, NEAR = (0,), (1,)
MESH = pl.DeviceIdType.MESH


def from_behind(value, axis, steps):
    count = lax.axis_size(axis)
    initial, last = (max(0, -steps), min(count, count - steps))
    return lax.ppermute(value, axis, [(source, source + steps) for source in range(initial, last)])


def add_products(pieces, normed):
    return tuple((jnp.dot(normed, piece, preferred_element_type=jnp.float32) for piece in pieces))


def convolve(gated, before, outer, conv_taps):
    extended = jnp.concatenate([before, gated], axis=0).astype(jnp.float32)
    length = gated.shape[0]
    conv = sum((conv_taps[k] * extended[k : k + length] for k in range(conv_taps.shape[0])))
    return (outer.astype(jnp.float32) * conv).astype(jnp.bfloat16)


def attention(queries, keys_ext, values_ext, sink_logits, offset):
    f32 = jnp.float32
    length = queries.shape[0]
    kv_local = keys_ext.shape[1] // HEAD
    group = QHEADS // KVHEADS
    heads_local = kv_local * group
    span = min(512, length)
    first = lax.axis_index("tp") * heads_local + 1
    slopes = jnp.exp2(
        -8.0 * (first + jnp.arange(heads_local, dtype=jnp.int32)).astype(f32) / QHEADS
    ).reshape(kv_local, group)
    sinks = sink_logits.reshape(kv_local, group)[:, :, None]

    def attend(block):
        start = block * span
        qblock = queries.reshape(span, kv_local, group, HEAD)
        kblock = keys_ext.reshape(span + WINDOW, kv_local, HEAD)
        vblock = values_ext.reshape(span + WINDOW, kv_local, HEAD)
        scores = jnp.einsum(
            "qhgd,shd->hgqs", qblock, kblock, preferred_element_type=f32
        ) * HEAD ** (-0.5)
        qpos = offset + start + jnp.arange(span, dtype=jnp.int32)
        kpos = offset + start - WINDOW + jnp.arange(span + WINDOW, dtype=jnp.int32)
        dist = qpos[:, None] - kpos[None, :]
        valid = (dist >= 0) & (dist < WINDOW) & (kpos >= 0)[None, :]
        scores = scores - slopes[:, :, None, None] * dist.astype(f32)
        scores = jnp.where(valid, scores, -1e30)
        top = jnp.maximum(jnp.max(scores, axis=-1), sinks)
        expo = jnp.exp(scores - top[..., None])
        total = jnp.sum(expo, axis=-1) + jnp.exp(sinks - top)
        probs = (expo / total[..., None]).astype(jnp.bfloat16)
        out = jnp.einsum("hgqs,shd->qhgd", probs, vblock, preferred_element_type=f32)
        return out.reshape(span, heads_local * HEAD)

    blocks = lax.map(attend, jnp.arange(length // span, dtype=jnp.int32))
    return blocks.reshape(length, heads_local * HEAD).astype(jnp.bfloat16)


def body(
    tokens,
    norm_gain,
    outer_gate_w,
    inner_gate_w,
    signal_w,
    conv_taps,
    query_w,
    key_w,
    value_w,
    sink_logits,
    out_conv_w,
    out_attn_w,
):
    f32 = jnp.float32
    bf16 = jnp.bfloat16
    whole = lax.all_gather(tokens, "tp", axis=1, tiled=True)
    x32 = whole.astype(f32)
    normed = (
        x32 * lax.rsqrt(jnp.mean(x32 * x32, axis=-1, keepdims=True) + 1e-06) * norm_gain
    ).astype(bf16)
    length = normed.shape[0]
    offset = lax.axis_index("sp") * length

    def fold_rows(pieces):
        return add_products(pieces, normed)

    conv_weights = (outer_gate_w, inner_gate_w, signal_w)
    conv_results = fold_rows(
        (
            lax.all_gather(conv_weights[0], "sp", axis=0, tiled=True),
            lax.all_gather(conv_weights[1], "sp", axis=0, tiled=True),
            lax.all_gather(conv_weights[2], "sp", axis=0, tiled=True),
        )
    )
    outer, inner, signal = tuple((result.astype(bf16) for result in conv_results))
    gated = (inner.astype(f32) * signal.astype(f32)).astype(bf16)
    before = from_behind(gated[length - TAPS + 1 :], "sp", 1)
    conv_out = convolve(gated, before, outer, conv_taps)
    attn_weights = (query_w, key_w, value_w)
    attn_results = fold_rows(
        (
            lax.all_gather(attn_weights[0], "sp", axis=0, tiled=True),
            lax.all_gather(attn_weights[1], "sp", axis=0, tiled=True),
            lax.all_gather(attn_weights[2], "sp", axis=0, tiled=True),
        )
    )
    queries, keys, values = tuple((result.astype(bf16) for result in attn_results))
    keys_before, values_before = from_behind(
        (keys[length - WINDOW :], values[length - WINDOW :]), "sp", 1
    )
    keys_ext = jnp.concatenate([keys_before, keys], axis=0)
    values_ext = jnp.concatenate([values_before, values], axis=0)
    attn_out = attention(queries, keys_ext, values_ext, sink_logits, offset)
    conv_whole, attn_whole = (
        lax.all_gather(out_conv_w, "sp", axis=1, tiled=True),
        lax.all_gather(out_attn_w, "sp", axis=1, tiled=True),
    )
    result = jnp.dot(conv_out, conv_whole, preferred_element_type=f32)
    mixed = lax.psum_scatter(
        (result + jnp.dot(attn_out, attn_whole, preferred_element_type=f32)).astype(jnp.bfloat16),
        "tp",
        scatter_dimension=0,
        tiled=True,
    ).astype(jnp.float32)
    return mixed.astype(bf16)

class Stream:
    def __init__(self, at, src, buf, sems, split):
        self.at, self.src, self.buf, self.split = at, src, buf, split
        self.zs, self.zr, self.ys, self.yr, self.xs, self.xr = sems
        self.rows = src.shape[1] // split

    def part(self, s):
        return pl.ds(s * self.rows, self.rows)

    def slot(self, t, origin, y, x, s):
        return self.buf.at[t, origin, y, x, self.part(s)]

    def origin(self, up, d):
        return self.at.z - d if up else self.at.z + d

    def column(self, r):
        return self.at.x if r == 0 else 1 - self.at.x

    def z_copy(self, up, d, r, t, s, send_d):
        at = self.at
        dst = self.slot(t, self.origin(up, d), at.y, self.column(r), s)
        src = self.src.at[2 * t + at.x, self.part(s)] if d == 0 and r == 0 else dst
        side = 0 if up else 1
        i = (((side * (at.layers - 1) + send_d) * 2 + r) * 2 + t) * self.split + s
        return remote(src, dst, self.zs.at[2 * side + t], self.zr.at[i], at.above if up else at.below)

    def z_send(self, up, d, r, t, s, only=True):
        z, layers = self.at.z, self.at.layers
        if d >= layers - 1:
            return
        if up:
            go = (z >= d) & (z + (1 if t else 2) < layers)
        else:
            go = (z + d < layers) & (z >= (2 if t else 1))

        @pl.when(go & only)
        def _():
            self.z_copy(up, d, r, t, s, d).start()

    def y_copy(self, up, d, r, s, y):
        at = self.at
        dst = self.slot(at.zl, self.origin(up, d), y, self.column(r), s)
        src = self.src.at[2 * at.zl + at.x, self.part(s)] if d == 0 and r == 0 else dst
        m = d if up or d == 0 else at.layers - 1 + d
        return remote(src, dst, self.ys.at[0], self.yr.at[m], at.ypeer)

    def x_copy(self, t, s, receive=False):
        at = self.at
        src = self.src.at[2 * t + 1 - at.x, self.part(s)]
        dst = self.slot(t, at.z, at.y, 1 - at.x if receive else at.x, s)
        return remote(src, dst, self.xs.at[0], self.xr.at[t * self.split + s], at.xpeer)

    def send_z(self, r, s, which=FAR + NEAR, only=True):
        for k in which:
            self.z_send(True, 0, r, 1 - k, s, only=only)
            self.z_send(False, 0, r, k, s, only=only)

    def start_x(self):
        for s in range(self.split):
            for t in range(2):
                self.x_copy(t, s).start()

    def wait_x(self, s):
        for t in range(2):
            self.x_copy(t, s, True).wait_recv()

    def send_y(self, r, s, only=True):
        @pl.when(only)
        def _():
            self.y_copy(True, 0, r, s, self.at.y).start()

    def on_z(self, d, r, s, which=FAR + NEAR, sides=BOTH, only=True):
        z, layers, zl = self.at.z, self.at.layers, self.at.zl

        def arrive(up, t):
            if up:
                here = (z >= d) if t else (z >= d) & (z + 1 < layers)
            else:
                here = (z + d < layers) & (z >= 1) if t else (z + d < layers)
            if sides == PAIR:
                here = here & (zl == (1 if up else 0))
            elif sides == APART:
                here = here & (zl == (0 if up else 1))

            @pl.when(here & only)
            def _():
                self.z_copy(up, d, r, t, s, d - 1).wait_recv()
                self.z_send(up, d, r, t, s)

                @pl.when(zl == t)
                def _():
                    self.y_copy(up, d, r, s, self.at.y).start()

        for k in which:
            arrive(True, 1 - k)
            arrive(False, k)

    def on_y(self, d, sides=BOTH, up=None):
        z, layers, y, zl = self.at.z, self.at.layers, self.at.y, self.at.zl

        def each(up):
            ref = self.buf.at[zl, self.origin(up, d), 1 - y]
            m = d if up or d == 0 else layers - 1 + d
            remote(ref, ref, self.ys.at[0], self.yr.at[m], self.at.ypeer).wait_recv()

        if d == 0 or up is not None:
            each(up is not False)
            return
        from_below, from_above = z >= d, z + d < layers
        if sides != BOTH:
            near = 1 if sides == PAIR else 0
            from_below, from_above = from_below & (zl == near), from_above & (zl == 1 - near)

        @pl.when(from_below)
        def _():
            each(True)

        @pl.when(from_above)
        def _():
            each(False)

    def finish(self):
        at = self.at
        layers = at.layers

        def sent(ref, sem):
            remote(ref, ref, sem, self.yr.at[0], at.ypeer).wait_send()

        sent(self.buf.at[0, 0, 0], self.xs.at[0])
        sent(self.buf.at[0, :, 0], self.ys.at[0])
        for up in (True, False):
            for t in range(2):
                for z in range(layers):
                    beyond = layers - z if up else z + 1
                    if beyond > (1 if (t == 1) == up else 2):
                        number = z + 1 if up else layers - z

                        @pl.when(at.z == z)
                        def _():
                            sent(self.buf.at[0, pl.ds(0, number), 0], self.zs.at[(0 if up else 2) + t])


def join(weights, out_ref):
    for p in range(PLANE):
        pieces = []
        for ref in weights:
            width = ref.shape[1] // PLANE
            pieces.append(ref[:, p * width : (p + 1) * width])
        out_ref[p] = jnp.concatenate(pieces, axis=1)


class Place:
    def __init__(self, count):
        me, core = lax.axis_index("sp"), lax.axis_index("tp")
        self.me, self.core, self.layers = me, core, count // PLANE
        self.z, self.y, self.x = me // PLANE, lax.rem(me // 2, 2), lax.rem(me, 2)
        self.zl, self.zh = lax.rem(self.z, 2), self.z // 2
        self.spot = 2 * self.zl + self.x

        def device(sp, tp=core):
            return {"sp": sp, "tp": tp}

        self.partner = device(me, 1 - core)
        self.xpeer = device(me + 1 - 2 * self.x)
        self.ypeer = device(me + 2 - 4 * self.y)
        self.zpeer = device(me + PLANE * (1 - 2 * self.zl))
        self.above, self.below = device(me + PLANE), device(me - PLANE)
        self.after, self.prior = device(me + PLANE + 2), device(me - PLANE - 2)
        self.has_after = (self.y == 1) & (self.zh + 1 < self.layers // 2)
        self.has_prior = (self.y == 0) & (self.zh > 0)

    def greet(self):
        barrier = pltpu.get_barrier_semaphore()

        def signal(target):
            pl.semaphore_signal(barrier, inc=1, device_id=target, device_id_type=MESH)

        for target in (self.partner, self.xpeer, self.ypeer):
            signal(target)
        number = 3
        for go, target in (
            (self.z + 1 < self.layers, self.above),
            (self.z > 0, self.below),
            (self.has_after, self.after),
            (self.has_prior, self.prior),
        ):
            pl.when(go)(functools.partial(signal, target))
            number = number + jnp.where(go, 1, 0)
        return lambda: pl.semaphore_wait(barrier, number)


def remote(src, dst, send_sem, recv_sem, target):
    return pltpu.make_async_remote_copy(
        src_ref=src, dst_ref=dst, send_sem=send_sem, recv_sem=recv_sem, device_id=target, device_id_type=MESH
    )


def layer_entry(
    count, chans, wide, split, slopes_ref, sinks_ref, tok_hbm, *refs,
):
    raw_hbm, (gain_hbm, taps_hbm, out_hbm, far_hbm), refs = refs[:8], refs[8:12], refs[12:]
    raw, refs = refs[:8], refs[8:]
    layer_kernel(count, chans, wide, split, slopes_ref, sinks_ref, tok_hbm, raw_hbm, gain_hbm, taps_hbm, out_hbm, far_hbm, raw, *refs)


def layer_kernel(
    count, chans, wide, split, slopes_ref, sinks_ref, tok_hbm, raw_hbm, gain_hbm, taps_hbm, out_hbm, far_hbm, raw,
    gain_ref, taps_ref, w_ref, o_ref, out_ref, ls, os, x_ref, nrm_ref, wbuf, obuf, acc_ref, ext, gext, bias, hid, dsend, drecv, own, s1, r1, s2,
    wzs, wzr, wys, wyr, wxs, wxr, ozs, ozr, oys, oyr, oxs, oxr, ts, tr, hs, hr, ds, dr, fs, fr, gs, gr,
):
    f32, bf16 = jnp.float32, jnp.bfloat16
    at = Place(count)
    core, layers, x, y, z, zl, zh, spot = at.core, at.layers, at.x, at.y, at.z, at.zl, at.zh, at.spot
    rows, half = tok_hbm.shape
    length = 2 * rows
    group = wide // HEAD
    front = 8
    ins = Stream(at, w_ref, wbuf, (wzs, wzr, wys, wyr, wxs, wxr), split)
    outs = Stream(at, o_ref, obuf, (ozs, ozr, oys, oyr, oxs, oxr), 1)
    arrived = at.greet()

    def block(p, side=None):
        return x_ref.at[core if side is None else side, pl.ds(pl.multiple_of(p * rows, rows), rows)]

    p_own, p_x, p_z, p_far = spot, 2 * zl + 1 - x, 2 * (1 - zl) + x, 2 * (1 - zl) + 1 - x
    loads = [
        pltpu.make_async_copy(src, dst, ls.at[k])
        for k, (src, dst) in enumerate(
            list(zip(raw_hbm[:6], raw[:6]))
            + [(tok_hbm, block(p_own))]
            + list(zip(raw_hbm[6:], raw[6:]))
            + [(gain_hbm, gain_ref), (taps_hbm, taps_ref)]
        )
    ]
    for load in loads:
        load.start()
    for load in loads[:6]:
        load.wait()
    join(raw[:6], w_ref)
    loads[6].wait()
    arrived()
    at_end = (z == 0) | (z == layers - 1)
    inside = jnp.logical_not(at_end)
    ins.send_z(0, 0, FAR)
    ins.start_x()
    ins.send_y(0, 0)
    ins.send_y(0, 1)
    ins.send_z(0, 1, FAR)
    ins.send_z(0, 0, NEAR)
    ins.send_z(0, 1, NEAR, at_end)
    def half_block(p, n):
        return x_ref.at[core, pl.ds(pl.multiple_of(p * rows + n * (rows // 2), rows // 2), rows // 2)]

    def tok_z(n, p=p_own):
        return remote(half_block(p, n), half_block(p, n), ts.at[0], tr.at[1 + n], at.zpeer)

    def tok_far(n, p=p_z):
        return remote(half_block(p, n), half_block(p, n), ts.at[0], tr.at[3 + n], at.xpeer)

    def send_tok_z(n, only):
        @pl.when(only)
        def _():
            tok_z(n).start()

    tok_x = remote(block(p_own), block(p_own), ts.at[0], tr.at[0], at.xpeer)
    swaps = [
        remote(block(p), block(p), ts.at[1], tr.at[5 + k], at.partner)
        for k, p in enumerate((p_own, p_x, p_z, p_far))
    ]
    tok_x.start()
    tok_z(0).start()
    swaps[0].start()
    wbuf[zl, z, y, x] = w_ref[2 * zl + x]
    for load in loads[7:]:
        load.wait()
    join(raw[6:], o_ref)
    obuf[zl, z, y, x] = o_ref[2 * zl + x]
    span = 2 * half // layers
    strip = 32

    def normalise(k, p):
        remote(block(p, core), block(p, 1 - core), ts.at[1], tr.at[5 + k], at.partner).wait_recv()

        def step(i, carry):
            at_rows = pl.ds(pl.multiple_of(p * rows + i * strip, strip), strip)
            whole = jnp.concatenate([x_ref[0, at_rows, :], x_ref[1, at_rows, :]], axis=1).astype(f32)
            mean = jnp.sum(whole * whole, axis=1, keepdims=True) / (2 * half)
            scaled = (whole * lax.rsqrt(mean + 1e-06) * gain_ref[...]).astype(bf16)
            for j in range(layers):
                nrm_ref[j, at_rows, :] = scaled[:, j * span : (j + 1) * span]
            return carry

        lax.fori_loop(0, rows // strip, step, 0)

    def add_layer(origin, fresh):
        def step(i, carry):
            at_rows = pl.ds(pl.multiple_of(i * rows, rows), rows)
            product = jnp.dot(
                nrm_ref[origin, at_rows, :],
                wbuf[zl, origin].reshape(span, wbuf.shape[5]),
                preferred_element_type=f32,
            )
            acc_ref[at_rows, :] = product if fresh else acc_ref[at_rows, :] + product
            return carry

        lax.fori_loop(0, PLANE, step, 0)

    def add_row(origin, row_y, first=0, stride=1):
        size = span // 2

        def step(i, carry):
            at_rows = pl.ds(pl.multiple_of((first + stride * i) * rows, rows), rows)
            acc_ref[at_rows, :] += jnp.dot(
                nrm_ref[origin, at_rows, pl.ds(pl.multiple_of(row_y * size, size), size)],
                wbuf[zl, origin, row_y].reshape(size, wbuf.shape[5]),
                preferred_element_type=f32,
            )
            return carry

        lax.fori_loop(0, PLANE // stride, step, 0)

    def add_last(rest=False):
        def two(d, up):
            if rest:
                add_row(ins.origin(up, d), 1 - y, 0, 2)
                return
            add_row(ins.origin(up, d), y)
            ins.on_y(d, up=up)
            add_row(ins.origin(up, d), 1 - y, 1, 2)

        for above in (False, True):
            for d, where in ((3, at_end), (2, inside)):
                mine = (z >= d) if above else (z + d < layers)

                @pl.when(mine & where)
                def _():
                    two(d, above)

    def add_both(d):
        ins.on_y(d)

        @pl.when(z >= d)
        def _():
            add_layer(z - d, False)

        @pl.when(z + d < layers)
        def _():
            add_layer(z + d, False)

    def from_x(s):
        ins.wait_x(s)
        ins.send_z(1, s, FAR)
        ins.send_z(1, s, NEAR, at_end)
        ins.send_y(1, s)
        ins.on_z(1, 0, s, FAR)

    from_x(0)
    send_tok_z(1, at_end)
    ins.on_z(1, 0, 0, NEAR, APART)
    from_x(1)
    send_tok_z(1, inside)
    ins.send_z(0, 1, NEAR, inside)
    for s in range(split):
        ins.send_z(1, s, NEAR, inside)
    outs.send_y(0, 0, inside)
    normalise(0, p_own)
    ins.on_z(1, 1, 0, FAR, PAIR, at_end)
    ins.on_z(2, 0, 0, FAR, only=at_end)
    ins.on_z(1, 1, 0, FAR, APART)
    ins.on_z(2, 0, 0, FAR, only=inside)
    ins.on_z(1, 1, 1, FAR, APART)
    tok_z(0, p_z).wait_recv()
    tok_far(0).start()
    ins.on_z(2, 0, 1, FAR, only=inside)
    ins.on_z(1, 1, 1, FAR, PAIR, at_end)
    ins.on_z(1, 0, 1, NEAR, APART)
    ins.on_z(1, 1, 0, FAR, PAIR, inside)
    for s in range(split):
        ins.on_z(1, 0, s, NEAR, PAIR)
    remote(block(p_x), block(p_x), ts.at[0], tr.at[0], at.xpeer).wait_recv()
    swaps[1].start()
    ins.on_z(2, 0, 1, FAR, only=at_end)
    outs.send_y(0, 0, at_end)
    ins.on_z(1, 1, 0, NEAR, APART)
    normalise(1, p_x)
    ins.on_z(1, 1, 1, NEAR, APART)
    tok_z(1, p_z).wait_recv()
    tok_far(1).start()
    swaps[2].start()
    outs.start_x()
    ins.on_z(2, 1, 0, FAR, only=inside)
    ins.on_z(2, 1, 0, FAR, only=at_end)
    normalise(2, p_z)
    ins.on_z(2, 0, 0, NEAR, only=inside)
    ins.on_z(1, 1, 1, FAR, PAIR, inside)
    for s in range(split):
        ins.on_z(1, 1, s, NEAR, PAIR)
    ins.on_z(3, 0, 0)
    outs.send_z(0, 0, only=at_end)
    ins.on_z(2, 0, 1, NEAR, only=inside)
    tok_far(0, p_far).wait_recv()
    tok_far(1, p_far).wait_recv()
    swaps[3].start()
    ins.on_z(2, 1, 1, FAR)
    ins.on_z(3, 0, 1)
    normalise(3, p_far)
    ins.on_z(2, 1, 0, NEAR, only=inside)
    ins.on_z(3, 1, 0)
    ins.on_y(0)
    add_layer(z, True)
    ins.on_z(2, 1, 1, NEAR, only=inside)
    outs.wait_x(0)
    outs.on_z(1, 0, 0, FAR, PAIR, inside)
    outs.send_z(0, 0, FAR, inside)
    outs.send_z(1, 0, FAR)
    outs.send_z(1, 0, NEAR, at_end)
    outs.send_y(1, 0, inside)
    ins.on_z(3, 1, 1)
    add_both(1)
    outs.send_y(1, 0, at_end)
    outs.on_z(1, 1, 0, FAR, PAIR, inside)
    outs.on_z(2, 0, 0, FAR, only=inside)

    @pl.when(at_end)
    def _():
        add_both(2)

    outs.on_z(1, 0, 0, FAR, APART)
    add_last()

    blocks = 2 * length // WINDOW

    def mix_spread(some):
        for i in some:
            run, start = i // 4, i % 4 * WINDOW
            here = pl.ds(i * WINDOW, WINDOW)
            ext[run, pl.ds(start + WINDOW, WINDOW), :] = acc_ref[here, 3 * chans + wide :].astype(bf16)
            both = acc_ref[here, chans : 3 * chans].astype(bf16).astype(f32)
            gext[run, pl.ds(start + front, WINDOW), :] = (both[:, :chans] * both[:, chans:]).astype(bf16).astype(f32)

    tail_blocks = range(blocks // 2 - 1, blocks, blocks // 2)
    mix_spread(tail_blocks)

    def tails(run, after, target, action):
        kv = remote(
            ext.at[run, pl.ds(length, WINDOW)], ext.at[after, pl.ds(0, WINDOW)],
            hs.at[2 * run], hr.at[2 * after], target,
        )
        gated = remote(
            gext.at[run, pl.ds(length, front)], gext.at[after, pl.ds(0, front)],
            hs.at[2 * run + 1], hr.at[2 * after + 1], target,
        )
        for copy in (kv, gated):
            getattr(copy, action)()

    def all_tails(action):
        @pl.when(y == 0)
        def _():
            for run in range(2):
                tails(run, run, at.ypeer, action)

        @pl.when(y == 1)
        def _():
            tails(0, 1, at.ypeer, action)

        @pl.when(at.has_after)
        def _():
            tails(1, 0, at.after, action)

    all_tails("start")
    for r in range(2):
        outs.on_z(1, r, 0, FAR, PAIR, at_end)
    add_last(True)
    mix_spread([i for i in range(blocks) if i not in tail_blocks])
    outs.on_z(3, 0, 0)
    for r in range(2):
        outs.on_z(1, r, 0, NEAR, PAIR)
        outs.send_z(r, 0, NEAR, inside)
    first_run = (y == 0) & (zh == 0)

    @pl.when(first_run)
    def _():
        ext[0, 0:WINDOW, :] = jnp.zeros((WINDOW, 2 * HEAD), bf16)
        gext[0, 0:front, :] = jnp.zeros((front, chans), f32)

    taps = sum(jnp.where(spot == c, taps_ref[:, c * chans : (c + 1) * chans], 0.0) for c in range(PLANE))
    row = lax.broadcasted_iota(jnp.int32, (WINDOW, 2 * WINDOW), 0)
    col = lax.broadcasted_iota(jnp.int32, (WINDOW, 2 * WINDOW), 1)
    dist = WINDOW + row - col
    near = (dist >= 0) & (dist < WINDOW)
    far = dist.astype(f32)

    for g in range(group):
        bias[g] = jnp.where(near, -slopes_ref[(core * PLANE + spot) * group + g] * far, -1e30)
    ones = jnp.where(lax.broadcasted_iota(jnp.int32, (2 * WINDOW, HEAD), 1) == 0, 1.0, 0.0).astype(bf16)

    def mix(run, blk, first=False):
        start = pl.multiple_of(blk * WINDOW, WINDOW)
        chunk = acc_ref[pl.ds(pl.multiple_of(run * length + start, WINDOW), WINDOW), :].astype(bf16)
        window = gext[run, pl.ds(start, WINDOW + front), :]
        conv = sum(
            taps[k : k + 1, :] * window[front - TAPS + 1 + k : front - TAPS + 1 + k + WINDOW]
            for k in range(TAPS)
        )
        pieces = [(chunk[:, :chans].astype(f32) * conv).astype(bf16)]
        kv = ext[run, pl.ds(start, 2 * WINDOW), :]
        keys, values = kv[:, :HEAD], jnp.concatenate([kv[:, HEAD:], ones], axis=1)
        offset = ((2 * zh + run) * 2 + y) * length
        for g in range(group):
            at_head = 3 * chans + g * HEAD
            query = chunk[:, at_head : at_head + HEAD] * jnp.asarray(HEAD ** (-0.5), bf16)
            scores = bias[g] + lax.dot_general(
                query, keys, (((1,), (1,)), ((), ())), preferred_element_type=f32
            )
            if first:
                scores = jnp.where(offset - WINDOW + col >= 0, scores, -1e30)
            sink = sinks_ref[spot * group + g]
            top = jnp.maximum(jnp.max(scores, axis=1, keepdims=True), sink)
            expo = jnp.exp(scores - top).astype(bf16)
            summed = jnp.dot(expo, values, preferred_element_type=f32)
            total = summed[:, HEAD : HEAD + 1] + jnp.exp(sink - top)
            pieces.append((summed[:, :HEAD] / total).astype(bf16))
        place = pl.ds(pl.multiple_of((2 * run + blk // 2) * WINDOW, WINDOW), WINDOW)
        hid[lax.rem(blk, 2), place, :] = jnp.concatenate(pieces, axis=1)

    def mix_run(run):
        for blk in range(1, 4):
            mix(run, blk)

    def mix_first():
        for run in range(2):
            mix(run, 0, True)

    outs.on_z(1, 1, 0, FAR, APART)
    mix_run(0)
    outs.on_z(2, 1, 0, FAR, only=inside)
    mix_run(1)

    def tails_in(after, target):
        for k, (ref, size) in enumerate(((ext, WINDOW), (gext, front))):
            remote(
                ref.at[after, pl.ds(length, size)], ref.at[after, pl.ds(0, size)],
                hs.at[2 * after + k], hr.at[2 * after + k], target,
            ).wait_recv()

    @pl.when(y == 1)
    def _():
        tails_in(0, at.ypeer)

    @pl.when(at.has_prior)
    def _():
        tails_in(0, at.prior)

    tails_in(1, at.ypeer)
    mix_first()

    lower = z < layers // 2
    cols = obuf.shape[3] * obuf.shape[4]
    order = [(0, True), (1, True), (0, False), (1, False), (3, True), (2, True), (3, False), (2, False)]
    chunks = len(order)

    def chunk_at(h):
        i, mine = order[h]
        return jnp.where(lower, i, layers - 1 - i), y if mine else 1 - y

    def product(side, h):
        layer, row_y = chunk_at(h)
        return lax.dot_general(
            hid[side], obuf[zl, layer, row_y].reshape(cols, hid.shape[2]),
            (((1,), (1,)), ((), ())), preferred_element_type=f32,
        )

    def slab(p):
        return pl.ds(pl.multiple_of(p * WINDOW, WINDOW), WINDOW)

    def swap(i):
        return remote(dsend.at[i], drecv.at[i], ds.at[0], dr.at[i], at.partner)

    def first_hop(i, j):
        if i % 2 == 0:
            target, p = at.xpeer, (2 * (1 - zl) if j == 0 else 2 * zl) + 1 - x
        else:
            target, p = at.zpeer, 2 * (1 - zl) + ((1 - x) if j == 0 else x)
        return remote(s1.at[i, slab(p)], r1.at[i, j], fs.at[0], fr.at[2 * i + j], target)

    def out_slab(i):
        layer, row_y = chunk_at(i)
        return pl.ds(pl.multiple_of((layer * 2 + row_y) * cols, cols), cols)

    def second_hop(i):
        return remote(s2.at[i], far_hbm.at[:, out_slab(i)], gs.at[0], gr.at[i], at.zpeer if i % 2 == 0 else at.xpeer)

    def begin(i):
        dsend[i] = product(1 - core, i).astype(bf16)
        own[i % 2] = product(core, i)
        swap(i).start()

    def fold(i):
        swap(i).wait_recv()
        s1[i] = (own[i % 2] + drecv[i].astype(f32)).astype(bf16)
        first_hop(i, 0).start()
        first_hop(i, 1).start()

    def relay(i):
        first_hop(i, 0).wait_recv()
        p = p_z if i % 2 == 0 else p_x
        s2[i] = (s1[i, slab(p), :].astype(f32) + r1[i, 0].astype(f32)).astype(bf16)
        second_hop(i).start()

    def out_copy(i):
        return pltpu.make_async_copy(out_ref.at[i], out_hbm.at[:, out_slab(i)], os.at[0])

    def collect(i):
        first_hop(i, 1).wait_recv()
        total = s1[i, slab(p_own), :].astype(f32) + r1[i, 1].astype(f32)
        out_ref[i] = total.astype(out_ref.dtype)
        out_copy(i).start()

    begin(0)
    outs.on_z(2, 0, 0, FAR, only=at_end)
    begin(1)
    fold(0)
    fold(1)
    outs.on_z(2, 1, 0, FAR, only=at_end)
    outs.on_z(2, 0, 0, NEAR, only=inside)
    outs.on_y(0)
    outs.on_y(1, sides=PAIR)
    begin(2)
    outs.on_z(1, 0, 0, NEAR, APART)
    outs.on_z(3, 1, 0)
    begin(3)
    fold(2)
    fold(3)
    outs.on_z(1, 1, 0, NEAR, APART)
    relay(0)
    outs.on_z(2, 1, 0, NEAR, only=inside)
    begin(4)
    relay(1)
    begin(5)
    fold(4)
    fold(5)
    collect(0)
    collect(1)
    relay(2)
    relay(3)
    outs.on_y(2)
    outs.on_y(3)
    begin(6)
    outs.on_y(1, sides=APART)
    begin(7)
    fold(6)
    fold(7)
    collect(2)
    collect(3)
    for h in range(4, chunks):
        relay(h)
        collect(h)

    def phase_finish():
        pltpu.make_async_copy(out_ref, out_ref, os.at[0]).wait()
        for h in range(chunks):
            second_hop(h).wait_recv()
        ins.finish()
        outs.finish()
        all_tails("wait_send")
        for ref, sem in (
            (x_ref.at[0, pl.ds(0, 3 * rows)], ts.at[0]),
            (x_ref.at[0], ts.at[1]),
            (dsend, ds.at[0]),
            (s1.at[pl.ds(0, chunks // 2)], fs.at[0]),
            (s2, gs.at[0]),
        ):
            remote(ref, ref, sem, dr.at[0], at.partner).wait_send()

    phase_finish()


def whole_layer(count, tokens, weights, gain, taps, slopes, sinks, wide):
    layers = count // PLANE
    rows, half = tokens.shape
    depth = weights[0].shape[0]
    width = sum(w.shape[1] for w in weights[:6]) // PLANE
    cols = weights[6].shape[0]
    inner = sum(w.shape[1] for w in weights[6:]) // PLANE
    chans = taps.shape[1] // PLANE
    bf16, f32 = jnp.bfloat16, jnp.float32
    dma = pltpu.SemaphoreType.DMA
    split = 2
    length = 2 * rows
    slab = 2 * cols
    chunks = 2 * layers

    def sems(parts):
        hops = 2 * (layers - 1) * 4 * parts
        return [dma((number,)) for number in (4, hops, 1, 2 * layers - 1, 1, 2 * parts)]

    smem = pl.BlockSpec(memory_space=pltpu.SMEM)
    return pl.pallas_call(
        functools.partial(layer_entry, count, chans, wide, split),
        out_shape=[jax.ShapeDtypeStruct((rows // 2, 2 * half), bf16)] * 2,
        in_specs=[smem] * 2 + [pl.BlockSpec(memory_space=pltpu.HBM)] * 11,
        out_specs=[pl.BlockSpec(memory_space=pltpu.HBM)] * 2,
        scratch_shapes=[pltpu.VMEM(w.shape, bf16) for w in weights]
        + [
            pltpu.VMEM(gain.shape, f32),
            pltpu.VMEM(taps.shape, f32),
            pltpu.VMEM((PLANE, depth, width), bf16),
            pltpu.VMEM((PLANE, cols, inner), bf16),
            pltpu.VMEM((chunks, WINDOW, slab), bf16),
            dma((11,)),
            dma((1,)),
            pltpu.VMEM((2, PLANE * rows, half), bf16),
            pltpu.VMEM((layers, PLANE * rows, 2 * half // layers), bf16),
            pltpu.VMEM((2, layers, 2, 2, depth, width), bf16),
            pltpu.VMEM((2, layers, 2, 2, cols, inner), bf16),
            pltpu.VMEM((PLANE * rows, width), f32),
            pltpu.VMEM((2, WINDOW + length, 2 * HEAD), bf16),
            pltpu.VMEM((2, 8 + length, chans), f32),
            pltpu.VMEM((QHEADS // KVHEADS, WINDOW, 2 * WINDOW), f32),
            pltpu.VMEM((2, PLANE * WINDOW, inner), bf16),
            pltpu.VMEM((chunks, PLANE * WINDOW, slab), bf16),
            pltpu.VMEM((chunks, PLANE * WINDOW, slab), bf16),
            pltpu.VMEM((2, PLANE * WINDOW, slab), f32),
            pltpu.VMEM((chunks, PLANE * WINDOW, slab), bf16),
            pltpu.VMEM((chunks, 2, WINDOW, slab), bf16),
            pltpu.VMEM((chunks, WINDOW, slab), bf16),
        ]
        + sems(split)
        + sems(1)
        + [dma((number,)) for number in (2, 9, 4, 4, 1, chunks, 1, 2 * chunks, 1, chunks)],
        compiler_params=pltpu.CompilerParams(
            collective_id=0, has_side_effects=True, vmem_limit_bytes=60 << 20
        ),
    )(slopes, sinks, tokens, *weights, gain, taps)


def add_kernel(a_ref, b_ref, out_ref):
    out_ref[...] = (a_ref[...].astype(jnp.float32) + b_ref[...].astype(jnp.float32)).astype(out_ref.dtype)


def add_pair(a, b):
    rows, cols = a.shape
    spec = pl.BlockSpec((rows // 2, cols), lambda i: (i, 0))
    return pl.pallas_call(
        add_kernel, grid=(2,), in_specs=[spec] * 2, out_specs=spec, out_shape=jax.ShapeDtypeStruct(a.shape, a.dtype)
    )(a, b)


def plane_body(
    tokens,
    norm_gain,
    outer_gate_w,
    inner_gate_w,
    signal_w,
    conv_taps,
    query_w,
    key_w,
    value_w,
    sink_logits,
    out_conv_w,
    out_attn_w,
):
    if tokens.shape[0] != 2 * WINDOW:
        return body(
            tokens, norm_gain, outer_gate_w, inner_gate_w, signal_w, conv_taps,
            query_w, key_w, value_w, sink_logits, out_conv_w, out_attn_w,
        )
    count = lax.axis_size("sp")
    wide = query_w.shape[1] // PLANE
    weights = (outer_gate_w, inner_gate_w, signal_w, query_w, key_w, value_w, out_conv_w.T, out_attn_w.T)
    slopes = jnp.array([2.0 ** (-8.0 * h / QHEADS) for h in range(1, QHEADS + 1)], jnp.float32)
    near, far = whole_layer(
        count, tokens, weights, norm_gain.reshape(1, -1), conv_taps, slopes, sink_logits, wide
    )
    return add_pair(near, far)


def solution(mesh):
    kv_local = KVHEADS // mesh.shape["tp"]
    fits = mesh.shape["tp"] == 2 and kv_local == PLANE and mesh.shape["sp"] == LAYERS * PLANE
    chosen = plane_body if fits else body
    in_specs = (
        P("sp", "tp"),
        P(),
        P("sp", "tp"),
        P("sp", "tp"),
        P("sp", "tp"),
        P(None, "tp"),
        P("sp", "tp"),
        P("sp", "tp"),
        P("sp", "tp"),
        P("tp"),
        P("tp", "sp"),
        P("tp", "sp"),
    )
    out_specs = P(("sp", "tp"), None)
    return jax.shard_map(chosen, mesh=mesh, in_specs=in_specs, out_specs=out_specs, check_vma=False)
```

```python
import functools

import jax
import jax.numpy as jnp
from jax import lax
from jax.experimental import pallas as pl
from jax.experimental.pallas import tpu as pltpu
from jax.sharding import PartitionSpec as P

QHEADS = 24
KVHEADS = 8
HEAD = 64
TAPS = 3
WINDOW = 128
PLANE = 4
LAYERS = 4
PAIR, APART, BOTH = 1, 2, 3
FAR, NEAR = (0,), (1,)
MESH = pl.DeviceIdType.MESH


def from_behind(value, axis, steps):
    count = lax.axis_size(axis)
    initial, last = (max(0, -steps), min(count, count - steps))
    return lax.ppermute(value, axis, [(source, source + steps) for source in range(initial, last)])


def add_products(pieces, normed):
    return tuple((jnp.dot(normed, piece, preferred_element_type=jnp.float32) for piece in pieces))


def convolve(gated, before, outer, conv_taps):
    extended = jnp.concatenate([before, gated], axis=0).astype(jnp.float32)
    length = gated.shape[0]
    conv = sum((conv_taps[k] * extended[k : k + length] for k in range(conv_taps.shape[0])))
    return (outer.astype(jnp.float32) * conv).astype(jnp.bfloat16)


def attention(queries, keys_ext, values_ext, sink_logits, offset):
    f32 = jnp.float32
    length = queries.shape[0]
    kv_local = keys_ext.shape[1] // HEAD
    group = QHEADS // KVHEADS
    heads_local = kv_local * group
    span = min(512, length)
    first = lax.axis_index("tp") * heads_local + 1
    slopes = jnp.exp2(
        -8.0 * (first + jnp.arange(heads_local, dtype=jnp.int32)).astype(f32) / QHEADS
    ).reshape(kv_local, group)
    sinks = sink_logits.reshape(kv_local, group)[:, :, None]

    def attend(block):
        start = block * span
        qblock = queries.reshape(span, kv_local, group, HEAD)
        kblock = keys_ext.reshape(span + WINDOW, kv_local, HEAD)
        vblock = values_ext.reshape(span + WINDOW, kv_local, HEAD)
        scores = jnp.einsum(
            "qhgd,shd->hgqs", qblock, kblock, preferred_element_type=f32
        ) * HEAD ** (-0.5)
        qpos = offset + start + jnp.arange(span, dtype=jnp.int32)
        kpos = offset + start - WINDOW + jnp.arange(span + WINDOW, dtype=jnp.int32)
        dist = qpos[:, None] - kpos[None, :]
        valid = (dist >= 0) & (dist < WINDOW) & (kpos >= 0)[None, :]
        scores = scores - slopes[:, :, None, None] * dist.astype(f32)
        scores = jnp.where(valid, scores, -1e30)
        top = jnp.maximum(jnp.max(scores, axis=-1), sinks)
        expo = jnp.exp(scores - top[..., None])
        total = jnp.sum(expo, axis=-1) + jnp.exp(sinks - top)
        probs = (expo / total[..., None]).astype(jnp.bfloat16)
        out = jnp.einsum("hgqs,shd->qhgd", probs, vblock, preferred_element_type=f32)
        return out.reshape(span, heads_local * HEAD)

    blocks = lax.map(attend, jnp.arange(length // span, dtype=jnp.int32))
    return blocks.reshape(length, heads_local * HEAD).astype(jnp.bfloat16)


def body(
    tokens,
    norm_gain,
    outer_gate_w,
    inner_gate_w,
    signal_w,
    conv_taps,
    query_w,
    key_w,
    value_w,
    sink_logits,
    out_conv_w,
    out_attn_w,
):
    f32 = jnp.float32
    bf16 = jnp.bfloat16
    whole = lax.all_gather(tokens, "tp", axis=1, tiled=True)
    x32 = whole.astype(f32)
    normed = (
        x32 * lax.rsqrt(jnp.mean(x32 * x32, axis=-1, keepdims=True) + 1e-06) * norm_gain
    ).astype(bf16)
    length = normed.shape[0]
    offset = lax.axis_index("sp") * length

    def fold_rows(pieces):
        return add_products(pieces, normed)

    conv_weights = (outer_gate_w, inner_gate_w, signal_w)
    conv_results = fold_rows(
        (
            lax.all_gather(conv_weights[0], "sp", axis=0, tiled=True),
            lax.all_gather(conv_weights[1], "sp", axis=0, tiled=True),
            lax.all_gather(conv_weights[2], "sp", axis=0, tiled=True),
        )
    )
    outer, inner, signal = tuple((result.astype(bf16) for result in conv_results))
    gated = (inner.astype(f32) * signal.astype(f32)).astype(bf16)
    before = from_behind(gated[length - TAPS + 1 :], "sp", 1)
    conv_out = convolve(gated, before, outer, conv_taps)
    attn_weights = (query_w, key_w, value_w)
    attn_results = fold_rows(
        (
            lax.all_gather(attn_weights[0], "sp", axis=0, tiled=True),
            lax.all_gather(attn_weights[1], "sp", axis=0, tiled=True),
            lax.all_gather(attn_weights[2], "sp", axis=0, tiled=True),
        )
    )
    queries, keys, values = tuple((result.astype(bf16) for result in attn_results))
    keys_before, values_before = from_behind(
        (keys[length - WINDOW :], values[length - WINDOW :]), "sp", 1
    )
    keys_ext = jnp.concatenate([keys_before, keys], axis=0)
    values_ext = jnp.concatenate([values_before, values], axis=0)
    attn_out = attention(queries, keys_ext, values_ext, sink_logits, offset)
    conv_whole, attn_whole = (
        lax.all_gather(out_conv_w, "sp", axis=1, tiled=True),
        lax.all_gather(out_attn_w, "sp", axis=1, tiled=True),
    )
    result = jnp.dot(conv_out, conv_whole, preferred_element_type=f32)
    mixed = lax.psum_scatter(
        (result + jnp.dot(attn_out, attn_whole, preferred_element_type=f32)).astype(jnp.bfloat16),
        "tp",
        scatter_dimension=0,
        tiled=True,
    ).astype(jnp.float32)
    return mixed.astype(bf16)

class Stream:
    def __init__(self, at, src, buf, sems, split):
        self.at, self.src, self.buf, self.split = at, src, buf, split
        self.zs, self.zr, self.ys, self.yr, self.xs, self.xr = sems
        self.rows = src.shape[1] // split

    def part(self, s):
        return pl.ds(s * self.rows, self.rows)

    def slot(self, t, origin, y, x, s):
        return self.buf.at[t, origin, y, x, self.part(s)]

    def origin(self, up, d):
        return self.at.z - d if up else self.at.z + d

    def column(self, r):
        return self.at.x if r == 0 else 1 - self.at.x

    def z_copy(self, up, d, r, t, s, send_d):
        at = self.at
        dst = self.slot(t, self.origin(up, d), at.y, self.column(r), s)
        src = self.src.at[2 * t + at.x, self.part(s)] if d == 0 and r == 0 else dst
        side = 0 if up else 1
        i = (((side * (at.layers - 1) + send_d) * 2 + r) * 2 + t) * self.split + s
        return remote(src, dst, self.zs.at[2 * side + t], self.zr.at[i], at.above if up else at.below)

    def z_send(self, up, d, r, t, s, only=True):
        z, layers = self.at.z, self.at.layers
        if d >= layers - 1:
            return
        if up:
            go = (z >= d) & (z + (1 if t else 2) < layers)
        else:
            go = (z + d < layers) & (z >= (2 if t else 1))

        @pl.when(go & only)
        def _():
            self.z_copy(up, d, r, t, s, d).start()

    def y_copy(self, up, d, r, s, y):
        at = self.at
        dst = self.slot(at.zl, self.origin(up, d), y, self.column(r), s)
        src = self.src.at[2 * at.zl + at.x, self.part(s)] if d == 0 and r == 0 else dst
        m = d if up or d == 0 else at.layers - 1 + d
        return remote(src, dst, self.ys.at[0], self.yr.at[m], at.ypeer)

    def x_copy(self, t, s, receive=False):
        at = self.at
        src = self.src.at[2 * t + 1 - at.x, self.part(s)]
        dst = self.slot(t, at.z, at.y, 1 - at.x if receive else at.x, s)
        return remote(src, dst, self.xs.at[0], self.xr.at[t * self.split + s], at.xpeer)

    def send_z(self, r, s, which=FAR + NEAR, only=True):
        for k in which:
            self.z_send(True, 0, r, 1 - k, s, only=only)
            self.z_send(False, 0, r, k, s, only=only)

    def start_x(self):
        for s in range(self.split):
            for t in range(2):
                self.x_copy(t, s).start()

    def wait_x(self, s):
        for t in range(2):
            self.x_copy(t, s, True).wait_recv()

    def send_y(self, r, s, only=True):
        @pl.when(only)
        def _():
            self.y_copy(True, 0, r, s, self.at.y).start()

    def on_z(self, d, r, s, which=FAR + NEAR, sides=BOTH, only=True):
        z, layers, zl = self.at.z, self.at.layers, self.at.zl

        def arrive(up, t):
            if up:
                here = (z >= d) if t else (z >= d) & (z + 1 < layers)
            else:
                here = (z + d < layers) & (z >= 1) if t else (z + d < layers)
            if sides == PAIR:
                here = here & (zl == (1 if up else 0))
            elif sides == APART:
                here = here & (zl == (0 if up else 1))

            @pl.when(here & only)
            def _():
                self.z_copy(up, d, r, t, s, d - 1).wait_recv()
                self.z_send(up, d, r, t, s)

                @pl.when(zl == t)
                def _():
                    self.y_copy(up, d, r, s, self.at.y).start()

        for k in which:
            arrive(True, 1 - k)
            arrive(False, k)

    def on_y(self, d, sides=BOTH, up=None):
        z, layers, y, zl = self.at.z, self.at.layers, self.at.y, self.at.zl

        def each(up):
            ref = self.buf.at[zl, self.origin(up, d), 1 - y]
            m = d if up or d == 0 else layers - 1 + d
            remote(ref, ref, self.ys.at[0], self.yr.at[m], self.at.ypeer).wait_recv()

        if d == 0 or up is not None:
            each(up is not False)
            return
        from_below, from_above = z >= d, z + d < layers
        if sides != BOTH:
            near = 1 if sides == PAIR else 0
            from_below, from_above = from_below & (zl == near), from_above & (zl == 1 - near)

        @pl.when(from_below)
        def _():
            each(True)

        @pl.when(from_above)
        def _():
            each(False)

    def finish(self):
        at = self.at
        layers = at.layers

        def sent(ref, sem):
            remote(ref, ref, sem, self.yr.at[0], at.ypeer).wait_send()

        sent(self.buf.at[0, 0, 0], self.xs.at[0])
        sent(self.buf.at[0, :, 0], self.ys.at[0])
        for up in (True, False):
            for t in range(2):
                for z in range(layers):
                    beyond = layers - z if up else z + 1
                    if beyond > (1 if (t == 1) == up else 2):
                        number = z + 1 if up else layers - z

                        @pl.when(at.z == z)
                        def _():
                            sent(self.buf.at[0, pl.ds(0, number), 0], self.zs.at[(0 if up else 2) + t])


def join(weights, out_ref):
    for p in range(PLANE):
        pieces = []
        for ref in weights:
            width = ref.shape[1] // PLANE
            pieces.append(ref[:, p * width : (p + 1) * width])
        out_ref[p] = jnp.concatenate(pieces, axis=1)


class Place:
    def __init__(self, count):
        me, core = lax.axis_index("sp"), lax.axis_index("tp")
        self.me, self.core, self.layers = me, core, count // PLANE
        self.z, self.y, self.x = me // PLANE, lax.rem(me // 2, 2), lax.rem(me, 2)
        self.zl, self.zh = lax.rem(self.z, 2), self.z // 2
        self.spot = 2 * self.zl + self.x

        def device(sp, tp=core):
            return {"sp": sp, "tp": tp}

        self.partner = device(me, 1 - core)
        self.xpeer = device(me + 1 - 2 * self.x)
        self.ypeer = device(me + 2 - 4 * self.y)
        self.zpeer = device(me + PLANE * (1 - 2 * self.zl))
        self.above, self.below = device(me + PLANE), device(me - PLANE)
        self.after, self.prior = device(me + PLANE + 2), device(me - PLANE - 2)
        self.has_after = (self.y == 1) & (self.zh + 1 < self.layers // 2)
        self.has_prior = (self.y == 0) & (self.zh > 0)

    def greet(self):
        barrier = pltpu.get_barrier_semaphore()

        def signal(target):
            pl.semaphore_signal(barrier, inc=1, device_id=target, device_id_type=MESH)

        for target in (self.partner, self.xpeer, self.ypeer):
            signal(target)
        number = 3
        for go, target in (
            (self.z + 1 < self.layers, self.above),
            (self.z > 0, self.below),
            (self.has_after, self.after),
            (self.has_prior, self.prior),
        ):
            pl.when(go)(functools.partial(signal, target))
            number = number + jnp.where(go, 1, 0)
        return lambda: pl.semaphore_wait(barrier, number)


def remote(src, dst, send_sem, recv_sem, target):
    return pltpu.make_async_remote_copy(
        src_ref=src, dst_ref=dst, send_sem=send_sem, recv_sem=recv_sem, device_id=target, device_id_type=MESH
    )


def layer_entry(
    count, chans, wide, split, slopes_ref, sinks_ref, tok_hbm, *refs,
):
    raw_hbm, (gain_hbm, taps_hbm, out_hbm, far_hbm), refs = refs[:8], refs[8:12], refs[12:]
    raw, refs = refs[:8], refs[8:]
    layer_kernel(count, chans, wide, split, slopes_ref, sinks_ref, tok_hbm, raw_hbm, gain_hbm, taps_hbm, out_hbm, far_hbm, raw, *refs)


def layer_kernel(
    count, chans, wide, split, slopes_ref, sinks_ref, tok_hbm, raw_hbm, gain_hbm, taps_hbm, out_hbm, far_hbm, raw,
    gain_ref, taps_ref, w_ref, o_ref, out_ref, ls, os, x_ref, nrm_ref, wbuf, obuf, acc_ref, ext, gext, bias, hid, dsend, drecv, own, s1, r1, s2,
    wzs, wzr, wys, wyr, wxs, wxr, ozs, ozr, oys, oyr, oxs, oxr, ts, tr, hs, hr, ds, dr, fs, fr, gs, gr,
):
    f32, bf16 = jnp.float32, jnp.bfloat16
    at = Place(count)
    core, layers, x, y, z, zl, zh, spot = at.core, at.layers, at.x, at.y, at.z, at.zl, at.zh, at.spot
    rows, half = tok_hbm.shape
    length = 2 * rows
    group = wide // HEAD
    front = 8
    ins = Stream(at, w_ref, wbuf, (wzs, wzr, wys, wyr, wxs, wxr), split)
    outs = Stream(at, o_ref, obuf, (ozs, ozr, oys, oyr, oxs, oxr), 1)
    arrived = at.greet()

    def block(p, side=None):
        return x_ref.at[core if side is None else side, pl.ds(pl.multiple_of(p * rows, rows), rows)]

    p_own, p_x, p_z, p_far = spot, 2 * zl + 1 - x, 2 * (1 - zl) + x, 2 * (1 - zl) + 1 - x
    loads = [
        pltpu.make_async_copy(src, dst, ls.at[k])
        for k, (src, dst) in enumerate(
            list(zip(raw_hbm[:6], raw[:6]))
            + [(tok_hbm, block(p_own))]
            + list(zip(raw_hbm[6:], raw[6:]))
            + [(gain_hbm, gain_ref), (taps_hbm, taps_ref)]
        )
    ]
    for load in loads:
        load.start()
    for load in loads[:6]:
        load.wait()
    join(raw[:6], w_ref)
    loads[6].wait()
    arrived()
    at_end = (z == 0) | (z == layers - 1)
    inside = jnp.logical_not(at_end)
    ins.send_z(0, 0, FAR)
    ins.start_x()
    ins.send_y(0, 0)
    ins.send_y(0, 1)
    ins.send_z(0, 1, FAR)
    ins.send_z(0, 0, NEAR)
    ins.send_z(0, 1, NEAR, at_end)
    def half_block(p, n):
        return x_ref.at[core, pl.ds(pl.multiple_of(p * rows + n * (rows // 2), rows // 2), rows // 2)]

    def tok_z(n, p=p_own):
        return remote(half_block(p, n), half_block(p, n), ts.at[0], tr.at[1 + n], at.zpeer)

    def tok_far(n, p=p_z):
        return remote(half_block(p, n), half_block(p, n), ts.at[0], tr.at[3 + n], at.xpeer)

    def send_tok_z(n, only):
        @pl.when(only)
        def _():
            tok_z(n).start()

    tok_x = remote(block(p_own), block(p_own), ts.at[0], tr.at[0], at.xpeer)
    swaps = [
        remote(block(p), block(p), ts.at[1], tr.at[5 + k], at.partner)
        for k, p in enumerate((p_own, p_x, p_z, p_far))
    ]
    tok_x.start()
    tok_z(0).start()
    swaps[0].start()
    wbuf[zl, z, y, x] = w_ref[2 * zl + x]
    for load in loads[7:]:
        load.wait()
    join(raw[6:], o_ref)
    obuf[zl, z, y, x] = o_ref[2 * zl + x]
    span = 2 * half // layers
    strip = 32

    def normalise(k, p):
        remote(block(p, core), block(p, 1 - core), ts.at[1], tr.at[5 + k], at.partner).wait_recv()

        def step(i, carry):
            at_rows = pl.ds(pl.multiple_of(p * rows + i * strip, strip), strip)
            whole = jnp.concatenate([x_ref[0, at_rows, :], x_ref[1, at_rows, :]], axis=1).astype(f32)
            mean = jnp.sum(whole * whole, axis=1, keepdims=True) / (2 * half)
            scaled = (whole * lax.rsqrt(mean + 1e-06) * gain_ref[...]).astype(bf16)
            for j in range(layers):
                nrm_ref[j, at_rows, :] = scaled[:, j * span : (j + 1) * span]
            return carry

        lax.fori_loop(0, rows // strip, step, 0)

    def add_layer(origin, fresh):
        def step(i, carry):
            at_rows = pl.ds(pl.multiple_of(i * rows, rows), rows)
            product = jnp.dot(
                nrm_ref[origin, at_rows, :],
                wbuf[zl, origin].reshape(span, wbuf.shape[5]),
                preferred_element_type=f32,
            )
            acc_ref[at_rows, :] = product if fresh else acc_ref[at_rows, :] + product
            return carry

        lax.fori_loop(0, PLANE, step, 0)

    def add_row(origin, row_y, first=0, stride=1):
        size = span // 2

        def step(i, carry):
            at_rows = pl.ds(pl.multiple_of((first + stride * i) * rows, rows), rows)
            acc_ref[at_rows, :] += jnp.dot(
                nrm_ref[origin, at_rows, pl.ds(pl.multiple_of(row_y * size, size), size)],
                wbuf[zl, origin, row_y].reshape(size, wbuf.shape[5]),
                preferred_element_type=f32,
            )
            return carry

        lax.fori_loop(0, PLANE // stride, step, 0)

    def add_last(rest=False):
        def two(d, up):
            if rest:
                add_row(ins.origin(up, d), 1 - y, 0, 2)
                return
            add_row(ins.origin(up, d), y)
            ins.on_y(d, up=up)
            add_row(ins.origin(up, d), 1 - y, 1, 2)

        for above in (False, True):
            for d, where in ((3, at_end), (2, inside)):
                mine = (z >= d) if above else (z + d < layers)

                @pl.when(mine & where)
                def _():
                    two(d, above)

    def add_both(d):
        ins.on_y(d)

        @pl.when(z >= d)
        def _():
            add_layer(z - d, False)

        @pl.when(z + d < layers)
        def _():
            add_layer(z + d, False)

    def from_x(s):
        ins.wait_x(s)
        ins.send_z(1, s, FAR)
        ins.send_z(1, s, NEAR, at_end)
        ins.send_y(1, s)
        ins.on_z(1, 0, s, FAR)

    from_x(0)
    send_tok_z(1, at_end)
    ins.on_z(1, 0, 0, NEAR, APART)
    from_x(1)
    send_tok_z(1, inside)
    ins.send_z(0, 1, NEAR, inside)
    for s in range(split):
        ins.send_z(1, s, NEAR, inside)
    outs.send_y(0, 0, inside)
    normalise(0, p_own)
    ins.on_z(1, 1, 0, FAR, PAIR, at_end)
    ins.on_z(2, 0, 0, FAR, only=at_end)
    ins.on_z(1, 1, 0, FAR, APART)
    ins.on_z(2, 0, 0, FAR, only=inside)
    ins.on_z(1, 1, 1, FAR, APART)
    tok_z(0, p_z).wait_recv()
    tok_far(0).start()
    ins.on_z(2, 0, 1, FAR, only=inside)
    ins.on_z(1, 1, 1, FAR, PAIR, at_end)
    ins.on_z(1, 0, 1, NEAR, APART)
    ins.on_z(1, 1, 0, FAR, PAIR, inside)
    for s in range(split):
        ins.on_z(1, 0, s, NEAR, PAIR)
    remote(block(p_x), block(p_x), ts.at[0], tr.at[0], at.xpeer).wait_recv()
    swaps[1].start()
    ins.on_z(2, 0, 1, FAR, only=at_end)
    outs.send_y(0, 0, at_end)
    ins.on_z(1, 1, 0, NEAR, APART)
    normalise(1, p_x)
    ins.on_z(1, 1, 1, NEAR, APART)
    tok_z(1, p_z).wait_recv()
    tok_far(1).start()
    swaps[2].start()
    outs.start_x()
    ins.on_z(2, 1, 0, FAR, only=inside)
    ins.on_z(2, 1, 0, FAR, only=at_end)
    normalise(2, p_z)
    ins.on_z(2, 0, 0, NEAR, only=inside)
    ins.on_z(1, 1, 1, FAR, PAIR, inside)
    for s in range(split):
        ins.on_z(1, 1, s, NEAR, PAIR)
    ins.on_z(3, 0, 0)
    outs.send_z(0, 0, only=at_end)
    ins.on_z(2, 0, 1, NEAR, only=inside)
    tok_far(0, p_far).wait_recv()
    tok_far(1, p_far).wait_recv()
    swaps[3].start()
    ins.on_z(2, 1, 1, FAR)
    ins.on_z(3, 0, 1)
    normalise(3, p_far)
    ins.on_z(2, 1, 0, NEAR, only=inside)
    ins.on_z(3, 1, 0)
    ins.on_y(0)
    add_layer(z, True)
    ins.on_z(2, 1, 1, NEAR, only=inside)
    outs.wait_x(0)
    outs.on_z(1, 0, 0, FAR, PAIR, inside)
    outs.send_z(0, 0, FAR, inside)
    outs.send_z(1, 0, FAR)
    outs.send_z(1, 0, NEAR, at_end)
    outs.send_y(1, 0, inside)
    ins.on_z(3, 1, 1)
    add_both(1)
    outs.send_y(1, 0, at_end & (core == 0))
    outs.on_z(1, 1, 0, FAR, PAIR, inside)
    outs.on_z(2, 0, 0, FAR, only=inside)

    @pl.when(at_end)
    def _():
        add_both(2)

    outs.on_z(1, 0, 0, FAR, APART)
    add_last()

    blocks = 2 * length // WINDOW

    def mix_spread(some):
        for i in some:
            run, start = i // 4, i % 4 * WINDOW
            here = pl.ds(i * WINDOW, WINDOW)
            ext[run, pl.ds(start + WINDOW, WINDOW), :] = acc_ref[here, 3 * chans + wide :].astype(bf16)
            both = acc_ref[here, chans : 3 * chans].astype(bf16).astype(f32)
            gext[run, pl.ds(start + front, WINDOW), :] = (both[:, :chans] * both[:, chans:]).astype(bf16).astype(f32)

    tail_blocks = range(blocks // 2 - 1, blocks, blocks // 2)
    mix_spread(tail_blocks)

    def tails(run, after, target, action):
        kv = remote(
            ext.at[run, pl.ds(length, WINDOW)], ext.at[after, pl.ds(0, WINDOW)],
            hs.at[2 * run], hr.at[2 * after], target,
        )
        gated = remote(
            gext.at[run, pl.ds(length, front)], gext.at[after, pl.ds(0, front)],
            hs.at[2 * run + 1], hr.at[2 * after + 1], target,
        )
        for copy in (kv, gated):
            getattr(copy, action)()

    def all_tails(action):
        @pl.when(y == 0)
        def _():
            for run in range(2):
                tails(run, run, at.ypeer, action)

        @pl.when(y == 1)
        def _():
            tails(0, 1, at.ypeer, action)

        @pl.when(at.has_after)
        def _():
            tails(1, 0, at.after, action)

    all_tails("start")
    outs.send_y(1, 0, at_end & (core == 1))
    for r in range(2):
        outs.on_z(1, r, 0, FAR, PAIR, at_end)
    add_last(True)
    mix_spread([i for i in range(blocks) if i not in tail_blocks])
    outs.on_z(3, 0, 0)
    for r in range(2):
        outs.on_z(1, r, 0, NEAR, PAIR)
        outs.send_z(r, 0, NEAR, inside)
    first_run = (y == 0) & (zh == 0)

    @pl.when(first_run)
    def _():
        ext[0, 0:WINDOW, :] = jnp.zeros((WINDOW, 2 * HEAD), bf16)
        gext[0, 0:front, :] = jnp.zeros((front, chans), f32)

    taps = sum(jnp.where(spot == c, taps_ref[:, c * chans : (c + 1) * chans], 0.0) for c in range(PLANE))
    row = lax.broadcasted_iota(jnp.int32, (WINDOW, 2 * WINDOW), 0)
    col = lax.broadcasted_iota(jnp.int32, (WINDOW, 2 * WINDOW), 1)
    dist = WINDOW + row - col
    near = (dist >= 0) & (dist < WINDOW)
    far = dist.astype(f32)

    for g in range(group):
        bias[g] = jnp.where(near, -slopes_ref[(core * PLANE + spot) * group + g] * far, -1e30)
    ones = jnp.where(lax.broadcasted_iota(jnp.int32, (2 * WINDOW, HEAD), 1) == 0, 1.0, 0.0).astype(bf16)

    def mix(run, blk, first=False):
        start = pl.multiple_of(blk * WINDOW, WINDOW)
        chunk = acc_ref[pl.ds(pl.multiple_of(run * length + start, WINDOW), WINDOW), :].astype(bf16)
        window = gext[run, pl.ds(start, WINDOW + front), :]
        conv = sum(
            taps[k : k + 1, :] * window[front - TAPS + 1 + k : front - TAPS + 1 + k + WINDOW]
            for k in range(TAPS)
        )
        pieces = [(chunk[:, :chans].astype(f32) * conv).astype(bf16)]
        kv = ext[run, pl.ds(start, 2 * WINDOW), :]
        keys, values = kv[:, :HEAD], jnp.concatenate([kv[:, HEAD:], ones], axis=1)
        offset = ((2 * zh + run) * 2 + y) * length
        for g in range(group):
            at_head = 3 * chans + g * HEAD
            query = chunk[:, at_head : at_head + HEAD] * jnp.asarray(HEAD ** (-0.5), bf16)
            scores = bias[g] + lax.dot_general(
                query, keys, (((1,), (1,)), ((), ())), preferred_element_type=f32
            )
            if first:
                scores = jnp.where(offset - WINDOW + col >= 0, scores, -1e30)
            sink = sinks_ref[spot * group + g]
            top = jnp.maximum(jnp.max(scores, axis=1, keepdims=True), sink)
            expo = jnp.exp(scores - top).astype(bf16)
            summed = jnp.dot(expo, values, preferred_element_type=f32)
            total = summed[:, HEAD : HEAD + 1] + jnp.exp(sink - top)
            pieces.append((summed[:, :HEAD] / total).astype(bf16))
        place = pl.ds(pl.multiple_of((2 * run + blk // 2) * WINDOW, WINDOW), WINDOW)
        hid[lax.rem(blk, 2), place, :] = jnp.concatenate(pieces, axis=1)

    def mix_run(run):
        for blk in range(1, 4):
            mix(run, blk)

    def mix_first():
        for run in range(2):
            mix(run, 0, True)

    outs.on_z(1, 1, 0, FAR, APART)
    mix_run(0)
    outs.on_z(2, 1, 0, FAR, only=inside)
    mix_run(1)

    def tails_in(after, target):
        for k, (ref, size) in enumerate(((ext, WINDOW), (gext, front))):
            remote(
                ref.at[after, pl.ds(length, size)], ref.at[after, pl.ds(0, size)],
                hs.at[2 * after + k], hr.at[2 * after + k], target,
            ).wait_recv()

    @pl.when(y == 1)
    def _():
        tails_in(0, at.ypeer)

    @pl.when(at.has_prior)
    def _():
        tails_in(0, at.prior)

    tails_in(1, at.ypeer)
    mix_first()

    lower = z < layers // 2
    cols = obuf.shape[3] * obuf.shape[4]
    order = [(0, True), (1, True), (0, False), (1, False), (3, True), (2, True), (3, False), (2, False)]
    chunks = len(order)

    def chunk_at(h):
        i, mine = order[h]
        return jnp.where(lower, i, layers - 1 - i), y if mine else 1 - y

    def product(side, h):
        layer, row_y = chunk_at(h)
        return lax.dot_general(
            hid[side], obuf[zl, layer, row_y].reshape(cols, hid.shape[2]),
            (((1,), (1,)), ((), ())), preferred_element_type=f32,
        )

    def slab(p):
        return pl.ds(pl.multiple_of(p * WINDOW, WINDOW), WINDOW)

    def swap(i):
        return remote(dsend.at[i], drecv.at[i], ds.at[0], dr.at[i], at.partner)

    def first_hop(i, j):
        if i % 2 == 0:
            target, p = at.xpeer, (2 * (1 - zl) if j == 0 else 2 * zl) + 1 - x
        else:
            target, p = at.zpeer, 2 * (1 - zl) + ((1 - x) if j == 0 else x)
        return remote(s1.at[i, slab(p)], r1.at[i, j], fs.at[0], fr.at[2 * i + j], target)

    def out_slab(i):
        layer, row_y = chunk_at(i)
        return pl.ds(pl.multiple_of((layer * 2 + row_y) * cols, cols), cols)

    def second_hop(i):
        return remote(s2.at[i], far_hbm.at[:, out_slab(i)], gs.at[0], gr.at[i], at.zpeer if i % 2 == 0 else at.xpeer)

    def begin(i):
        dsend[i] = product(1 - core, i).astype(bf16)
        own[i % 2] = product(core, i)
        swap(i).start()

    def fold(i):
        swap(i).wait_recv()
        s1[i] = (own[i % 2] + drecv[i].astype(f32)).astype(bf16)
        first_hop(i, 0).start()
        first_hop(i, 1).start()

    def relay(i):
        first_hop(i, 0).wait_recv()
        p = p_z if i % 2 == 0 else p_x
        s2[i] = (s1[i, slab(p), :].astype(f32) + r1[i, 0].astype(f32)).astype(bf16)
        second_hop(i).start()

    def out_copy(i):
        return pltpu.make_async_copy(out_ref.at[i], out_hbm.at[:, out_slab(i)], os.at[0])

    def collect(i):
        first_hop(i, 1).wait_recv()
        total = s1[i, slab(p_own), :].astype(f32) + r1[i, 1].astype(f32)
        out_ref[i] = total.astype(out_ref.dtype)
        out_copy(i).start()

    begin(0)
    outs.on_z(2, 0, 0, FAR, only=at_end)
    begin(1)
    fold(0)
    fold(1)
    outs.on_z(2, 1, 0, FAR, only=at_end)
    outs.on_z(2, 0, 0, NEAR, only=inside)
    outs.on_y(0)
    outs.on_y(1, sides=PAIR)
    begin(2)
    outs.on_z(1, 0, 0, NEAR, APART)
    outs.on_z(3, 1, 0)
    begin(3)
    fold(2)
    fold(3)
    outs.on_z(1, 1, 0, NEAR, APART)
    outs.on_z(2, 1, 0, NEAR, only=inside)
    begin(4)
    begin(5)
    fold(4)
    relay(0)
    fold(5)
    relay(1)
    collect(0)
    collect(1)
    relay(2)
    relay(3)
    outs.on_y(2)
    outs.on_y(3)
    begin(6)
    outs.on_y(1, sides=APART)
    begin(7)
    fold(6)
    fold(7)
    collect(2)
    collect(3)
    for h in range(4, chunks):
        relay(h)
        collect(h)

    def phase_finish():
        pltpu.make_async_copy(out_ref, out_ref, os.at[0]).wait()
        for h in range(chunks):
            second_hop(h).wait_recv()
        ins.finish()
        outs.finish()
        all_tails("wait_send")
        for ref, sem in (
            (x_ref.at[0, pl.ds(0, 3 * rows)], ts.at[0]),
            (x_ref.at[0], ts.at[1]),
            (dsend, ds.at[0]),
            (s1.at[pl.ds(0, chunks // 2)], fs.at[0]),
            (s2, gs.at[0]),
        ):
            remote(ref, ref, sem, dr.at[0], at.partner).wait_send()

    phase_finish()


def whole_layer(count, tokens, weights, gain, taps, slopes, sinks, wide):
    layers = count // PLANE
    rows, half = tokens.shape
    depth = weights[0].shape[0]
    width = sum(w.shape[1] for w in weights[:6]) // PLANE
    cols = weights[6].shape[0]
    inner = sum(w.shape[1] for w in weights[6:]) // PLANE
    chans = taps.shape[1] // PLANE
    bf16, f32 = jnp.bfloat16, jnp.float32
    dma = pltpu.SemaphoreType.DMA
    split = 2
    length = 2 * rows
    slab = 2 * cols
    chunks = 2 * layers

    def sems(parts):
        hops = 2 * (layers - 1) * 4 * parts
        return [dma((number,)) for number in (4, hops, 1, 2 * layers - 1, 1, 2 * parts)]

    smem = pl.BlockSpec(memory_space=pltpu.SMEM)
    return pl.pallas_call(
        functools.partial(layer_entry, count, chans, wide, split),
        out_shape=[jax.ShapeDtypeStruct((rows // 2, 2 * half), bf16)] * 2,
        in_specs=[smem] * 2 + [pl.BlockSpec(memory_space=pltpu.HBM)] * 11,
        out_specs=[pl.BlockSpec(memory_space=pltpu.HBM)] * 2,
        scratch_shapes=[pltpu.VMEM(w.shape, bf16) for w in weights]
        + [
            pltpu.VMEM(gain.shape, f32),
            pltpu.VMEM(taps.shape, f32),
            pltpu.VMEM((PLANE, depth, width), bf16),
            pltpu.VMEM((PLANE, cols, inner), bf16),
            pltpu.VMEM((chunks, WINDOW, slab), bf16),
            dma((11,)),
            dma((1,)),
            pltpu.VMEM((2, PLANE * rows, half), bf16),
            pltpu.VMEM((layers, PLANE * rows, 2 * half // layers), bf16),
            pltpu.VMEM((2, layers, 2, 2, depth, width), bf16),
            pltpu.VMEM((2, layers, 2, 2, cols, inner), bf16),
            pltpu.VMEM((PLANE * rows, width), f32),
            pltpu.VMEM((2, WINDOW + length, 2 * HEAD), bf16),
            pltpu.VMEM((2, 8 + length, chans), f32),
            pltpu.VMEM((QHEADS // KVHEADS, WINDOW, 2 * WINDOW), f32),
            pltpu.VMEM((2, PLANE * WINDOW, inner), bf16),
            pltpu.VMEM((chunks, PLANE * WINDOW, slab), bf16),
            pltpu.VMEM((chunks, PLANE * WINDOW, slab), bf16),
            pltpu.VMEM((2, PLANE * WINDOW, slab), f32),
            pltpu.VMEM((chunks, PLANE * WINDOW, slab), bf16),
            pltpu.VMEM((chunks, 2, WINDOW, slab), bf16),
            pltpu.VMEM((chunks, WINDOW, slab), bf16),
        ]
        + sems(split)
        + sems(1)
        + [dma((number,)) for number in (2, 9, 4, 4, 1, chunks, 1, 2 * chunks, 1, chunks)],
        compiler_params=pltpu.CompilerParams(
            collective_id=0, has_side_effects=True, vmem_limit_bytes=60 << 20
        ),
    )(slopes, sinks, tokens, *weights, gain, taps)


def add_kernel(a_ref, b_ref, out_ref):
    out_ref[...] = (a_ref[...].astype(jnp.float32) + b_ref[...].astype(jnp.float32)).astype(out_ref.dtype)


def add_pair(a, b):
    rows, cols = a.shape
    spec = pl.BlockSpec((rows // 2, cols), lambda i: (i, 0))
    return pl.pallas_call(
        add_kernel, grid=(2,), in_specs=[spec] * 2, out_specs=spec, out_shape=jax.ShapeDtypeStruct(a.shape, a.dtype)
    )(a, b)


def plane_body(
    tokens,
    norm_gain,
    outer_gate_w,
    inner_gate_w,
    signal_w,
    conv_taps,
    query_w,
    key_w,
    value_w,
    sink_logits,
    out_conv_w,
    out_attn_w,
):
    if tokens.shape[0] != 2 * WINDOW:
        return body(
            tokens, norm_gain, outer_gate_w, inner_gate_w, signal_w, conv_taps,
            query_w, key_w, value_w, sink_logits, out_conv_w, out_attn_w,
        )
    count = lax.axis_size("sp")
    wide = query_w.shape[1] // PLANE
    weights = (outer_gate_w, inner_gate_w, signal_w, query_w, key_w, value_w, out_conv_w.T, out_attn_w.T)
    slopes = jnp.array([2.0 ** (-8.0 * h / QHEADS) for h in range(1, QHEADS + 1)], jnp.float32)
    near, far = whole_layer(
        count, tokens, weights, norm_gain.reshape(1, -1), conv_taps, slopes, sink_logits, wide
    )
    return add_pair(near, far)


def solution(mesh):
    kv_local = KVHEADS // mesh.shape["tp"]
    fits = mesh.shape["tp"] == 2 and kv_local == PLANE and mesh.shape["sp"] == LAYERS * PLANE
    chosen = plane_body if fits else body
    in_specs = (
        P("sp", "tp"),
        P(),
        P("sp", "tp"),
        P("sp", "tp"),
        P("sp", "tp"),
        P(None, "tp"),
        P("sp", "tp"),
        P("sp", "tp"),
        P("sp", "tp"),
        P("tp"),
        P("tp", "sp"),
        P("tp", "sp"),
    )
    out_specs = P(("sp", "tp"), None)
    return jax.shard_map(chosen, mesh=mesh, in_specs=in_specs, out_specs=out_specs, check_vma=False)
```

```python
import functools

import jax
import jax.numpy as jnp
from jax import lax
from jax.experimental import pallas as pl
from jax.experimental.pallas import tpu as pltpu
from jax.sharding import PartitionSpec as P

QHEADS = 24
KVHEADS = 8
HEAD = 64
TAPS = 3
WINDOW = 128
PLANE = 4
LAYERS = 4
PAIR, APART, BOTH = 1, 2, 3
FAR, NEAR = (0,), (1,)
MESH = pl.DeviceIdType.MESH


def from_behind(value, axis, steps):
    count = lax.axis_size(axis)
    initial, last = (max(0, -steps), min(count, count - steps))
    return lax.ppermute(value, axis, [(source, source + steps) for source in range(initial, last)])


def add_products(pieces, normed):
    return tuple((jnp.dot(normed, piece, preferred_element_type=jnp.float32) for piece in pieces))


def convolve(gated, before, outer, conv_taps):
    extended = jnp.concatenate([before, gated], axis=0).astype(jnp.float32)
    length = gated.shape[0]
    conv = sum((conv_taps[k] * extended[k : k + length] for k in range(conv_taps.shape[0])))
    return (outer.astype(jnp.float32) * conv).astype(jnp.bfloat16)


def attention(queries, keys_ext, values_ext, sink_logits, offset):
    f32 = jnp.float32
    length = queries.shape[0]
    kv_local = keys_ext.shape[1] // HEAD
    group = QHEADS // KVHEADS
    heads_local = kv_local * group
    span = min(512, length)
    first = lax.axis_index("tp") * heads_local + 1
    slopes = jnp.exp2(
        -8.0 * (first + jnp.arange(heads_local, dtype=jnp.int32)).astype(f32) / QHEADS
    ).reshape(kv_local, group)
    sinks = sink_logits.reshape(kv_local, group)[:, :, None]

    def attend(block):
        start = block * span
        qblock = queries.reshape(span, kv_local, group, HEAD)
        kblock = keys_ext.reshape(span + WINDOW, kv_local, HEAD)
        vblock = values_ext.reshape(span + WINDOW, kv_local, HEAD)
        scores = jnp.einsum(
            "qhgd,shd->hgqs", qblock, kblock, preferred_element_type=f32
        ) * HEAD ** (-0.5)
        qpos = offset + start + jnp.arange(span, dtype=jnp.int32)
        kpos = offset + start - WINDOW + jnp.arange(span + WINDOW, dtype=jnp.int32)
        dist = qpos[:, None] - kpos[None, :]
        valid = (dist >= 0) & (dist < WINDOW) & (kpos >= 0)[None, :]
        scores = scores - slopes[:, :, None, None] * dist.astype(f32)
        scores = jnp.where(valid, scores, -1e30)
        top = jnp.maximum(jnp.max(scores, axis=-1), sinks)
        expo = jnp.exp(scores - top[..., None])
        total = jnp.sum(expo, axis=-1) + jnp.exp(sinks - top)
        probs = (expo / total[..., None]).astype(jnp.bfloat16)
        out = jnp.einsum("hgqs,shd->qhgd", probs, vblock, preferred_element_type=f32)
        return out.reshape(span, heads_local * HEAD)

    blocks = lax.map(attend, jnp.arange(length // span, dtype=jnp.int32))
    return blocks.reshape(length, heads_local * HEAD).astype(jnp.bfloat16)


def body(
    tokens,
    norm_gain,
    outer_gate_w,
    inner_gate_w,
    signal_w,
    conv_taps,
    query_w,
    key_w,
    value_w,
    sink_logits,
    out_conv_w,
    out_attn_w,
):
    f32 = jnp.float32
    bf16 = jnp.bfloat16
    whole = lax.all_gather(tokens, "tp", axis=1, tiled=True)
    x32 = whole.astype(f32)
    normed = (
        x32 * lax.rsqrt(jnp.mean(x32 * x32, axis=-1, keepdims=True) + 1e-06) * norm_gain
    ).astype(bf16)
    length = normed.shape[0]
    offset = lax.axis_index("sp") * length

    def fold_rows(pieces):
        return add_products(pieces, normed)

    conv_weights = (outer_gate_w, inner_gate_w, signal_w)
    conv_results = fold_rows(
        (
            lax.all_gather(conv_weights[0], "sp", axis=0, tiled=True),
            lax.all_gather(conv_weights[1], "sp", axis=0, tiled=True),
            lax.all_gather(conv_weights[2], "sp", axis=0, tiled=True),
        )
    )
    outer, inner, signal = tuple((result.astype(bf16) for result in conv_results))
    gated = (inner.astype(f32) * signal.astype(f32)).astype(bf16)
    before = from_behind(gated[length - TAPS + 1 :], "sp", 1)
    conv_out = convolve(gated, before, outer, conv_taps)
    attn_weights = (query_w, key_w, value_w)
    attn_results = fold_rows(
        (
            lax.all_gather(attn_weights[0], "sp", axis=0, tiled=True),
            lax.all_gather(attn_weights[1], "sp", axis=0, tiled=True),
            lax.all_gather(attn_weights[2], "sp", axis=0, tiled=True),
        )
    )
    queries, keys, values = tuple((result.astype(bf16) for result in attn_results))
    keys_before, values_before = from_behind(
        (keys[length - WINDOW :], values[length - WINDOW :]), "sp", 1
    )
    keys_ext = jnp.concatenate([keys_before, keys], axis=0)
    values_ext = jnp.concatenate([values_before, values], axis=0)
    attn_out = attention(queries, keys_ext, values_ext, sink_logits, offset)
    conv_whole, attn_whole = (
        lax.all_gather(out_conv_w, "sp", axis=1, tiled=True),
        lax.all_gather(out_attn_w, "sp", axis=1, tiled=True),
    )
    result = jnp.dot(conv_out, conv_whole, preferred_element_type=f32)
    mixed = lax.psum_scatter(
        (result + jnp.dot(attn_out, attn_whole, preferred_element_type=f32)).astype(jnp.bfloat16),
        "tp",
        scatter_dimension=0,
        tiled=True,
    ).astype(jnp.float32)
    return mixed.astype(bf16)

class Stream:
    def __init__(self, at, src, buf, sems, split):
        self.at, self.src, self.buf, self.split = at, src, buf, split
        self.zs, self.zr, self.ys, self.yr, self.xs, self.xr = sems
        self.rows = src.shape[1] // split

    def part(self, s):
        return pl.ds(s * self.rows, self.rows)

    def slot(self, t, origin, y, x, s):
        return self.buf.at[t, origin, y, x, self.part(s)]

    def origin(self, up, d):
        return self.at.z - d if up else self.at.z + d

    def column(self, r):
        return self.at.x if r == 0 else 1 - self.at.x

    def z_copy(self, up, d, r, t, s):
        at = self.at
        dst = self.slot(t, self.origin(up, d), at.y, self.column(r), s)
        src = self.src.at[2 * t + at.x, self.part(s)] if d == 0 and r == 0 else dst
        side = 0 if up else 1
        i = ((self.origin(up, d) * 2 + r) * 2 + t) * self.split + s
        return remote(src, dst, self.zs.at[2 * side + t], self.zr.at[i], at.above if up else at.below)

    def z_send(self, up, d, r, t, s, only=True):
        z, layers = self.at.z, self.at.layers
        if d >= layers - 1:
            return
        if up:
            go = (z >= d) & (z + (1 if t else 2) < layers)
        else:
            go = (z + d < layers) & (z >= (2 if t else 1))

        @pl.when(go & only)
        def _():
            self.z_copy(up, d, r, t, s).start()

    def y_copy(self, up, d, r, s, y):
        at = self.at
        dst = self.slot(at.zl, self.origin(up, d), y, self.column(r), s)
        src = self.src.at[2 * at.zl + at.x, self.part(s)] if d == 0 and r == 0 else dst
        m = self.origin(up, d)
        return remote(src, dst, self.ys.at[0], self.yr.at[m], at.ypeer)

    def x_copy(self, t, s, receive=False):
        at = self.at
        src = self.src.at[2 * t + 1 - at.x, self.part(s)]
        dst = self.slot(t, at.z, at.y, 1 - at.x if receive else at.x, s)
        return remote(src, dst, self.xs.at[0], self.xr.at[t * self.split + s], at.xpeer)

    def send_z(self, r, s, which=FAR + NEAR, only=True):
        for k in which:
            self.z_send(True, 0, r, 1 - k, s, only=only)
            self.z_send(False, 0, r, k, s, only=only)

    def start_x(self):
        for s in range(self.split):
            for t in range(2):
                self.x_copy(t, s).start()

    def wait_x(self, s):
        for t in range(2):
            self.x_copy(t, s, True).wait_recv()

    def send_y(self, r, s, only=True):
        @pl.when(only)
        def _():
            self.y_copy(True, 0, r, s, self.at.y).start()

    def on_z(self, d, r, s, which=FAR + NEAR, sides=BOTH, only=True):
        z, layers, zl = self.at.z, self.at.layers, self.at.zl

        def arrive(up, t):
            if up:
                here = (z >= d) if t else (z >= d) & (z + 1 < layers)
            else:
                here = (z + d < layers) & (z >= 1) if t else (z + d < layers)
            if sides == PAIR:
                here = here & (zl == (1 if up else 0))
            elif sides == APART:
                here = here & (zl == (0 if up else 1))

            @pl.when(here & only)
            def _():
                self.z_copy(up, d, r, t, s).wait_recv()
                self.z_send(up, d, r, t, s)

                @pl.when(zl == t)
                def _():
                    self.y_copy(up, d, r, s, self.at.y).start()

        for k in which:
            arrive(True, 1 - k)
            arrive(False, k)

    def on_y(self, d, sides=BOTH, up=None):
        z, layers, y, zl = self.at.z, self.at.layers, self.at.y, self.at.zl

        def each(up):
            ref = self.buf.at[zl, self.origin(up, d), 1 - y]
            m = self.origin(up, d)
            remote(ref, ref, self.ys.at[0], self.yr.at[m], self.at.ypeer).wait_recv()

        if d == 0 or up is not None:
            each(up is not False)
            return
        from_below, from_above = z >= d, z + d < layers
        if sides != BOTH:
            near = 1 if sides == PAIR else 0
            from_below, from_above = from_below & (zl == near), from_above & (zl == 1 - near)

        @pl.when(from_below)
        def _():
            each(True)

        @pl.when(from_above)
        def _():
            each(False)

    def finish(self):
        at = self.at
        layers = at.layers

        def sent(ref, sem):
            remote(ref, ref, sem, self.yr.at[0], at.ypeer).wait_send()

        sent(self.buf.at[0, 0, 0], self.xs.at[0])
        sent(self.buf.at[0, :, 0], self.ys.at[0])
        for up in (True, False):
            for t in range(2):
                for z in range(layers):
                    beyond = layers - z if up else z + 1
                    if beyond > (1 if (t == 1) == up else 2):
                        number = z + 1 if up else layers - z

                        @pl.when(at.z == z)
                        def _():
                            sent(self.buf.at[0, pl.ds(0, number), 0], self.zs.at[(0 if up else 2) + t])


def join(weights, out_ref):
    for p in range(PLANE):
        pieces = []
        for ref in weights:
            width = ref.shape[1] // PLANE
            pieces.append(ref[:, p * width : (p + 1) * width])
        out_ref[p] = jnp.concatenate(pieces, axis=1)


class Place:
    def __init__(self, count):
        me, core = lax.axis_index("sp"), lax.axis_index("tp")
        self.me, self.core, self.layers = me, core, count // PLANE
        self.z, self.y, self.x = me // PLANE, lax.rem(me // 2, 2), lax.rem(me, 2)
        self.zl, self.zh = lax.rem(self.z, 2), self.z // 2
        self.spot = 2 * self.zl + self.x

        def device(sp, tp=core):
            return {"sp": sp, "tp": tp}

        self.partner = device(me, 1 - core)
        self.xpeer = device(me + 1 - 2 * self.x)
        self.ypeer = device(me + 2 - 4 * self.y)
        self.zpeer = device(me + PLANE * (1 - 2 * self.zl))
        self.above, self.below = device(me + PLANE), device(me - PLANE)
        self.after, self.prior = device(me + PLANE + 2), device(me - PLANE - 2)
        self.has_after = (self.y == 1) & (self.zh + 1 < self.layers // 2)
        self.has_prior = (self.y == 0) & (self.zh > 0)

    def greet(self):
        barrier = pltpu.get_barrier_semaphore()

        def signal(target):
            pl.semaphore_signal(barrier, inc=1, device_id=target, device_id_type=MESH)

        for target in (self.partner, self.xpeer, self.ypeer):
            signal(target)
        number = 3
        for go, target in (
            (self.z + 1 < self.layers, self.above),
            (self.z > 0, self.below),
            (self.has_after, self.after),
            (self.has_prior, self.prior),
        ):
            pl.when(go)(functools.partial(signal, target))
            number = number + jnp.where(go, 1, 0)
        return lambda: pl.semaphore_wait(barrier, number)


def remote(src, dst, send_sem, recv_sem, target):
    return pltpu.make_async_remote_copy(
        src_ref=src, dst_ref=dst, send_sem=send_sem, recv_sem=recv_sem, device_id=target, device_id_type=MESH
    )


def layer_entry(
    count, chans, wide, split, slopes_ref, sinks_ref, tok_hbm, *refs,
):
    raw_hbm, (gain_hbm, taps_hbm, out_hbm, far_hbm), refs = refs[:8], refs[8:12], refs[12:]
    raw, refs = refs[:8], refs[8:]
    layer_kernel(count, chans, wide, split, slopes_ref, sinks_ref, tok_hbm, raw_hbm, gain_hbm, taps_hbm, out_hbm, far_hbm, raw, *refs)


def layer_kernel(
    count, chans, wide, split, slopes_ref, sinks_ref, tok_hbm, raw_hbm, gain_hbm, taps_hbm, out_hbm, far_hbm, raw,
    gain_ref, taps_ref, w_ref, o_ref, out_ref, ls, os, x_ref, nrm_ref, wbuf, obuf, acc_ref, ext, gext, bias, hid, dsend, drecv, own, s1, r1, s2,
    wzs, wzr, wys, wyr, wxs, wxr, ozs, ozr, oys, oyr, oxs, oxr, ts, tr, hs, hr, ds, dr, fs, fr, gs, gr,
):
    f32, bf16 = jnp.float32, jnp.bfloat16
    at = Place(count)
    core, layers, x, y, z, zl, zh, spot = at.core, at.layers, at.x, at.y, at.z, at.zl, at.zh, at.spot
    rows, half = tok_hbm.shape
    length = 2 * rows
    group = wide // HEAD
    front = 8
    ins = Stream(at, w_ref, wbuf, (wzs, wzr, wys, wyr, wxs, wxr), split)
    outs = Stream(at, o_ref, obuf, (ozs, ozr, oys, oyr, oxs, oxr), 1)
    arrived = at.greet()

    def block(p, side=None):
        return x_ref.at[core if side is None else side, pl.ds(pl.multiple_of(p * rows, rows), rows)]

    p_own, p_x, p_z, p_far = spot, 2 * zl + 1 - x, 2 * (1 - zl) + x, 2 * (1 - zl) + 1 - x
    loads = [
        pltpu.make_async_copy(src, dst, ls.at[k])
        for k, (src, dst) in enumerate(
            list(zip(raw_hbm[:6], raw[:6]))
            + [(tok_hbm, block(p_own))]
            + list(zip(raw_hbm[6:], raw[6:]))
            + [(gain_hbm, gain_ref), (taps_hbm, taps_ref)]
        )
    ]
    for load in loads:
        load.start()
    for load in loads[:6]:
        load.wait()
    join(raw[:6], w_ref)
    loads[6].wait()
    arrived()
    at_end = (z == 0) | (z == layers - 1)
    inside = jnp.logical_not(at_end)
    ins.send_z(0, 0, FAR)
    ins.start_x()
    ins.send_y(0, 0)
    ins.send_y(0, 1)
    ins.send_z(0, 1, FAR)
    ins.send_z(0, 0, NEAR)
    ins.send_z(0, 1, NEAR, at_end)
    def half_block(p, n):
        return x_ref.at[core, pl.ds(pl.multiple_of(p * rows + n * (rows // 2), rows // 2), rows // 2)]

    def tok_z(n, p=p_own):
        return remote(half_block(p, n), half_block(p, n), ts.at[0], tr.at[1 + n], at.zpeer)

    def tok_far(n, p=p_z):
        return remote(half_block(p, n), half_block(p, n), ts.at[0], tr.at[3 + n], at.xpeer)

    def send_tok_z(n, only):
        @pl.when(only)
        def _():
            tok_z(n).start()

    tok_x = remote(block(p_own), block(p_own), ts.at[0], tr.at[0], at.xpeer)
    swaps = [
        remote(block(p), block(p), ts.at[1], tr.at[5 + k], at.partner)
        for k, p in enumerate((p_own, p_x, p_z, p_far))
    ]
    tok_x.start()
    tok_z(0).start()
    swaps[0].start()
    wbuf[zl, z, y, x] = w_ref[2 * zl + x]
    for load in loads[7:]:
        load.wait()
    join(raw[6:], o_ref)
    obuf[zl, z, y, x] = o_ref[2 * zl + x]
    span = 2 * half // layers
    strip = 32

    def normalise(k, p):
        remote(block(p, core), block(p, 1 - core), ts.at[1], tr.at[5 + k], at.partner).wait_recv()

        def step(i, carry):
            at_rows = pl.ds(pl.multiple_of(p * rows + i * strip, strip), strip)
            whole = jnp.concatenate([x_ref[0, at_rows, :], x_ref[1, at_rows, :]], axis=1).astype(f32)
            mean = jnp.sum(whole * whole, axis=1, keepdims=True) / (2 * half)
            scaled = (whole * lax.rsqrt(mean + 1e-06) * gain_ref[...]).astype(bf16)
            for j in range(layers):
                nrm_ref[j, at_rows, :] = scaled[:, j * span : (j + 1) * span]
            return carry

        lax.fori_loop(0, rows // strip, step, 0)

    def add_layer(origin, fresh):
        def step(i, carry):
            at_rows = pl.ds(pl.multiple_of(i * rows, rows), rows)
            product = jnp.dot(
                nrm_ref[origin, at_rows, :],
                wbuf[zl, origin].reshape(span, wbuf.shape[5]),
                preferred_element_type=f32,
            )
            acc_ref[at_rows, :] = product if fresh else acc_ref[at_rows, :] + product
            return carry

        lax.fori_loop(0, PLANE, step, 0)

    def add_row(origin, row_y, first=0, stride=1):
        size = span // 2

        def step(i, carry):
            at_rows = pl.ds(pl.multiple_of((first + stride * i) * rows, rows), rows)
            acc_ref[at_rows, :] += jnp.dot(
                nrm_ref[origin, at_rows, pl.ds(pl.multiple_of(row_y * size, size), size)],
                wbuf[zl, origin, row_y].reshape(size, wbuf.shape[5]),
                preferred_element_type=f32,
            )
            return carry

        lax.fori_loop(0, PLANE // stride, step, 0)

    def add_last(rest=False):
        def two(d, up):
            if rest:
                add_row(ins.origin(up, d), 1 - y, 0, 2)
                return
            add_row(ins.origin(up, d), y)
            ins.on_y(d, up=up)
            add_row(ins.origin(up, d), 1 - y, 1, 2)

        for above in (False, True):
            for d, where in ((3, at_end), (2, inside)):
                mine = (z >= d) if above else (z + d < layers)

                @pl.when(mine & where)
                def _():
                    two(d, above)

    def add_both(d):
        ins.on_y(d)

        @pl.when(z >= d)
        def _():
            add_layer(z - d, False)

        @pl.when(z + d < layers)
        def _():
            add_layer(z + d, False)

    def from_x(s):
        ins.wait_x(s)
        ins.send_z(1, s, FAR)
        ins.send_z(1, s, NEAR, at_end)
        ins.send_y(1, s)
        ins.on_z(1, 0, s, FAR)

    from_x(0)
    send_tok_z(1, at_end)
    ins.on_z(1, 0, 0, NEAR, APART)
    from_x(1)
    send_tok_z(1, inside)
    ins.send_z(0, 1, NEAR, inside)
    for s in range(split):
        ins.send_z(1, s, NEAR, inside)
    outs.send_y(0, 0, inside)
    normalise(0, p_own)
    ins.on_z(1, 1, 0, FAR, PAIR, at_end)
    ins.on_z(2, 0, 0, FAR, only=at_end)
    ins.on_z(1, 1, 0, FAR, APART)
    ins.on_z(2, 0, 0, FAR, only=inside)
    ins.on_z(1, 1, 1, FAR, APART)
    tok_z(0, p_z).wait_recv()
    tok_far(0).start()
    ins.on_z(2, 0, 1, FAR, only=inside)
    ins.on_z(1, 1, 1, FAR, PAIR, at_end)
    ins.on_z(1, 0, 1, NEAR, APART)
    ins.on_z(1, 1, 0, FAR, PAIR, inside)
    for s in range(split):
        ins.on_z(1, 0, s, NEAR, PAIR)
    remote(block(p_x), block(p_x), ts.at[0], tr.at[0], at.xpeer).wait_recv()
    swaps[1].start()
    ins.on_z(2, 0, 1, FAR, only=at_end)
    outs.send_y(0, 0, at_end)
    ins.on_z(1, 1, 0, NEAR, APART)
    normalise(1, p_x)
    ins.on_z(1, 1, 1, NEAR, APART)
    tok_z(1, p_z).wait_recv()
    tok_far(1).start()
    swaps[2].start()
    outs.start_x()
    ins.on_z(2, 1, 0, FAR, only=inside)
    ins.on_z(2, 1, 0, FAR, only=at_end)
    normalise(2, p_z)
    ins.on_z(2, 0, 0, NEAR, only=inside)
    ins.on_z(1, 1, 1, FAR, PAIR, inside)
    for s in range(split):
        ins.on_z(1, 1, s, NEAR, PAIR)
    ins.on_z(3, 0, 0)
    outs.send_z(0, 0, only=at_end)
    ins.on_z(2, 0, 1, NEAR, only=inside)
    tok_far(0, p_far).wait_recv()
    tok_far(1, p_far).wait_recv()
    swaps[3].start()
    ins.on_z(2, 1, 1, FAR)
    ins.on_z(3, 0, 1)
    normalise(3, p_far)
    ins.on_z(2, 1, 0, NEAR, only=inside)
    ins.on_z(3, 1, 0)
    ins.on_y(0)
    add_layer(z, True)
    ins.on_z(2, 1, 1, NEAR, only=inside)
    outs.wait_x(0)
    outs.on_z(1, 0, 0, FAR, PAIR, inside)
    outs.send_z(0, 0, FAR, inside)
    outs.send_z(1, 0, FAR)
    outs.send_z(1, 0, NEAR, at_end)
    outs.send_y(1, 0, inside)
    ins.on_z(3, 1, 1)
    add_both(1)
    outs.send_y(1, 0, at_end)
    outs.on_z(1, 1, 0, FAR, PAIR, inside)
    outs.on_z(2, 0, 0, FAR, only=inside)

    @pl.when(at_end)
    def _():
        add_both(2)

    outs.on_z(1, 0, 0, FAR, APART)
    add_last()

    blocks = 2 * length // WINDOW

    def mix_spread(some):
        for i in some:
            run, start = i // 4, i % 4 * WINDOW
            here = pl.ds(i * WINDOW, WINDOW)
            ext[run, pl.ds(start + WINDOW, WINDOW), :] = acc_ref[here, 3 * chans + wide :].astype(bf16)
            both = acc_ref[here, chans : 3 * chans].astype(bf16).astype(f32)
            gext[run, pl.ds(start + front, WINDOW), :] = (both[:, :chans] * both[:, chans:]).astype(bf16).astype(f32)

    tail_blocks = range(blocks // 2 - 1, blocks, blocks // 2)
    mix_spread(tail_blocks)

    def tails(run, after, target, action):
        kv = remote(
            ext.at[run, pl.ds(length, WINDOW)], ext.at[after, pl.ds(0, WINDOW)],
            hs.at[2 * run], hr.at[2 * after], target,
        )
        gated = remote(
            gext.at[run, pl.ds(length, front)], gext.at[after, pl.ds(0, front)],
            hs.at[2 * run + 1], hr.at[2 * after + 1], target,
        )
        for copy in (kv, gated):
            getattr(copy, action)()

    def all_tails(action):
        @pl.when(y == 0)
        def _():
            for run in range(2):
                tails(run, run, at.ypeer, action)

        @pl.when(y == 1)
        def _():
            tails(0, 1, at.ypeer, action)

        @pl.when(at.has_after)
        def _():
            tails(1, 0, at.after, action)

    all_tails("start")
    for r in range(2):
        outs.on_z(1, r, 0, FAR, PAIR, at_end)
    add_last(True)
    mix_spread([i for i in range(blocks) if i not in tail_blocks])
    outs.on_z(3, 0, 0)
    for r in range(2):
        outs.on_z(1, r, 0, NEAR, PAIR)
        outs.send_z(r, 0, NEAR, inside)
    first_run = (y == 0) & (zh == 0)

    @pl.when(first_run)
    def _():
        ext[0, 0:WINDOW, :] = jnp.zeros((WINDOW, 2 * HEAD), bf16)
        gext[0, 0:front, :] = jnp.zeros((front, chans), f32)

    taps = sum(jnp.where(spot == c, taps_ref[:, c * chans : (c + 1) * chans], 0.0) for c in range(PLANE))
    row = lax.broadcasted_iota(jnp.int32, (WINDOW, 2 * WINDOW), 0)
    col = lax.broadcasted_iota(jnp.int32, (WINDOW, 2 * WINDOW), 1)
    dist = WINDOW + row - col
    near = (dist >= 0) & (dist < WINDOW)
    far = dist.astype(f32)

    for g in range(group):
        bias[g] = jnp.where(near, -slopes_ref[(core * PLANE + spot) * group + g] * far, -1e30)
    ones = jnp.where(lax.broadcasted_iota(jnp.int32, (2 * WINDOW, HEAD), 1) == 0, 1.0, 0.0).astype(bf16)

    def mix(run, blk, first=False):
        start = pl.multiple_of(blk * WINDOW, WINDOW)
        chunk = acc_ref[pl.ds(pl.multiple_of(run * length + start, WINDOW), WINDOW), :].astype(bf16)
        window = gext[run, pl.ds(start, WINDOW + front), :]
        conv = sum(
            taps[k : k + 1, :] * window[front - TAPS + 1 + k : front - TAPS + 1 + k + WINDOW]
            for k in range(TAPS)
        )
        pieces = [(chunk[:, :chans].astype(f32) * conv).astype(bf16)]
        kv = ext[run, pl.ds(start, 2 * WINDOW), :]
        keys, values = kv[:, :HEAD], jnp.concatenate([kv[:, HEAD:], ones], axis=1)
        offset = ((2 * zh + run) * 2 + y) * length
        for g in range(group):
            at_head = 3 * chans + g * HEAD
            query = chunk[:, at_head : at_head + HEAD] * jnp.asarray(HEAD ** (-0.5), bf16)
            scores = bias[g] + lax.dot_general(
                query, keys, (((1,), (1,)), ((), ())), preferred_element_type=f32
            )
            if first:
                scores = jnp.where(offset - WINDOW + col >= 0, scores, -1e30)
            sink = sinks_ref[spot * group + g]
            top = jnp.maximum(jnp.max(scores, axis=1, keepdims=True), sink)
            expo = jnp.exp(scores - top).astype(bf16)
            summed = jnp.dot(expo, values, preferred_element_type=f32)
            total = summed[:, HEAD : HEAD + 1] + jnp.exp(sink - top)
            pieces.append((summed[:, :HEAD] / total).astype(bf16))
        place = pl.ds(pl.multiple_of((2 * run + blk // 2) * WINDOW, WINDOW), WINDOW)
        hid[lax.rem(blk, 2), place, :] = jnp.concatenate(pieces, axis=1)

    def mix_run(run):
        for blk in range(1, 4):
            mix(run, blk)

    def mix_first():
        for run in range(2):
            mix(run, 0, True)

    outs.on_z(1, 1, 0, FAR, APART)
    mix_run(0)
    outs.on_z(2, 1, 0, FAR, only=inside)
    mix_run(1)

    def tails_in(after, target):
        for k, (ref, size) in enumerate(((ext, WINDOW), (gext, front))):
            remote(
                ref.at[after, pl.ds(length, size)], ref.at[after, pl.ds(0, size)],
                hs.at[2 * after + k], hr.at[2 * after + k], target,
            ).wait_recv()

    @pl.when(y == 1)
    def _():
        tails_in(0, at.ypeer)

    @pl.when(at.has_prior)
    def _():
        tails_in(0, at.prior)

    tails_in(1, at.ypeer)
    mix_first()

    lower = z < layers // 2
    cols = obuf.shape[3] * obuf.shape[4]
    order = [(0, True), (1, True), (0, False), (1, False), (3, True), (2, True), (3, False), (2, False)]
    chunks = len(order)

    def chunk_at(h):
        i, mine = order[h]
        return jnp.where(lower, i, layers - 1 - i), y if mine else 1 - y

    def product(side, h):
        layer, row_y = chunk_at(h)
        return lax.dot_general(
            hid[side], obuf[zl, layer, row_y].reshape(cols, hid.shape[2]),
            (((1,), (1,)), ((), ())), preferred_element_type=f32,
        )

    def slab(p):
        return pl.ds(pl.multiple_of(p * WINDOW, WINDOW), WINDOW)

    def swap(i):
        return remote(dsend.at[i], drecv.at[i], ds.at[0], dr.at[i], at.partner)

    def first_hop(i, j):
        if i % 2 == 0:
            target, p = at.xpeer, (2 * (1 - zl) if j == 0 else 2 * zl) + 1 - x
        else:
            target, p = at.zpeer, 2 * (1 - zl) + ((1 - x) if j == 0 else x)
        return remote(s1.at[i, slab(p)], r1.at[i, j], fs.at[0], fr.at[2 * i + j], target)

    def out_slab(i):
        layer, row_y = chunk_at(i)
        return pl.ds(pl.multiple_of((layer * 2 + row_y) * cols, cols), cols)

    def second_hop(i):
        return remote(s2.at[i], far_hbm.at[:, out_slab(i)], gs.at[0], gr.at[i], at.zpeer if i % 2 == 0 else at.xpeer)

    def begin(i):
        dsend[i] = product(1 - core, i).astype(bf16)
        own[i % 2] = product(core, i)
        swap(i).start()

    def fold(i):
        swap(i).wait_recv()
        s1[i] = (own[i % 2] + drecv[i].astype(f32)).astype(bf16)
        first_hop(i, 0).start()
        first_hop(i, 1).start()

    def relay(i):
        first_hop(i, 0).wait_recv()
        p = p_z if i % 2 == 0 else p_x
        s2[i] = (s1[i, slab(p), :].astype(f32) + r1[i, 0].astype(f32)).astype(bf16)
        second_hop(i).start()

    def out_copy(i):
        return pltpu.make_async_copy(out_ref.at[i], out_hbm.at[:, out_slab(i)], os.at[0])

    def collect(i):
        first_hop(i, 1).wait_recv()
        total = s1[i, slab(p_own), :].astype(f32) + r1[i, 1].astype(f32)
        out_ref[i] = total.astype(out_ref.dtype)
        out_copy(i).start()

    begin(0)
    outs.on_z(2, 0, 0, FAR, only=at_end)
    begin(1)
    fold(0)
    fold(1)
    outs.on_z(2, 1, 0, FAR, only=at_end)
    outs.on_z(2, 0, 0, NEAR, only=inside)
    outs.on_y(0)
    outs.on_y(1, sides=PAIR)
    begin(2)
    outs.on_z(1, 0, 0, NEAR, APART)
    outs.on_z(3, 1, 0)
    begin(3)
    fold(2)
    fold(3)
    outs.on_z(1, 1, 0, NEAR, APART)
    relay(0)
    outs.on_z(2, 1, 0, NEAR, only=inside)
    begin(4)
    relay(1)
    begin(5)
    fold(4)
    fold(5)
    collect(0)
    collect(1)
    relay(2)
    relay(3)
    outs.on_y(2)
    outs.on_y(3)
    begin(6)
    outs.on_y(1, sides=APART)
    begin(7)
    fold(6)
    fold(7)
    collect(2)
    collect(3)
    for h in range(4, chunks):
        relay(h)
        collect(h)

    def phase_finish():
        pltpu.make_async_copy(out_ref, out_ref, os.at[0]).wait()
        for h in range(chunks):
            second_hop(h).wait_recv()
        ins.finish()
        outs.finish()
        all_tails("wait_send")
        for ref, sem in (
            (x_ref.at[0, pl.ds(0, 3 * rows)], ts.at[0]),
            (x_ref.at[0], ts.at[1]),
            (dsend, ds.at[0]),
            (s1.at[pl.ds(0, chunks // 2)], fs.at[0]),
            (s2, gs.at[0]),
        ):
            remote(ref, ref, sem, dr.at[0], at.partner).wait_send()

    phase_finish()


def whole_layer(count, tokens, weights, gain, taps, slopes, sinks, wide):
    layers = count // PLANE
    rows, half = tokens.shape
    depth = weights[0].shape[0]
    width = sum(w.shape[1] for w in weights[:6]) // PLANE
    cols = weights[6].shape[0]
    inner = sum(w.shape[1] for w in weights[6:]) // PLANE
    chans = taps.shape[1] // PLANE
    bf16, f32 = jnp.bfloat16, jnp.float32
    dma = pltpu.SemaphoreType.DMA
    split = 2
    length = 2 * rows
    slab = 2 * cols
    chunks = 2 * layers

    def sems(parts):
        hops = layers * 4 * parts
        return [dma((number,)) for number in (4, hops, 1, layers, 1, 2 * parts)]

    smem = pl.BlockSpec(memory_space=pltpu.SMEM)
    return pl.pallas_call(
        functools.partial(layer_entry, count, chans, wide, split),
        out_shape=[jax.ShapeDtypeStruct((rows // 2, 2 * half), bf16)] * 2,
        in_specs=[smem] * 2 + [pl.BlockSpec(memory_space=pltpu.HBM)] * 11,
        out_specs=[pl.BlockSpec(memory_space=pltpu.HBM)] * 2,
        scratch_shapes=[pltpu.VMEM(w.shape, bf16) for w in weights]
        + [
            pltpu.VMEM(gain.shape, f32),
            pltpu.VMEM(taps.shape, f32),
            pltpu.VMEM((PLANE, depth, width), bf16),
            pltpu.VMEM((PLANE, cols, inner), bf16),
            pltpu.VMEM((chunks, WINDOW, slab), bf16),
            dma((11,)),
            dma((1,)),
            pltpu.VMEM((2, PLANE * rows, half), bf16),
            pltpu.VMEM((layers, PLANE * rows, 2 * half // layers), bf16),
            pltpu.VMEM((2, layers, 2, 2, depth, width), bf16),
            pltpu.VMEM((2, layers, 2, 2, cols, inner), bf16),
            pltpu.VMEM((PLANE * rows, width), f32),
            pltpu.VMEM((2, WINDOW + length, 2 * HEAD), bf16),
            pltpu.VMEM((2, 8 + length, chans), f32),
            pltpu.VMEM((QHEADS // KVHEADS, WINDOW, 2 * WINDOW), f32),
            pltpu.VMEM((2, PLANE * WINDOW, inner), bf16),
            pltpu.VMEM((chunks, PLANE * WINDOW, slab), bf16),
            pltpu.VMEM((chunks, PLANE * WINDOW, slab), bf16),
            pltpu.VMEM((2, PLANE * WINDOW, slab), f32),
            pltpu.VMEM((chunks, PLANE * WINDOW, slab), bf16),
            pltpu.VMEM((chunks, 2, WINDOW, slab), bf16),
            pltpu.VMEM((chunks, WINDOW, slab), bf16),
        ]
        + sems(split)
        + sems(1)
        + [dma((number,)) for number in (2, 9, 4, 4, 1, chunks, 1, 2 * chunks, 1, chunks)],
        compiler_params=pltpu.CompilerParams(
            collective_id=0, has_side_effects=True, vmem_limit_bytes=60 << 20
        ),
    )(slopes, sinks, tokens, *weights, gain, taps)


def add_kernel(a_ref, b_ref, out_ref):
    out_ref[...] = (a_ref[...].astype(jnp.float32) + b_ref[...].astype(jnp.float32)).astype(out_ref.dtype)


def add_pair(a, b):
    rows, cols = a.shape
    spec = pl.BlockSpec((rows // 2, cols), lambda i: (i, 0))
    return pl.pallas_call(
        add_kernel, grid=(2,), in_specs=[spec] * 2, out_specs=spec, out_shape=jax.ShapeDtypeStruct(a.shape, a.dtype)
    )(a, b)


def plane_body(
    tokens,
    norm_gain,
    outer_gate_w,
    inner_gate_w,
    signal_w,
    conv_taps,
    query_w,
    key_w,
    value_w,
    sink_logits,
    out_conv_w,
    out_attn_w,
):
    if tokens.shape[0] != 2 * WINDOW:
        return body(
            tokens, norm_gain, outer_gate_w, inner_gate_w, signal_w, conv_taps,
            query_w, key_w, value_w, sink_logits, out_conv_w, out_attn_w,
        )
    count = lax.axis_size("sp")
    wide = query_w.shape[1] // PLANE
    weights = (outer_gate_w, inner_gate_w, signal_w, query_w, key_w, value_w, out_conv_w.T, out_attn_w.T)
    slopes = jnp.array([2.0 ** (-8.0 * h / QHEADS) for h in range(1, QHEADS + 1)], jnp.float32)
    near, far = whole_layer(
        count, tokens, weights, norm_gain.reshape(1, -1), conv_taps, slopes, sink_logits, wide
    )
    return add_pair(near, far)


def solution(mesh):
    kv_local = KVHEADS // mesh.shape["tp"]
    fits = mesh.shape["tp"] == 2 and kv_local == PLANE and mesh.shape["sp"] == LAYERS * PLANE
    chosen = plane_body if fits else body
    in_specs = (
        P("sp", "tp"),
        P(),
        P("sp", "tp"),
        P("sp", "tp"),
        P("sp", "tp"),
        P(None, "tp"),
        P("sp", "tp"),
        P("sp", "tp"),
        P("sp", "tp"),
        P("tp"),
        P("tp", "sp"),
        P("tp", "sp"),
    )
    out_specs = P(("sp", "tp"), None)
    return jax.shard_map(chosen, mesh=mesh, in_specs=in_specs, out_specs=out_specs, check_vma=False)
```
